32 devices in a mesh: sp: 8 (over z, y), tp: 4 (over x, core).
Axes of the slice: x: 2, y: 2, z: 4, core: 2. Of those that a mesh axis runs over, the one named last changes fastest.
Arguments:
- queries: bfloat16 [4096, 1024], P('sp', 'tp'), may hold values from -6 to 6
- keys: bfloat16 [4096, 1024], P('sp', 'tp'), may hold values from -6 to 6
- values: bfloat16 [4096, 1024], P('sp', 'tp'), may hold values from -6 to 6
- output_gate_logits: bfloat16 [4096, 1024], P('sp', 'tp'), may hold values from -6 to 6
- input_gate_log: float32 [4096, 8], P('sp', 'tp'), may hold values from -5 to 125
- forget_gate_logits: float32 [4096, 8], P('sp', 'tp')
- extra_decay_log: float32 [4096, 8], P('sp', 'tp'), may hold values from -1 to 0
- document: int32 [4096], P('sp'), may hold values from 0 to 3, never falling along the last dimension, each value on 1 to 2048 neighbouring positions
- residual: bfloat16 [4096, 2048], P('sp', 'tp'), may hold values from -16 to 16
- cell_norm_gain: bfloat16 [1024], P('tp'), may hold values from 0.099609375 to 1.8984375
- output_weight: bfloat16 [1024, 2048], P('tp'), may hold values from -0.1875 to 0.1875
- mixer_norm_gain: bfloat16 [2048], P('tp'), may hold values from 0.099609375 to 1.8984375
- up_weight: bfloat16 [2048, 8192], P('sp', 'tp'), may hold values from -0.125 to 0.125
- down_weight: bfloat16 [8192, 2048], P('tp', 'sp'), may hold values from -0.0625 to 0.0625
Outputs:
- layer_out: bfloat16 [4096, 2048], P('sp', 'tp')
The draws below stay inside these ranges and needn't reach their ends.
All inputs are finite; a program needn't handle non-finite values.
Results may differ from the reference program's by a relative error of at most 0.015.
Values may be sent and summed in bfloat16 or wider, within the bound.
A program may use at most 128 MiB of HBM per device.

```python
import math
import jax
import jax.numpy as jnp
import numpy as np
from jax import lax

D = 2048
FF = 8192
HM = 8
DH = 128
BLOCK = 128
TOK_DEV = 512
TOKENS = 4096
DOCS = 4
MOST = 2048
N_SP = 8
N_TP = 4


def draw_input_gate_log(key, part):
    key_base = jax.random.fold_in(key, 0)
    return jnp.clip(jax.random.normal(key_base, (TOKENS, HM), jnp.float32), -4.0, 4.0)


def draw_forget_gate_logits(key, part):
    key_kind, key_device, key_noise = jax.random.split(key, 3)
    fast_heads = jax.random.randint(key_kind, (HM,), 0, 2) == 1
    device_rate = jax.random.uniform(key_device, (TOKENS // TOK_DEV, 1, 1), jnp.float32, 0.0, math.log(4.0))
    jitter = jax.random.uniform(key_noise, (TOKENS // TOK_DEV, TOK_DEV, HM), jnp.float32, -0.7, 0.7)
    slow_pre = math.log(8.0 * MOST) - device_rate + jitter
    fast_pre = math.log(40.0) + jitter
    result = jnp.where(fast_heads[None, None, :], fast_pre, slow_pre)
    return result.reshape(TOKENS, HM)


def draw_extra_decay_log(key, part):
    key_spot, key_head, key_depth = jax.random.split(key, 3)
    places = max(TOKENS // TOK_DEV * 2, 4)
    spots = jax.random.randint(key_spot, (places,), 0, TOKENS)
    heads_hit = jax.random.randint(key_head, (places,), 0, HM)
    depths = jax.random.uniform(key_depth, (places,), jnp.float32, math.log(0.5), math.log(0.8))
    return jnp.zeros((TOKENS, HM), jnp.float32).at[spots, heads_hit].min(depths)


def draw_residual(key, part):
    key_values = jax.random.fold_in(key, 0)
    ramp = jnp.exp(jnp.linspace(0.0, math.log(3.0), D)).astype(jnp.float32)
    entries = jnp.clip(jax.random.normal(key_values, (TOKENS, D), jnp.float32), -4.0, 4.0)
    return (entries * ramp[None, :] / 1.7).astype(jnp.bfloat16)


def shard_levels(rng, dims, cuts, smallest, high):
    loudness = 1.0
    for axis_at, parts in cuts:
        draws = jax.random.uniform(jax.random.fold_in(jax.random.fold_in(rng, 6), axis_at), (parts,), jnp.float32, smallest / len(cuts), high / len(cuts))
        loudness = loudness * jnp.repeat(jnp.exp(draws), dims[axis_at] // parts).reshape((-1,) + (1,) * (len(dims) - 1 - axis_at))
    return loudness


def split_up(amount, total, most, slope):
    portions = [(1 << 20) // math.isqrt(grade ** slope) + 1 for grade in range(2, amount + 1)]
    surplus, counts = total - most - (amount - 1), [1] * (amount - 1)
    while surplus > 0:
        free = [i for i in range(amount - 1) if counts[i] < most]
        mass, budget = sum([portions[i] for i in free]), surplus
        for i in free:
            more = min(most - counts[i], max(1, budget * portions[i] // mass), surplus)
            counts[i] = counts[i] + more
            surplus = surplus - more
    return np.array([most] + counts)


def ragged_sizes(stream_key, count, total, limit, lean):
    if count == 2:
        one = jax.random.randint(stream_key, (), max(1, total - limit), min(limit, total - 1) + 1)
        return jnp.stack([one, total - one])
    lengths = jnp.asarray(split_up(count, total, limit, lean), jnp.int32)
    couples = (count - 1) // 2
    source_of, receiver = lengths[1:1 + 2 * couples:2], lengths[2:2 + 2 * couples:2]
    slack = jnp.minimum(source_of - 1, limit - receiver)
    passed = jax.random.randint(jax.random.fold_in(stream_key, 1), (couples,), 0, 1 << 20) % (slack + 1)
    lengths = lengths.at[1:1 + 2 * couples:2].set(source_of - passed).at[2:2 + 2 * couples:2].set(receiver + passed)
    return lengths[jax.random.permutation(jax.random.fold_in(stream_key, 2), count)]


def gaussian(key, extent, scale, bound, cuts=(), dtype=jnp.bfloat16):
    values = jax.random.normal(key, extent, jnp.float32) * scale
    if len(cuts) > 0:
        values = shard_levels(key, extent, cuts, -0.22, 0.18) * values
    return jnp.clip(values, min=-bound, max=bound).astype(dtype)


def setup_inputs(seed: int = 0) -> dict:
    streams_of = jax.random.split(jax.random.key(seed), 15)
    queries = gaussian(streams_of[0], (TOKENS, HM * DH), 1.0, 6.0, ((0, 8), (1, 4)))
    keys = gaussian(streams_of[1], (TOKENS, HM * DH), 1.0, 6.0, ((0, 8), (1, 4)))
    values = gaussian(streams_of[2], (TOKENS, HM * DH), 1.0, 6.0, ((0, 8), (1, 4)))
    output_gate_logits = gaussian(streams_of[3], (TOKENS, HM * DH), 1.0, 6.0, ((0, 8), (1, 4)))
    input_gate_log = draw_input_gate_log(jax.random.fold_in(streams_of[14], 71), 0)
    forget_gate_logits = draw_forget_gate_logits(jax.random.fold_in(streams_of[14], 71), 0)
    extra_decay_log = draw_extra_decay_log(jax.random.fold_in(streams_of[14], 71), 0)
    document = jnp.searchsorted(jnp.cumsum(ragged_sizes(streams_of[7], DOCS, TOKENS, MOST, 0)), jnp.arange(TOKENS), side="right").astype(jnp.int32)
    residual = draw_residual(jax.random.fold_in(streams_of[14], 71), 0)
    cell_norm_gain = jnp.clip(1.0 + 0.18 * jax.random.normal(streams_of[9], (HM * DH,), jnp.float32), 0.099609375, 1.8984375).astype(jnp.bfloat16)
    output_weight = gaussian(streams_of[10], (HM * DH, D), (HM * DH) ** -0.5, 0.1875, ((0, 4),))
    mixer_norm_gain = jnp.clip(1.0 + 0.18 * jax.random.normal(streams_of[11], (D,), jnp.float32), 0.099609375, 1.8984375).astype(jnp.bfloat16)
    up_weight = gaussian(streams_of[12], (D, FF), D ** -0.5, 0.125, ((0, 8), (1, 4)))
    down_weight = gaussian(streams_of[13], (FF, D), FF ** -0.5, 0.0625, ((0, 4), (1, 8)))
    return dict(queries=queries, keys=keys, values=values, output_gate_logits=output_gate_logits, input_gate_log=input_gate_log, forget_gate_logits=forget_gate_logits, extra_decay_log=extra_decay_log, document=document, residual=residual, cell_norm_gain=cell_norm_gain, output_weight=output_weight, mixer_norm_gain=mixer_norm_gain, up_weight=up_weight, down_weight=down_weight)


NEG = -1e+30
EPS = 1e-06
HIGH = lax.Precision.HIGHEST

def block_terms(carry, inputs):
    memory, normer, stabil, last_doc = carry
    q_blk, k_blk, v_blk, gate_in, gate_log, doc_blk = inputs
    length = doc_blk.shape[0]
    causal = jnp.arange(length)[:, None] >= jnp.arange(length)[None, :]
    cumulative = jnp.cumsum(gate_log, axis=-1)
    same_doc = (doc_blk[:, None] == doc_blk[None, :]) & causal
    pair_log = cumulative[:, :, None] - cumulative[:, None, :] + gate_in[:, None, :]
    pair_log = jnp.where(same_doc[None], pair_log, NEG)
    live_rows = doc_blk == last_doc
    carried_log = jnp.where(live_rows[None, :], cumulative + stabil[:, None], NEG)
    peak_log = jnp.maximum(carried_log, lax.optimization_barrier(jnp.max(pair_log, axis=-1)))
    weights = jnp.exp(pair_log - peak_log[:, :, None])
    carried = jnp.exp(carried_log - peak_log)
    scores = jnp.einsum('htd,hsd->hts', q_blk, k_blk, precision=HIGH) * weights
    numerator = carried[:, :, None] * jnp.einsum('htd,hde->hte', q_blk, memory, precision=HIGH)
    numerator = numerator + jnp.einsum('hts,hse->hte', scores, v_blk, precision=HIGH)
    denominator = carried * jnp.einsum('htd,hd->ht', q_blk, normer, precision=HIGH) + lax.optimization_barrier(jnp.sum(scores, axis=-1))
    end_doc = doc_blk[-1]
    end_cum = cumulative[:, -1]
    keep_log = jnp.where((doc_blk == end_doc)[None, :], end_cum[:, None] - cumulative + gate_in, NEG)
    old_log = jnp.where(last_doc == end_doc, end_cum + stabil, NEG)
    new_stab = jnp.maximum(old_log, lax.optimization_barrier(jnp.max(keep_log, axis=-1)))
    scaled = jnp.exp(keep_log - new_stab[:, None])
    decayed = jnp.exp(old_log - new_stab)
    memory = decayed[:, None, None] * memory + jnp.einsum('hs,hsd,hse->hde', scaled, k_blk, v_blk, precision=HIGH)
    normer = decayed[:, None] * normer + jnp.einsum('hs,hsd->hd', scaled, k_blk, precision=HIGH)
    return ((memory, normer, new_stab, end_doc), (numerator, denominator, peak_log, cumulative))

def split_heads(source, blocks):
    return source.astype(jnp.float32).reshape(blocks, BLOCK, -1, DH).transpose(0, 2, 1, 3)

def split_gates(source, blocks):
    return source.reshape(blocks, BLOCK, -1).transpose(0, 2, 1)

def within_block_pass(queries, keys, values, input_gate_log, forget_gate_logits, extra_decay_log, document):
    blocks = queries.shape[0] // BLOCK
    head_count = queries.shape[1] // DH
    query_heads = split_heads(queries, blocks) * DH ** (-0.5)
    forget_log_values = jax.nn.log_sigmoid(forget_gate_logits) + extra_decay_log
    inputs = (query_heads, split_heads(keys, blocks), split_heads(values, blocks), split_gates(input_gate_log, blocks), split_gates(forget_log_values, blocks), document.reshape(blocks, BLOCK))
    initial = (jnp.zeros((head_count, DH, DH), jnp.float32), jnp.zeros((head_count, DH), jnp.float32), jnp.full((head_count,), NEG, jnp.float32), jnp.array(-1, jnp.int32))
    final_state, output_rows = lax.scan(block_terms, initial, inputs)
    return (query_heads, final_state, output_rows)

def head_mix(cell_out, output_gate_logits, cell_norm_gain):
    row_count = output_gate_logits.shape[0]
    head_count = cell_out.shape[1]
    hidden = cell_out.transpose(0, 2, 1, 3).reshape(row_count, head_count * DH)
    inverse = lax.rsqrt(lax.optimization_barrier(jnp.mean(hidden * hidden, axis=1, keepdims=True)) + EPS)
    gated = jax.nn.sigmoid(output_gate_logits.astype(jnp.float32))
    gains = cell_norm_gain.astype(jnp.float32)
    return (gated * hidden * inverse * gains[None, :]).astype(jnp.bfloat16)

def reference(queries, keys, values, output_gate_logits, input_gate_log, forget_gate_logits, extra_decay_log, document, residual, cell_norm_gain, output_weight, mixer_norm_gain, up_weight, down_weight):
    query_heads, final_state, output_rows = within_block_pass(queries, keys, values, input_gate_log, forget_gate_logits, extra_decay_log, document)
    numerator, denominator, peak_log, cumulative = output_rows
    cell_out = numerator / jnp.maximum(jnp.abs(denominator), 1.0)[..., None]
    mixed = head_mix(cell_out, output_gate_logits, cell_norm_gain)
    out_groups = output_weight.reshape(N_TP, -1, D).astype(jnp.float32)
    down_groups = down_weight.reshape(N_TP, -1, D).astype(jnp.float32)
    gain_wide = mixer_norm_gain.astype(jnp.float32)

    def rows_step(row_args):
        mixed_rows, resid_rows = row_args
        row_count = mixed_rows.shape[0]
        group_parts = jnp.einsum('rgk,gkd->grd', mixed_rows.reshape(row_count, N_TP, -1).astype(jnp.float32), out_groups)
        group_parts = lax.optimization_barrier(group_parts.astype(jnp.bfloat16)).astype(jnp.float32)
        first_sum = (resid_rows.astype(jnp.float32) + lax.optimization_barrier(jnp.sum(group_parts, axis=0))).astype(jnp.bfloat16)
        first_wide = lax.optimization_barrier(first_sum).astype(jnp.float32)
        inverse = lax.rsqrt(lax.optimization_barrier(jnp.mean(first_wide * first_wide, axis=1, keepdims=True)) + EPS)
        normed = (first_wide * inverse * gain_wide).astype(jnp.bfloat16)
        hidden = jnp.dot(normed, up_weight, preferred_element_type=jnp.float32)
        squared = jnp.square(jax.nn.relu(hidden)).astype(jnp.bfloat16)
        channel_parts = jnp.einsum('rgf,gfd->grd', squared.reshape(row_count, N_TP, -1).astype(jnp.float32), down_groups)
        channel_parts = lax.optimization_barrier(channel_parts.astype(jnp.bfloat16)).astype(jnp.float32)
        return (first_wide + lax.optimization_barrier(jnp.sum(channel_parts, axis=0))).astype(jnp.bfloat16)
    layer = lax.map(rows_step, (mixed.reshape(N_SP, -1, mixed.shape[1]), residual.reshape(N_SP, -1, D)))
    return layer.reshape(-1, D)
```

```python
import functools

import jax
import jax.numpy as jnp
from jax import lax
from jax.experimental import pallas as pl
from jax.experimental.pallas import tpu as pltpu
from jax.sharding import PartitionSpec as P

DH = 128
BLOCK = 128
MOST = 2048


NEG = -1e30
EPS = 1e-06
HIGH = lax.Precision.HIGHEST


def carried_in(value, axis, join, neutral):
    count, mine = (lax.axis_size(axis), lax.axis_index(axis))
    pieces = jax.tree.map(lambda part: lax.all_gather(part, axis), value)
    subtotal = jax.tree.map(
        lambda part, zero: jnp.full_like(part, 0) + jnp.asarray(zero, part.dtype), value, neutral
    )

    def step(position, subtotal):
        longer = join(subtotal, jax.tree.map(lambda part: part[position], pieces))
        return jax.tree.map(lambda new, old: jnp.where(position < mine, new, old), longer, subtotal)

    return lax.fori_loop(0, count - 1, step, subtotal)


def block_terms(carry, inputs):
    memory, normer, stabil, last_doc = carry
    q_blk, k_blk, v_blk, gate_in, gate_log, doc_blk = inputs
    length = doc_blk.shape[0]
    causal = jnp.arange(length)[:, None] >= jnp.arange(length)[None, :]
    cumulative = jnp.cumsum(gate_log, axis=-1)
    same_doc = (doc_blk[:, None] == doc_blk[None, :]) & causal
    pair_log = cumulative[:, :, None] - cumulative[:, None, :] + gate_in[:, None, :]
    pair_log = jnp.where(same_doc[None], pair_log, NEG)
    live_rows = doc_blk == last_doc
    carried_log = jnp.where(live_rows[None, :], cumulative + stabil[:, None], NEG)
    peak_log = jnp.maximum(carried_log, jnp.max(pair_log, axis=-1))
    weights = jnp.exp(pair_log - peak_log[:, :, None])
    carried = jnp.exp(carried_log - peak_log)
    scores = jnp.einsum("htd,hsd->hts", q_blk, k_blk, precision=HIGH) * weights
    numerator = carried[:, :, None] * jnp.einsum("htd,hde->hte", q_blk, memory, precision=HIGH)
    numerator = numerator + jnp.einsum("hts,hse->hte", scores, v_blk, precision=HIGH)
    denominator = carried * jnp.einsum("htd,hd->ht", q_blk, normer, precision=HIGH) + jnp.sum(
        scores, axis=-1
    )
    end_doc = doc_blk[-1]
    end_cum = cumulative[:, -1]
    keep_log = jnp.where(
        (doc_blk == end_doc)[None, :], end_cum[:, None] - cumulative + gate_in, NEG
    )
    old_log = jnp.where(last_doc == end_doc, end_cum + stabil, NEG)
    new_stab = jnp.maximum(old_log, jnp.max(keep_log, axis=-1))
    scaled = jnp.exp(keep_log - new_stab[:, None])
    decayed = jnp.exp(old_log - new_stab)
    memory = decayed[:, None, None] * memory + jnp.einsum(
        "hs,hsd,hse->hde", scaled, k_blk, v_blk, precision=HIGH
    )
    normer = decayed[:, None] * normer + jnp.einsum("hs,hsd->hd", scaled, k_blk, precision=HIGH)
    return ((memory, normer, new_stab, end_doc), (numerator, denominator, peak_log, cumulative))


def split_heads(source, blocks):
    return source.astype(jnp.float32).reshape(blocks, BLOCK, -1, DH).transpose(0, 2, 1, 3)


def split_gates(source, blocks):
    return source.reshape(blocks, BLOCK, -1).transpose(0, 2, 1)


def within_block_pass(
    queries, keys, values, input_gate_log, forget_gate_logits, extra_decay_log, document
):
    blocks = queries.shape[0] // BLOCK
    head_count = queries.shape[1] // DH
    query_heads = split_heads(queries, blocks) * DH ** (-0.5)
    forget_log_values = jax.nn.log_sigmoid(forget_gate_logits) + extra_decay_log
    inputs = (
        query_heads,
        split_heads(keys, blocks),
        split_heads(values, blocks),
        split_gates(input_gate_log, blocks),
        split_gates(forget_log_values, blocks),
        document.reshape(blocks, BLOCK),
    )
    initial = (
        jnp.zeros((head_count, DH, DH), jnp.float32),
        jnp.zeros((head_count, DH), jnp.float32),
        jnp.full((head_count,), NEG, jnp.float32),
        jnp.array(-1, jnp.int32),
    )
    final_state, output_rows = lax.scan(block_terms, initial, inputs)
    return (query_heads, final_state, output_rows)


def head_mix(cell_out, output_gate_logits, cell_norm_gain):
    row_count = output_gate_logits.shape[0]
    head_count = cell_out.shape[1]
    hidden = cell_out.transpose(0, 2, 1, 3).reshape(row_count, head_count * DH)
    squares = lax.psum(jnp.sum(hidden * hidden, axis=1), "tp")
    inverse = lax.rsqrt(squares / (head_count * DH * lax.axis_size("tp")) + EPS)
    gated = jax.nn.sigmoid(output_gate_logits.astype(jnp.float32))
    gains = cell_norm_gain.astype(jnp.float32)
    return (gated * hidden * inverse[:, None] * gains[None, :]).astype(jnp.bfloat16)


def join_states(earlier, later):
    mem_a, norm_a, stab_a, log_a, first_a, last_a = earlier
    mem_b, norm_b, stab_b, log_b, first_b, last_b = later
    joined = last_a == last_b
    stab_ab = jnp.where(joined, jnp.maximum(log_b + stab_a, stab_b), stab_b)
    weight_a = jnp.where(joined, jnp.exp(log_b + stab_a - stab_ab), 0.0)
    weight_b = jnp.exp(stab_b - stab_ab)
    memory = weight_a[:, None, None] * mem_a + weight_b[:, None, None] * mem_b
    normer = weight_a[:, None] * norm_a + weight_b[:, None] * norm_b
    blank_b = last_b < 0
    memory = jnp.where(blank_b, mem_a, memory)
    normer = jnp.where(blank_b, norm_a, normer)
    stabil = jnp.where(blank_b, stab_a, stab_ab)
    first_doc = jnp.where(first_a < 0, first_b, first_a)
    last_doc = jnp.where(blank_b, last_a, last_b)
    return (memory, normer, stabil, log_a + log_b, first_doc, last_doc)


def local(
    queries,
    keys,
    values,
    output_gate_logits,
    input_gate_log,
    forget_gate_logits,
    extra_decay_log,
    document,
    residual,
    cell_norm_gain,
    output_weight,
    mixer_norm_gain,
    up_weight,
    down_weight,
):
    query_heads, final_state, output_rows = within_block_pass(
        queries, keys, values, input_gate_log, forget_gate_logits, extra_decay_log, document
    )
    numerator, denominator, peak_log, cumulative = output_rows
    memory, normer, stabil, last_doc = final_state
    step_logs = cumulative[:, :, -1]
    offsets = jnp.cumsum(step_logs, axis=0) - step_logs
    through = cumulative + offsets[:, :, None]
    summary = (memory, normer, stabil, jnp.sum(step_logs, axis=0), document[0], last_doc)
    identity = (
        jnp.zeros_like(memory),
        jnp.zeros_like(normer),
        jnp.full_like(stabil, NEG),
        jnp.zeros_like(stabil),
        jnp.array(-1, jnp.int32),
        jnp.array(-1, jnp.int32),
    )
    prefix = carried_in(summary, "sp", join_states, identity)
    doc_blocks = document.reshape(-1, BLOCK)
    carried_log = jnp.where(
        (doc_blocks == prefix[5])[:, None, :], through + prefix[2][None, :, None], NEG
    )
    merged_peak = jnp.maximum(peak_log, carried_log)
    own_weight = jnp.exp(peak_log - merged_peak)
    far_weight = jnp.exp(carried_log - merged_peak)
    numerator = own_weight[..., None] * numerator + far_weight[..., None] * jnp.einsum(
        "nhtd,hde->nhte", query_heads, prefix[0], precision=HIGH
    )
    denominator = own_weight * denominator + far_weight * jnp.einsum(
        "nhtd,hd->nht", query_heads, prefix[1], precision=HIGH
    )
    cell_out = numerator / jnp.maximum(jnp.abs(denominator), 1.0)[..., None]
    mixed = head_mix(cell_out, output_gate_logits, cell_norm_gain)
    head_terms = jnp.dot(mixed, output_weight, preferred_element_type=jnp.float32)
    width = residual.shape[1]
    model_width = width * lax.axis_size("tp")
    own_sum = lax.psum_scatter(
        head_terms.astype(jnp.bfloat16), "tp", scatter_dimension=1, tiled=True
    ).astype(jnp.float32)
    first_sum = (residual.astype(jnp.float32) + own_sum).astype(jnp.bfloat16)
    first_wide = lax.optimization_barrier(first_sum).astype(jnp.float32)
    squares = lax.psum(jnp.sum(first_wide * first_wide, axis=1), "tp")
    inverse = lax.rsqrt(squares / model_width + EPS)
    normed_own = (first_wide * inverse[:, None] * mixer_norm_gain.astype(jnp.float32)).astype(
        jnp.bfloat16
    )
    normed_full = lax.all_gather(normed_own, "tp", axis=1, tiled=True)
    hidden = jnp.dot(
        normed_full,
        lax.all_gather(up_weight, "sp", axis=0, tiled=True),
        preferred_element_type=jnp.float32,
    )
    squared = jnp.square(jax.nn.relu(hidden)).astype(jnp.bfloat16)
    channel = jnp.dot(
        squared,
        lax.all_gather(down_weight, "sp", axis=1, tiled=True),
        preferred_element_type=jnp.float32,
    )
    own_channel = lax.psum_scatter(
        channel.astype(jnp.bfloat16), "tp", scatter_dimension=1, tiled=True
    ).astype(jnp.float32)
    return (lax.optimization_barrier(first_sum).astype(jnp.float32) + own_channel).astype(
        jnp.bfloat16
    )


MESH = pl.DeviceIdType.MESH
F32 = jnp.float32
BF16 = jnp.bfloat16
CHUNKS = 2


def to_columns(rows):
    pad = jnp.zeros((128 - rows.shape[0], rows.shape[1]), F32)
    return jnp.transpose(jnp.concatenate([rows, pad], axis=0))


def to_rows(column):
    return jnp.transpose(jnp.broadcast_to(column, (column.shape[0], 128)))[0:8, :]


def halves(wide):
    high = wide.astype(BF16)
    return high, (wide - high.astype(F32)).astype(BF16)


def two_pass(wide, narrow):
    high, low = halves(wide)
    return jnp.dot(high, narrow, preferred_element_type=F32) + jnp.dot(
        low, narrow, preferred_element_type=F32
    )


def layer_kernel(
    n,
    m,
    back,
    q_ref,
    k_ref,
    v_ref,
    og_ref,
    forget_ref,
    extra_ref,
    input_ref,
    doc_ref,
    resid_ref,
    cell_gain_ref,
    mixer_gain_ref,
    wout_ref,
    up_ref,
    down_ref,
    out_ref,
    up_all,
    down_all,
    wcols,
    state_out,
    state_in,
    tail_out,
    tail_in,
    numer_ref,
    y_all,
    squares_out,
    squares_in,
    first_ref,
    normed,
    sums_out,
    sums_in,
    squared,
    parts,
    sib_in,
    comb,
    rs_in,
    w_send,
    w_recv,
    z_send,
    z_recv,
    y_send,
    y_recv,
    state_send,
    state_recv,
    tail_send,
    tail_recv,
    mix_send,
    mix_recv,
    squares_send,
    squares_recv,
    normed_send,
    normed_recv,
    sums_send,
    sums_recv,
    sib_send,
    sib_recv,
    rs_send,
    rs_recv,
):
    sp, tp = lax.axis_index("sp"), lax.axis_index("tp")
    rows, heads = q_ref.shape[0], q_ref.shape[1] // DH
    depth, hidden_width = up_ref.shape
    own_width = hidden_width // 2
    width = resid_ref.shape[1]
    up_piece, down_piece = depth // CHUNKS, own_width // CHUNKS
    z, y = sp // 2, sp % 2
    p, x, c = z % 2, tp // 2, tp % 2

    def z_at(j):
        return (z, z + 1 - 2 * p, z + 2 - 4 * (z // 2), n // 2 - 1 - z)[j]

    def tp_at(bits):
        far_c = c + (bits % 2) * (1 - 2 * c)
        far_x = x + ((bits // 2) % 2) * (1 - 2 * x)
        return 2 * far_x + far_c

    partner = 2 * z_at(1) + y
    beside = 2 * z + 1 - y

    barrier = pltpu.get_barrier_semaphore()
    for k in range(1, n):
        pl.semaphore_signal(barrier, device_id=((sp + k) % n, tp), device_id_type=MESH)
    for k in range(1, m):
        pl.semaphore_signal(barrier, device_id=(sp, (tp + k) % m), device_id_type=MESH)
    pl.semaphore_signal(barrier, device_id=(partner, tp_at(2)), device_id_type=MESH)
    pl.semaphore_wait(barrier, n + m - 1)

    def remote(src, dst, send_sem, recv_sem, device):
        return pltpu.make_async_remote_copy(
            src_ref=src,
            dst_ref=dst,
            send_sem=send_sem,
            recv_sem=recv_sem,
            device_id=device,
            device_id_type=MESH,
        )

    def cols_of(owner):
        return pl.ds(pl.multiple_of(owner * width, width), width)

    def w_copy(k):
        return remote(
            wout_ref.at[:, cols_of(tp_at(k))],
            wcols.at[tp],
            w_send.at[k - 1],
            w_recv.at[k - 1],
            (sp, tp_at(k)),
        )

    def w_arrival(k):
        there = wcols.at[tp_at(k)]
        return remote(there, there, w_send.at[k - 1], w_recv.at[k - 1], (sp, tp_at(k)))

    def slot(stream, block, piece):
        if stream == 0:
            start = pl.multiple_of(block * depth + piece * up_piece, up_piece)
            return up_all.at[pl.ds(start, up_piece), :]
        return down_all.at[block, pl.ds(piece * down_piece, down_piece), :]

    def own_piece(stream, half, piece):
        if stream == 0:
            lanes = pl.ds(pl.multiple_of(half * own_width, own_width), own_width)
            return up_ref.at[pl.ds(piece * up_piece, up_piece), lanes]
        deep = pl.multiple_of(half * own_width + piece * down_piece, down_piece)
        return down_ref.at[pl.ds(deep, down_piece), :]

    def z_copy(stream, j, piece):
        return remote(
            own_piece(stream, z_at(j) % 2, piece),
            slot(stream, sp, piece),
            z_send.at[stream, j - 1, piece],
            z_recv.at[stream, j - 1, piece],
            (2 * z_at(j) + y, tp),
        )

    def z_arrival(stream, j, piece):
        there = slot(stream, 2 * z_at(j) + y, piece)
        return remote(
            there,
            there,
            z_send.at[stream, j - 1, piece],
            z_recv.at[stream, j - 1, piece],
            (2 * z_at(j) + y, tp),
        )

    def y_copy(stream, i, piece):
        there = slot(stream, 2 * z_at(i) + y, piece)
        return remote(
            own_piece(stream, p, piece) if i == 0 else there,
            there,
            y_send.at[stream, i, piece],
            y_recv.at[stream, i, piece],
            (beside, tp),
        )

    def y_arrival(stream, i, piece):
        there = slot(stream, 2 * z_at(i) + 1 - y, piece)
        return remote(
            there,
            there,
            y_send.at[stream, i, piece],
            y_recv.at[stream, i, piece],
            (beside, tp),
        )

    events = [(0, j, piece) for piece in range(CHUNKS) for j in range(1, n // 2)]
    events += [(1, j, piece) for j in range(1, n // 2) for piece in range(CHUNKS)]
    done = [0]

    def pump(until):
        while done[0] < until:
            stream, j, piece = events[done[0]]
            done[0] += 1
            z_arrival(stream, j, piece).wait_recv()
            y_copy(stream, j, piece).start()

    ups = CHUNKS * (n // 2 - 1)

    for k in range(1, m):
        w_copy(k).start()
    for j in range(1, n // 2):
        z_copy(0, j, 0).start()
    y_copy(0, 0, 0).start()

    document = doc_ref[...].astype(F32)
    across = lax.broadcasted_iota(jnp.int32, (rows, rows), 1)
    along = lax.broadcasted_iota(jnp.int32, (rows, rows), 0)
    upper = (along <= across).astype(BF16)
    forget = jax.nn.log_sigmoid(forget_ref[...]) + extra_ref[...]
    high = forget.astype(BF16).astype(F32)
    middle = (forget - high).astype(BF16).astype(F32)
    low = forget - high - middle
    slab = lax.broadcasted_iota(jnp.int32, (8, rows), 0)
    split = jnp.zeros((8, rows), F32)
    for h in range(heads):
        for i, part in enumerate((high, middle, low)):
            split = jnp.where(slab == heads * i + h, part[h : h + 1, :], split)
    summed = jnp.dot(split.astype(BF16), upper, preferred_element_type=F32)
    last_doc = document[:, rows - 1 : rows]
    sums, entry, totals, stabs, scaled = [], [], [], [], []
    for h in range(heads):
        line_sum = summed[h : h + 1, :]
        for i in range(1, 3):
            line_sum = line_sum + summed[heads * i + h : heads * i + h + 1, :]
        sums.append(line_sum)
        entry.append(input_ref[h : h + 1, :] - line_sum)
        total = line_sum[:, rows - 1 : rows]
        keep = jnp.where(document == last_doc, total + entry[h], NEG)
        stab = jnp.max(keep, axis=1, keepdims=True)
        totals.append(total)
        stabs.append(stab)
        scaled.append(jnp.exp(keep - stab))
    packed = jnp.broadcast_to(document, (8, rows))
    for h in range(heads):
        packed = jnp.where(slab == h, sums[h], packed)
        packed = jnp.where(slab == heads + h, scaled[h], packed)
    columns = to_columns(packed)
    doc_col = columns[:, 2 * heads : 2 * heads + 1]
    line = lax.broadcasted_iota(jnp.int32, (8, DH), 0)
    for h in range(heads):
        mine = slice(h * DH, (h + 1) * DH)
        weighted = k_ref[:, mine].astype(F32) * columns[:, heads + h : heads + h + 1]
        state_out[h] = lax.dot_general(
            weighted.astype(BF16),
            v_ref[:, mine],
            (((0,), (0,)), ((), ())),
            preferred_element_type=F32,
        ).astype(BF16)
        tail = jnp.broadcast_to(jnp.sum(weighted, axis=0, keepdims=True), (8, DH))
        tail = jnp.where(line == 1, stabs[h], tail)
        tail = jnp.where(line == 2, totals[h], tail)
        tail = jnp.where(line == 3, last_doc, tail)
        tail_out[h] = tail

    def state_copies(k):
        return [
            remote(src, dst.at[k - 1], send_sem.at[k - 1], recv_sem.at[k - 1], ((sp + k) % n, tp))
            for src, dst, send_sem, recv_sem in (
                (tail_out, tail_in, tail_send, tail_recv),
                (state_out, state_in, state_send, state_recv),
            )
        ]

    for k in range(1, back + 1):

        @pl.when(sp + k < n)
        def _():
            for copy in state_copies(k):
                copy.start()

        @pl.when(sp < k)
        def _():
            tail_in[k - 1] = jnp.zeros((heads, 8, DH), F32)
            state_in[k - 1] = jnp.zeros((heads, DH, DH), BF16)

    for piece in range(1, CHUNKS):
        for j in range(1, n // 2):
            z_copy(0, j, piece).start()
        y_copy(0, 0, piece).start()

    half_lanes = pl.ds(pl.multiple_of(p * own_width, own_width), own_width)
    up_all[pl.ds(pl.multiple_of(sp * depth, depth), depth), :] = up_ref[:, half_lanes]
    down_all[sp] = down_ref[half_lanes, :]

    step = min(rows, 256)
    locals_of = []
    for h in range(heads):
        mine = slice(h * DH, (h + 1) * DH)
        peaks, denoms = [], []
        for start in range(0, rows, step):
            stop = start + step
            here = slice(start, stop)
            scores = lax.dot_general(
                q_ref[here, mine],
                k_ref[0:stop, mine],
                (((1,), (1,)), ((), ())),
                preferred_element_type=F32,
            ) * (DH**-0.5)
            pair = columns[here, h : h + 1] + entry[h][:, 0:stop]
            seen = (doc_col[here] == document[:, 0:stop]) & (
                along[here, 0:stop] >= across[here, 0:stop]
            )
            pair = jnp.where(seen, pair, NEG)
            peak = jnp.max(pair, axis=1, keepdims=True)
            scores = scores * jnp.exp(pair - peak)
            numer_ref[h, here, :] = two_pass(scores, v_ref[0:stop, mine])
            peaks.append(peak)
            denoms.append(jnp.sum(scores, axis=1, keepdims=True))
        locals_of.append((jnp.concatenate(peaks, axis=0), jnp.concatenate(denoms, axis=0)))
        pump(PUMPS_LOCAL[h] if h < len(PUMPS_LOCAL) else 0)

    for k in range(1, back + 1):

        @pl.when(sp >= k)
        def _():
            for copy in state_copies(k):
                copy.wait_recv()

    def mix_copy(k, h):
        here = y_all.at[tp, :, pl.ds(h * DH, DH)]
        return remote(
            here, here, mix_send.at[k - 1, h], mix_recv.at[k - 1, h], (sp, tp_at(k))
        )

    def mix_forward(h):
        there = y_all.at[tp_at(2), :, pl.ds(h * DH, DH)]
        return remote(there, there, mix_send.at[2, h], mix_recv.at[2, h], (sp, tp_at(1)))

    def mix_arrival(k, h):
        there = y_all.at[tp_at(k), :, pl.ds(h * DH, DH)]
        return remote(
            there, there, mix_send.at[k - 1, h], mix_recv.at[k - 1, h], (sp, tp_at(k))
        )

    first_doc = document[:, 0:1]
    square_sum = jnp.zeros((rows, DH), F32)
    for h in range(heads):
        mine = slice(h * DH, (h + 1) * DH)
        between = jnp.zeros((1, DH), F32)
        logs, valids = [], []
        best = jnp.full((1, DH), NEG, F32)
        for k in range(1, back + 1):
            tail = tail_in[k - 1, h]
            far = lax.broadcasted_iota(jnp.int32, (1, DH), 1) * 0 + sp
            valid = (tail[3:4, :] == first_doc) & (far >= k)
            log = jnp.where(valid, between + tail[1:2, :], NEG)
            between = between + tail[2:3, :]
            best = jnp.maximum(best, log)
            logs.append(log)
            valids.append(valid)
        memory = jnp.zeros((DH, DH), F32)
        normer = jnp.zeros((1, DH), F32)
        for k in range(1, back + 1):
            weight = jnp.where(valids[k - 1], jnp.exp(logs[k - 1] - best), 0.0)
            memory = memory + jnp.where(
                valids[k - 1], weight * state_in[k - 1, h].astype(F32), 0.0
            )
            normer = normer + jnp.where(
                valids[k - 1], weight * tail_in[k - 1, h, 0:1, :], 0.0
            )
        peak, denom = locals_of[h]
        carried = jnp.where(doc_col == first_doc, columns[:, h : h + 1] + best[:, 0:1], NEG)
        merged = jnp.maximum(peak, carried)
        own = jnp.exp(peak - merged)
        other = jnp.exp(carried - merged) * (DH**-0.5)
        query = q_ref[:, mine]
        high, low = halves(memory)
        reached = jnp.dot(query, high, preferred_element_type=F32) + jnp.dot(
            query, low, preferred_element_type=F32
        )
        numer = own * numer_ref[h] + other * reached
        denom = own * denom + other * jnp.sum(
            query.astype(F32) * normer, axis=1, keepdims=True
        )
        cell = numer / jnp.maximum(jnp.abs(denom), 1.0)
        square_sum = square_sum + cell * cell
        gated = jax.nn.sigmoid(og_ref[:, mine].astype(F32))
        y_all[tp, :, mine] = (gated * cell * cell_gain_ref[:, mine].astype(F32)).astype(BF16)
        for k in range(1, 3):
            mix_copy(k, h).start()
    squares_out[...] = to_rows(jnp.sum(square_sum, axis=1, keepdims=True))

    def square_copy(k):
        return remote(
            squares_out,
            squares_in.at[k - 1],
            squares_send.at[k - 1],
            squares_recv.at[k - 1],
            (sp, tp_at(k)),
        )

    for k in range(1, m):
        square_copy(k).start()
    here = cols_of(tp)
    attn = jnp.dot(y_all[tp], wout_ref[:, here], preferred_element_type=F32)
    pump(PUMPS_MIX)
    for h in range(heads):
        mix_arrival(2, h).wait_recv()
        mix_forward(h).start()
    for k in (1, 2, 3):
        w_arrival(k).wait_recv()
        if k != 2:
            for h in range(heads):
                mix_arrival(k, h).wait_recv()
        attn = attn + jnp.dot(
            y_all[tp_at(k)], wcols[tp_at(k)], preferred_element_type=F32
        )
    squares = squares_out[...]
    for k in range(1, m):
        square_copy(k).wait_recv()
        squares = squares + squares_in[k - 1]
    inverse = lax.rsqrt(to_columns(squares)[:, 0:1] / (heads * DH * m) + EPS)
    first = (resid_ref[...].astype(F32) + attn * inverse).astype(BF16)
    first_ref[...] = first
    first = first.astype(F32)

    def plane(bit):
        return p + bit * (1 - 2 * p)

    def rows_of(bit):
        return pl.ds(pl.multiple_of(plane(bit) * rows, rows), rows)

    normed[rows_of(0), here] = (first * mixer_gain_ref[...].astype(F32)).astype(BF16)

    def group_at(bits):
        return (sp + (bits // 4) * (partner - sp), tp_at(bits % 4))

    def normed_block(bits):
        return normed.at[rows_of(bits // 4), cols_of(tp_at(bits % 4))]

    def normed_copy(source, flip):
        block = normed_block(source)
        rel = source + flip - 1
        return remote(block, block, normed_send.at[rel], normed_recv.at[rel], group_at(flip))

    def normed_arrival(rel):
        block = normed_block(rel)
        return remote(
            block, block, normed_send.at[rel - 1], normed_recv.at[rel - 1], group_at(rel % 2 or rel)
        )

    routes = ((0, 2), (0, 4), (0, 1), (2, 1), (4, 2), (4, 1), (6, 1))
    for route in routes[:3]:
        normed_copy(*route).start()
    sums_out[0] = to_rows(jnp.sum(first * first, axis=1, keepdims=True))

    def sums_copy(k):
        return remote(
            sums_out.at[k // 4],
            sums_in.at[k - 1],
            sums_send.at[k - 1],
            sums_recv.at[k - 1],
            group_at(k),
        )

    for k in range(1, m):
        sums_copy(k).start()

    for j in range(1, n // 2):
        for piece in range(CHUNKS):
            z_copy(1, j, piece).start()
    for piece in range(CHUNKS):
        y_copy(1, 0, piece).start()

    total = sums_out[0]
    for k in range(1, m):
        sums_copy(k).wait_recv()
        total = total + sums_in[k - 1]
    sums_out[1] = total
    sums_copy(4).start()

    normed_arrival(2).wait_recv()
    normed_copy(2, 1).start()
    pump(PUMPS_NORMED)
    normed_arrival(4).wait_recv()
    normed_copy(4, 2).start()
    normed_copy(4, 1).start()
    normed_arrival(1).wait_recv()
    normed_arrival(3).wait_recv()
    pump(ups)
    for i in range(n // 2):
        for piece in range(CHUNKS):
            y_arrival(0, i, piece).wait_recv()

    tile = min(own_width, 256)

    def up_half(bit, line_sums):
        scale = lax.rsqrt(to_columns(line_sums)[:, 0:1] / (width * m) + EPS)

        def up_tile(t, carry):
            cols = pl.ds(pl.multiple_of(t * tile, tile), tile)
            raw = jnp.dot(normed[rows_of(bit), :], up_all[:, cols], preferred_element_type=F32)
            hidden = jnp.maximum(raw * scale, 0.0)
            squared[rows_of(bit), cols] = (hidden * hidden).astype(BF16)
            return carry

        lax.fori_loop(0, own_width // tile, up_tile, 0)

    up_half(0, total)
    normed_arrival(6).wait_recv()
    normed_copy(6, 1).start()
    normed_arrival(5).wait_recv()
    normed_arrival(7).wait_recv()
    sums_copy(4).wait_recv()
    up_half(1, sums_in[3])

    blocks = [(j, side) for j in range(n // 2) for side in range(2)]

    def place(i):
        j, side = blocks[i]
        owner = z_at(j)
        return owner, owner // 2, y + side * (1 - 2 * y)

    def sib_copy(i):
        _, far_x, half = place(i)
        return remote(
            parts.at[i],
            sib_in.at[far_x, half],
            sib_send.at[far_x, half],
            sib_recv.at[far_x, half],
            (sp, tp_at(1)),
        )

    def rs_copy(i, cross):
        _, far_x, half = place(i)
        turn = (far_x + x) % 2
        rel = turn + 2 * cross - 1
        return turn, remote(
            comb.at[far_x, half, rows_of(cross), :],
            rs_in.at[rel, half],
            rs_send.at[far_x, half, cross],
            rs_recv.at[rel, half],
            (sp + cross * (partner - sp), 2 * far_x + c),
        )

    def down_block(i):
        j, side = blocks[i]
        owner, _, half = place(i)
        block = 2 * owner + half
        for bit in range(2):
            there = slice(bit * rows, (bit + 1) * rows)
            parts[i, there, :] = jnp.dot(
                squared[there, :], down_all[block], preferred_element_type=F32
            ).astype(BF16)

        @pl.when(owner % 2 != c)
        def _():
            sib_copy(i).start()

    def combine(i):
        owner, far_x, half = place(i)

        @pl.when(owner % 2 == c)
        def _():
            sib_copy(i).wait_recv()
            comb[far_x, half] = (
                parts[i].astype(F32) + sib_in[far_x, half].astype(F32)
            ).astype(BF16)
            rs_copy(i, 1)[1].start()
            turn, copy = rs_copy(i, 0)

            @pl.when(turn == 1)
            def _():
                copy.start()

    for i, (j, side) in enumerate(blocks):
        if side == 0:
            if j > 0:
                pump(ups + CHUNKS * j)
        else:
            for piece in range(CHUNKS):
                y_arrival(1, j, piece).wait_recv()
        down_block(i)
        if i > 0:
            combine(i - 1)
    combine(len(blocks) - 1)

    for half in range(2):
        cols = slice(half * depth, (half + 1) * depth)
        total = first_ref[:, cols].astype(F32) + comb[x, half, rows_of(0), :].astype(F32)
        for rel in range(1, 4):
            there = rs_in.at[rel - 1, half]
            remote(
                there,
                there,
                rs_send.at[0, 0, 0],
                rs_recv.at[rel - 1, half],
                group_at(2 * (rel % 2) + 4 * (rel // 2)),
            ).wait_recv()
            total = total + rs_in[rel - 1, half].astype(F32)
        out_ref[:, cols] = total.astype(BF16)

    for k in range(1, m):
        w_copy(k).wait_send()
        square_copy(k).wait_send()
        for h in range(heads):
            (mix_copy(k, h) if k < 3 else mix_forward(h)).wait_send()
    for k in range(1, m + 1):
        sums_copy(k).wait_send()
    for route in routes:
        normed_copy(*route).wait_send()
    for stream in range(2):
        for piece in range(CHUNKS):
            for j in range(1, n // 2):
                z_copy(stream, j, piece).wait_send()
            for i in range(n // 2):
                y_copy(stream, i, piece).wait_send()
    for k in range(1, back + 1):

        @pl.when(sp + k < n)
        def _():
            for copy in state_copies(k):
                copy.wait_send()

    for i in range(len(blocks)):
        owner = place(i)[0]

        @pl.when(owner % 2 != c)
        def _():
            sib_copy(i).wait_send()

        @pl.when(owner % 2 == c)
        def _():
            rs_copy(i, 1)[1].wait_send()
            turn, copy = rs_copy(i, 0)

            @pl.when(turn == 1)
            def _():
                copy.wait_send()


PUMPS_LOCAL = (0, 1)
PUMPS_MIX = 2
PUMPS_NORMED = 5


def fused(
    n,
    m,
    queries,
    keys,
    values,
    output_gate_logits,
    input_gate_log,
    forget_gate_logits,
    extra_decay_log,
    document,
    residual,
    cell_norm_gain,
    output_weight,
    mixer_norm_gain,
    up_weight,
    down_weight,
):
    rows, heads = queries.shape[0], queries.shape[1] // DH
    depth, hidden_width = up_weight.shape
    width = residual.shape[1]
    own_width = hidden_width // 2
    back = min(n - 1, (MOST - 2) // rows + 1)
    dma = pltpu.SemaphoreType.DMA
    lines = n // 2
    return pl.pallas_call(
        functools.partial(layer_kernel, n, m, back),
        out_shape=jax.ShapeDtypeStruct((rows, width), BF16),
        in_specs=[pl.BlockSpec(memory_space=pltpu.VMEM)] * 14,
        out_specs=pl.BlockSpec(memory_space=pltpu.VMEM),
        scratch_shapes=[
            pltpu.VMEM((n * depth, own_width), BF16),
            pltpu.VMEM((n, own_width, depth), BF16),
            pltpu.VMEM((m, heads * DH, width), BF16),
            pltpu.VMEM((heads, DH, DH), BF16),
            pltpu.VMEM((back, heads, DH, DH), BF16),
            pltpu.VMEM((heads, 8, DH), F32),
            pltpu.VMEM((back, heads, 8, DH), F32),
            pltpu.VMEM((heads, rows, DH), F32),
            pltpu.VMEM((m, rows, heads * DH), BF16),
            pltpu.VMEM((8, rows), F32),
            pltpu.VMEM((m - 1, 8, rows), F32),
            pltpu.VMEM((rows, width), BF16),
            pltpu.VMEM((2 * rows, m * width), BF16),
            pltpu.VMEM((2, 8, rows), F32),
            pltpu.VMEM((m, 8, rows), F32),
            pltpu.VMEM((2 * rows, own_width), BF16),
            pltpu.VMEM((n, 2 * rows, depth), BF16),
            pltpu.VMEM((2, 2, 2 * rows, depth), BF16),
            pltpu.VMEM((2, 2, 2 * rows, depth), BF16),
            pltpu.VMEM((3, 2, rows, depth), BF16),
            dma((m - 1,)),
            dma((m - 1,)),
            dma((2, lines - 1, CHUNKS)),
            dma((2, lines - 1, CHUNKS)),
            dma((2, lines, CHUNKS)),
            dma((2, lines, CHUNKS)),
            dma((back,)),
            dma((back,)),
            dma((back,)),
            dma((back,)),
            dma((m - 1, heads)),
            dma((m - 1, heads)),
            dma((m - 1,)),
            dma((m - 1,)),
            dma((2 * m - 1,)),
            dma((2 * m - 1,)),
            dma((m,)),
            dma((m,)),
            dma((2, 2)),
            dma((2, 2)),
            dma((2, 2, 2)),
            dma((3, 2)),
        ],
        compiler_params=pltpu.CompilerParams(
            collective_id=0, has_side_effects=True, vmem_limit_bytes=60 * 1024 * 1024
        ),
        name="layer",
    )(
        queries,
        keys,
        values,
        output_gate_logits,
        forget_gate_logits.T,
        extra_decay_log.T,
        input_gate_log.T,
        document[None, :],
        residual,
        cell_norm_gain[None, :],
        mixer_norm_gain[None, :],
        output_weight,
        up_weight,
        down_weight,
    )


def either(n, m, *args):
    depth, hidden_width = args[12].shape
    heads = args[0].shape[1] // DH
    fits = n == 8 and m == 4 and depth % 128 == 0 and hidden_width % 512 == 0
    fits = fits and 3 * heads <= 8 and args[8].shape[1] == 2 * depth
    fits = fits and args[0].shape[0] % 256 == 0
    if fits:
        return fused(n, m, *args)
    return local(*args)


def solution(mesh):
    in_specs = (
        P("sp", "tp"),
        P("sp", "tp"),
        P("sp", "tp"),
        P("sp", "tp"),
        P("sp", "tp"),
        P("sp", "tp"),
        P("sp", "tp"),
        P("sp"),
        P("sp", "tp"),
        P("tp"),
        P("tp", None),
        P("tp"),
        P("sp", "tp"),
        P("tp", "sp"),
    )
    out_specs = P("sp", "tp")
    body = functools.partial(either, mesh.shape["sp"], mesh.shape["tp"])
    return jax.shard_map(body, mesh=mesh, in_specs=in_specs, out_specs=out_specs, check_vma=False)
```

```python
import functools

import jax
import jax.numpy as jnp
from jax import lax
from jax.experimental import pallas as pl
from jax.experimental.pallas import tpu as pltpu
from jax.sharding import PartitionSpec as P

DH = 128
BLOCK = 128
MOST = 2048


NEG = -1e30
EPS = 1e-06
HIGH = lax.Precision.HIGHEST


def carried_in(value, axis, join, neutral):
    count, mine = (lax.axis_size(axis), lax.axis_index(axis))
    pieces = jax.tree.map(lambda part: lax.all_gather(part, axis), value)
    subtotal = jax.tree.map(
        lambda part, zero: jnp.full_like(part, 0) + jnp.asarray(zero, part.dtype), value, neutral
    )

    def step(position, subtotal):
        longer = join(subtotal, jax.tree.map(lambda part: part[position], pieces))
        return jax.tree.map(lambda new, old: jnp.where(position < mine, new, old), longer, subtotal)

    return lax.fori_loop(0, count - 1, step, subtotal)


def block_terms(carry, inputs):
    memory, normer, stabil, last_doc = carry
    q_blk, k_blk, v_blk, gate_in, gate_log, doc_blk = inputs
    length = doc_blk.shape[0]
    causal = jnp.arange(length)[:, None] >= jnp.arange(length)[None, :]
    cumulative = jnp.cumsum(gate_log, axis=-1)
    same_doc = (doc_blk[:, None] == doc_blk[None, :]) & causal
    pair_log = cumulative[:, :, None] - cumulative[:, None, :] + gate_in[:, None, :]
    pair_log = jnp.where(same_doc[None], pair_log, NEG)
    live_rows = doc_blk == last_doc
    carried_log = jnp.where(live_rows[None, :], cumulative + stabil[:, None], NEG)
    peak_log = jnp.maximum(carried_log, jnp.max(pair_log, axis=-1))
    weights = jnp.exp(pair_log - peak_log[:, :, None])
    carried = jnp.exp(carried_log - peak_log)
    scores = jnp.einsum("htd,hsd->hts", q_blk, k_blk, precision=HIGH) * weights
    numerator = carried[:, :, None] * jnp.einsum("htd,hde->hte", q_blk, memory, precision=HIGH)
    numerator = numerator + jnp.einsum("hts,hse->hte", scores, v_blk, precision=HIGH)
    denominator = carried * jnp.einsum("htd,hd->ht", q_blk, normer, precision=HIGH) + jnp.sum(
        scores, axis=-1
    )
    end_doc = doc_blk[-1]
    end_cum = cumulative[:, -1]
    keep_log = jnp.where(
        (doc_blk == end_doc)[None, :], end_cum[:, None] - cumulative + gate_in, NEG
    )
    old_log = jnp.where(last_doc == end_doc, end_cum + stabil, NEG)
    new_stab = jnp.maximum(old_log, jnp.max(keep_log, axis=-1))
    scaled = jnp.exp(keep_log - new_stab[:, None])
    decayed = jnp.exp(old_log - new_stab)
    memory = decayed[:, None, None] * memory + jnp.einsum(
        "hs,hsd,hse->hde", scaled, k_blk, v_blk, precision=HIGH
    )
    normer = decayed[:, None] * normer + jnp.einsum("hs,hsd->hd", scaled, k_blk, precision=HIGH)
    return ((memory, normer, new_stab, end_doc), (numerator, denominator, peak_log, cumulative))


def split_heads(source, blocks):
    return source.astype(jnp.float32).reshape(blocks, BLOCK, -1, DH).transpose(0, 2, 1, 3)


def split_gates(source, blocks):
    return source.reshape(blocks, BLOCK, -1).transpose(0, 2, 1)


def within_block_pass(
    queries, keys, values, input_gate_log, forget_gate_logits, extra_decay_log, document
):
    blocks = queries.shape[0] // BLOCK
    head_count = queries.shape[1] // DH
    query_heads = split_heads(queries, blocks) * DH ** (-0.5)
    forget_log_values = jax.nn.log_sigmoid(forget_gate_logits) + extra_decay_log
    inputs = (
        query_heads,
        split_heads(keys, blocks),
        split_heads(values, blocks),
        split_gates(input_gate_log, blocks),
        split_gates(forget_log_values, blocks),
        document.reshape(blocks, BLOCK),
    )
    initial = (
        jnp.zeros((head_count, DH, DH), jnp.float32),
        jnp.zeros((head_count, DH), jnp.float32),
        jnp.full((head_count,), NEG, jnp.float32),
        jnp.array(-1, jnp.int32),
    )
    final_state, output_rows = lax.scan(block_terms, initial, inputs)
    return (query_heads, final_state, output_rows)


def head_mix(cell_out, output_gate_logits, cell_norm_gain):
    row_count = output_gate_logits.shape[0]
    head_count = cell_out.shape[1]
    hidden = cell_out.transpose(0, 2, 1, 3).reshape(row_count, head_count * DH)
    squares = lax.psum(jnp.sum(hidden * hidden, axis=1), "tp")
    inverse = lax.rsqrt(squares / (head_count * DH * lax.axis_size("tp")) + EPS)
    gated = jax.nn.sigmoid(output_gate_logits.astype(jnp.float32))
    gains = cell_norm_gain.astype(jnp.float32)
    return (gated * hidden * inverse[:, None] * gains[None, :]).astype(jnp.bfloat16)


def join_states(earlier, later):
    mem_a, norm_a, stab_a, log_a, first_a, last_a = earlier
    mem_b, norm_b, stab_b, log_b, first_b, last_b = later
    joined = last_a == last_b
    stab_ab = jnp.where(joined, jnp.maximum(log_b + stab_a, stab_b), stab_b)
    weight_a = jnp.where(joined, jnp.exp(log_b + stab_a - stab_ab), 0.0)
    weight_b = jnp.exp(stab_b - stab_ab)
    memory = weight_a[:, None, None] * mem_a + weight_b[:, None, None] * mem_b
    normer = weight_a[:, None] * norm_a + weight_b[:, None] * norm_b
    blank_b = last_b < 0
    memory = jnp.where(blank_b, mem_a, memory)
    normer = jnp.where(blank_b, norm_a, normer)
    stabil = jnp.where(blank_b, stab_a, stab_ab)
    first_doc = jnp.where(first_a < 0, first_b, first_a)
    last_doc = jnp.where(blank_b, last_a, last_b)
    return (memory, normer, stabil, log_a + log_b, first_doc, last_doc)


def local(
    queries,
    keys,
    values,
    output_gate_logits,
    input_gate_log,
    forget_gate_logits,
    extra_decay_log,
    document,
    residual,
    cell_norm_gain,
    output_weight,
    mixer_norm_gain,
    up_weight,
    down_weight,
):
    query_heads, final_state, output_rows = within_block_pass(
        queries, keys, values, input_gate_log, forget_gate_logits, extra_decay_log, document
    )
    numerator, denominator, peak_log, cumulative = output_rows
    memory, normer, stabil, last_doc = final_state
    step_logs = cumulative[:, :, -1]
    offsets = jnp.cumsum(step_logs, axis=0) - step_logs
    through = cumulative + offsets[:, :, None]
    summary = (memory, normer, stabil, jnp.sum(step_logs, axis=0), document[0], last_doc)
    identity = (
        jnp.zeros_like(memory),
        jnp.zeros_like(normer),
        jnp.full_like(stabil, NEG),
        jnp.zeros_like(stabil),
        jnp.array(-1, jnp.int32),
        jnp.array(-1, jnp.int32),
    )
    prefix = carried_in(summary, "sp", join_states, identity)
    doc_blocks = document.reshape(-1, BLOCK)
    carried_log = jnp.where(
        (doc_blocks == prefix[5])[:, None, :], through + prefix[2][None, :, None], NEG
    )
    merged_peak = jnp.maximum(peak_log, carried_log)
    own_weight = jnp.exp(peak_log - merged_peak)
    far_weight = jnp.exp(carried_log - merged_peak)
    numerator = own_weight[..., None] * numerator + far_weight[..., None] * jnp.einsum(
        "nhtd,hde->nhte", query_heads, prefix[0], precision=HIGH
    )
    denominator = own_weight * denominator + far_weight * jnp.einsum(
        "nhtd,hd->nht", query_heads, prefix[1], precision=HIGH
    )
    cell_out = numerator / jnp.maximum(jnp.abs(denominator), 1.0)[..., None]
    mixed = head_mix(cell_out, output_gate_logits, cell_norm_gain)
    head_terms = jnp.dot(mixed, output_weight, preferred_element_type=jnp.float32)
    width = residual.shape[1]
    model_width = width * lax.axis_size("tp")
    own_sum = lax.psum_scatter(
        head_terms.astype(jnp.bfloat16), "tp", scatter_dimension=1, tiled=True
    ).astype(jnp.float32)
    first_sum = (residual.astype(jnp.float32) + own_sum).astype(jnp.bfloat16)
    first_wide = lax.optimization_barrier(first_sum).astype(jnp.float32)
    squares = lax.psum(jnp.sum(first_wide * first_wide, axis=1), "tp")
    inverse = lax.rsqrt(squares / model_width + EPS)
    normed_own = (first_wide * inverse[:, None] * mixer_norm_gain.astype(jnp.float32)).astype(
        jnp.bfloat16
    )
    normed_full = lax.all_gather(normed_own, "tp", axis=1, tiled=True)
    hidden = jnp.dot(
        normed_full,
        lax.all_gather(up_weight, "sp", axis=0, tiled=True),
        preferred_element_type=jnp.float32,
    )
    squared = jnp.square(jax.nn.relu(hidden)).astype(jnp.bfloat16)
    channel = jnp.dot(
        squared,
        lax.all_gather(down_weight, "sp", axis=1, tiled=True),
        preferred_element_type=jnp.float32,
    )
    own_channel = lax.psum_scatter(
        channel.astype(jnp.bfloat16), "tp", scatter_dimension=1, tiled=True
    ).astype(jnp.float32)
    return (lax.optimization_barrier(first_sum).astype(jnp.float32) + own_channel).astype(
        jnp.bfloat16
    )


MESH = pl.DeviceIdType.MESH
F32 = jnp.float32
BF16 = jnp.bfloat16
CHUNKS = 2


def to_columns(rows):
    pad = jnp.zeros((128 - rows.shape[0], rows.shape[1]), F32)
    return jnp.transpose(jnp.concatenate([rows, pad], axis=0))


def to_rows(column):
    return jnp.transpose(jnp.broadcast_to(column, (column.shape[0], 128)))[0:8, :]


def halves(wide):
    high = wide.astype(BF16)
    return high, (wide - high.astype(F32)).astype(BF16)


def two_pass(wide, narrow):
    high, low = halves(wide)
    return jnp.dot(high, narrow, preferred_element_type=F32) + jnp.dot(
        low, narrow, preferred_element_type=F32
    )


def layer_kernel(
    n,
    m,
    back,
    q_ref,
    k_ref,
    v_ref,
    og_ref,
    forget_ref,
    extra_ref,
    input_ref,
    doc_ref,
    resid_ref,
    cell_gain_ref,
    mixer_gain_ref,
    wout_ref,
    up_ref,
    down_ref,
    out_ref,
    up_all,
    down_all,
    wcols,
    state_out,
    near_state,
    pair_state,
    state_in,
    tail_out,
    near_tail,
    pair_tail,
    tail_in,
    numer_ref,
    y_all,
    squares_out,
    squares_in,
    first_ref,
    normed,
    sums_out,
    sums_in,
    squared,
    parts,
    sib_in,
    comb,
    x_in,
    last_out,
    last_in,
    w_send,
    w_recv,
    z_send,
    z_recv,
    relay_send,
    y_send,
    y_recv,
    near_send,
    near_recv,
    state_send,
    state_recv,
    mix_send,
    mix_recv,
    squares_send,
    squares_recv,
    normed_send,
    normed_recv,
    sums_send,
    sums_recv,
    sib_send,
    sib_recv,
    x_send,
    x_recv,
    last_send,
    last_recv,
):
    sp, tp = lax.axis_index("sp"), lax.axis_index("tp")
    rows, heads = q_ref.shape[0], q_ref.shape[1] // DH
    depth, hidden_width = up_ref.shape
    own_width = hidden_width // 2
    width = resid_ref.shape[1]
    up_piece, down_piece = depth // CHUNKS, depth // CHUNKS
    z, y, lines = sp // 2, sp % 2, n // 2
    p, x, c = z % 2, tp // 2, tp % 2

    def z_at(j):
        return (z, z + 1 - 2 * p, z + 2 - 4 * (z // 2), n // 2 - 1 - z)[j]

    def tp_at(bits):
        far_c = c + (bits % 2) * (1 - 2 * c)
        far_x = x + ((bits // 2) % 2) * (1 - 2 * x)
        return 2 * far_x + far_c

    partner = 2 * z_at(1) + y
    beside = 2 * z + 1 - y

    barrier = pltpu.get_barrier_semaphore()
    for k in range(1, n):
        pl.semaphore_signal(barrier, device_id=((sp + k) % n, tp), device_id_type=MESH)
    for k in range(1, m):
        pl.semaphore_signal(barrier, device_id=(sp, (tp + k) % m), device_id_type=MESH)
    pl.semaphore_wait(barrier, n + m - 2)

    def remote(src, dst, send_sem, recv_sem, device):
        return pltpu.make_async_remote_copy(
            src_ref=src,
            dst_ref=dst,
            send_sem=send_sem,
            recv_sem=recv_sem,
            device_id=device,
            device_id_type=MESH,
        )

    def cols_of(owner):
        return pl.ds(pl.multiple_of(owner * width, width), width)

    def w_copy(k):
        return remote(
            wout_ref.at[:, cols_of(tp_at(k))],
            wcols.at[tp],
            w_send.at[k - 1],
            w_recv.at[k - 1],
            (sp, tp_at(k)),
        )

    def w_arrival(k):
        there = wcols.at[tp_at(k)]
        return remote(there, there, w_send.at[k - 1], w_recv.at[k - 1], (sp, tp_at(k)))

    def slot(stream, block, piece):
        if stream == 0:
            start = pl.multiple_of(block * depth + piece * up_piece, up_piece)
            return up_all.at[pl.ds(start, up_piece), :]
        return down_all.at[block, piece]

    def own_piece(stream, half, piece):
        if stream == 0:
            lanes = pl.ds(pl.multiple_of(half * own_width, own_width), own_width)
            return up_ref.at[pl.ds(piece * up_piece, up_piece), lanes]
        deep = pl.ds(pl.multiple_of(half * own_width, own_width), own_width)
        return down_ref.at[deep, pl.ds(piece * down_piece, down_piece)]

    def z_copy(stream, j, piece):
        return remote(
            own_piece(stream, z_at(j) % 2, piece),
            slot(stream, sp, piece),
            z_send.at[stream, j - 1, piece],
            z_recv.at[stream, j - 1, piece],
            (2 * z_at(j) + y, tp),
        )

    inner = p + z // 2 == 1

    def z_forward(stream, piece):
        there = slot(stream, 2 * z_at(1) + y, piece)
        return remote(
            there,
            there,
            relay_send.at[stream, piece],
            z_recv.at[stream, 2, piece],
            (2 * z_at(2) + y, tp),
        )

    def z_arrival(stream, j, piece):
        there = slot(stream, 2 * z_at(j) + y, piece)
        return remote(
            there,
            there,
            z_send.at[stream, j - 1, piece],
            z_recv.at[stream, j - 1, piece],
            (2 * z_at(j) + y, tp),
        )

    def y_copy(stream, i, piece):
        there = slot(stream, 2 * z_at(i) + y, piece)
        return remote(
            own_piece(stream, p, piece) if i == 0 else there,
            there,
            y_send.at[stream, i, piece],
            y_recv.at[stream, i, piece],
            (beside, tp),
        )

    def y_arrival(stream, i, piece):
        there = slot(stream, 2 * z_at(i) + 1 - y, piece)
        return remote(
            there,
            there,
            y_send.at[stream, i, piece],
            y_recv.at[stream, i, piece],
            (beside, tp),
        )

    order = ((1, 0), (1, 1), (2, 0), (3, 0), (2, 1), (3, 1))
    events = [(stream, j, piece) for stream in range(2) for j, piece in order]
    done = [0]

    def pump(until):
        while done[0] < until:
            event = done[0]
            stream, j, piece = events[event]
            done[0] += 1
            z_arrival(stream, j, piece).wait_recv()
            y_copy(stream, j, piece).start()
            if j == 1:

                @pl.when(inner)
                def _():
                    z_forward(stream, piece).start()

    ups = len(order)

    for k in range(1, m):
        w_copy(k).start()

    document = doc_ref[...].astype(F32)
    across = lax.broadcasted_iota(jnp.int32, (rows, rows), 1)
    along = lax.broadcasted_iota(jnp.int32, (rows, rows), 0)
    upper = (along <= across).astype(BF16)
    forget = jax.nn.log_sigmoid(forget_ref[...]) + extra_ref[...]
    high = forget.astype(BF16).astype(F32)
    middle = (forget - high).astype(BF16).astype(F32)
    low = forget - high - middle
    slab = lax.broadcasted_iota(jnp.int32, (8, rows), 0)
    split = jnp.zeros((8, rows), F32)
    for h in range(heads):
        for i, part in enumerate((high, middle, low)):
            split = jnp.where(slab == heads * i + h, part[h : h + 1, :], split)
    summed = jnp.dot(split.astype(BF16), upper, preferred_element_type=F32)
    last_doc = document[:, rows - 1 : rows]
    sums, entry, totals, stabs, scaled = [], [], [], [], []
    for h in range(heads):
        line_sum = summed[h : h + 1, :]
        for i in range(1, 3):
            line_sum = line_sum + summed[heads * i + h : heads * i + h + 1, :]
        sums.append(line_sum)
        entry.append(input_ref[h : h + 1, :] - line_sum)
        total = line_sum[:, rows - 1 : rows]
        keep = jnp.where(document == last_doc, total + entry[h], NEG)
        stab = jnp.max(keep, axis=1, keepdims=True)
        totals.append(total)
        stabs.append(stab)
        scaled.append(jnp.exp(keep - stab))
    packed = jnp.broadcast_to(document, (8, rows))
    for h in range(heads):
        packed = jnp.where(slab == h, sums[h], packed)
        packed = jnp.where(slab == heads + h, scaled[h], packed)
    columns = to_columns(packed)
    doc_col = columns[:, 2 * heads : 2 * heads + 1]
    line = lax.broadcasted_iota(jnp.int32, (8, DH), 0)
    for h in range(heads):
        mine = slice(h * DH, (h + 1) * DH)
        weighted = k_ref[:, mine].astype(F32) * columns[:, heads + h : heads + h + 1]
        state_out[h] = lax.dot_general(
            weighted.astype(BF16),
            v_ref[:, mine],
            (((0,), (0,)), ((), ())),
            preferred_element_type=F32,
        ).astype(BF16)
        tail = jnp.broadcast_to(jnp.sum(weighted, axis=0, keepdims=True), (8, DH))
        tail = jnp.where(line == 1, stabs[h], tail)
        tail = jnp.where(line == 2, totals[h], tail)
        tail = jnp.where(line == 3, last_doc, tail)
        tail_out[h] = tail

    def pair_of(refs, send_sem, recv_sem, device):
        return [
            remote(src, dst, send_sem.at[i], recv_sem.at[i], device)
            for i, (src, dst) in enumerate(refs)
        ]

    def near_copies():
        refs = ((tail_out, near_tail), (state_out, near_state))
        return pair_of(refs, near_send, near_recv, (beside, tp))

    def state_copies(k):
        refs = ((pair_tail, tail_in.at[k - 1]), (pair_state, state_in.at[k - 1]))
        return pair_of(
            refs, state_send.at[k - 1], state_recv.at[k - 1], (2 * ((z + k) % lines) + y, tp)
        )

    for copy in near_copies():
        copy.start()
    z_copy(0, 1, 0).start()

    @pl.when(inner)
    def _():
        z_copy(0, 3, 0).start()

    for piece in range(CHUNKS):
        y_copy(0, 0, piece).start()

    for k in range(1, back + 1):

        @pl.when(z < k)
        def _():
            tail_in[k - 1] = jnp.zeros((heads, 8, DH), F32)
            state_in[k - 1] = jnp.zeros((heads, DH, DH), BF16)

    half_lanes = pl.ds(pl.multiple_of(p * own_width, own_width), own_width)
    up_all[pl.ds(pl.multiple_of(sp * depth, depth), depth), :] = up_ref[:, half_lanes]
    for piece in range(CHUNKS):
        cols = slice(piece * down_piece, (piece + 1) * down_piece)
        down_all[sp, piece] = down_ref[half_lanes, cols]

    step = min(rows, 256)
    locals_of = []
    for h in range(heads):
        mine = slice(h * DH, (h + 1) * DH)
        peaks, denoms = [], []
        for start in range(0, rows, step):
            stop = start + step
            here = slice(start, stop)
            scores = lax.dot_general(
                q_ref[here, mine],
                k_ref[0:stop, mine],
                (((1,), (1,)), ((), ())),
                preferred_element_type=F32,
            ) * (DH**-0.5)
            pair = columns[here, h : h + 1] + entry[h][:, 0:stop]
            seen = (doc_col[here] == document[:, 0:stop]) & (
                along[here, 0:stop] >= across[here, 0:stop]
            )
            pair = jnp.where(seen, pair, NEG)
            peak = jnp.max(pair, axis=1, keepdims=True)
            scores = scores * jnp.exp(pair - peak)
            numer_ref[h, here, :] = two_pass(scores, v_ref[0:stop, mine])
            peaks.append(peak)
            denoms.append(jnp.sum(scores, axis=1, keepdims=True))
        locals_of.append((jnp.concatenate(peaks, axis=0), jnp.concatenate(denoms, axis=0)))

    for copy in near_copies():
        copy.wait_recv()
    for h in range(heads):
        own_tail, far_tail = tail_out[h], near_tail[h]
        old_tail = jnp.where(y == 0, own_tail, far_tail)
        new_tail = jnp.where(y == 0, far_tail, own_tail)
        own_state, far_state = state_out[h].astype(F32), near_state[h].astype(F32)
        old_state = jnp.where(y == 0, own_state, far_state)
        new_state = jnp.where(y == 0, far_state, own_state)
        joined = old_tail[3:4, :] == new_tail[3:4, :]
        old_log = jnp.where(joined, old_tail[1:2, :] + new_tail[2:3, :], NEG)
        stab = jnp.maximum(old_log, new_tail[1:2, :])
        old_weight = jnp.where(joined, jnp.exp(old_log - stab), 0.0)
        new_weight = jnp.exp(new_tail[1:2, :] - stab)
        pair_state[h] = (
            jnp.where(joined, old_weight * old_state, 0.0) + new_weight * new_state
        ).astype(BF16)
        tail = jnp.where(joined, old_weight * old_tail, 0.0) + new_weight * new_tail
        tail = jnp.where(line == 1, stab, tail)
        tail = jnp.where(line == 2, old_tail + new_tail, tail)
        pair_tail[h] = jnp.where(line == 3, new_tail, tail)

    for k in range(1, back + 1):

        @pl.when(z + k < lines)
        def _():
            for copy in state_copies(k):
                copy.start()

    z_copy(0, 1, 1).start()
    z_copy(0, 2, 0).start()
    for k in range(1, back + 1):

        @pl.when(z >= k)
        def _():
            for copy in state_copies(k):
                copy.wait_recv()

    def mix_copy(k, h):
        here = y_all.at[tp, :, pl.ds(h * DH, DH)]
        return remote(
            here, here, mix_send.at[k - 1, h], mix_recv.at[k - 1, h], (sp, tp_at(k))
        )

    def mix_forward(h):
        there = y_all.at[tp_at(2), :, pl.ds(h * DH, DH)]
        return remote(there, there, mix_send.at[2, h], mix_recv.at[2, h], (sp, tp_at(1)))

    def mix_arrival(k, h):
        there = y_all.at[tp_at(k), :, pl.ds(h * DH, DH)]
        return remote(
            there, there, mix_send.at[k - 1, h], mix_recv.at[k - 1, h], (sp, tp_at(k))
        )

    first_doc = document[:, 0:1]
    square_sum = jnp.zeros((rows, DH), F32)
    for h in range(heads):
        mine = slice(h * DH, (h + 1) * DH)
        earlier = [(near_tail, near_state, y == 1)]
        earlier += [(tail_in.at[k], state_in.at[k], z > k) for k in range(back)]
        between = jnp.zeros((1, DH), F32)
        logs, valids = [], []
        best = jnp.full((1, DH), NEG, F32)
        for tails, _, exists in earlier:
            tail = tails[h]
            valid = (tail[3:4, :] == first_doc) & jnp.broadcast_to(exists, (1, DH))
            log = jnp.where(valid, between + tail[1:2, :], NEG)
            between = between + jnp.where(exists, tail[2:3, :], 0.0)
            best = jnp.maximum(best, log)
            logs.append(log)
            valids.append(valid)
        memory = jnp.zeros((DH, DH), F32)
        normer = jnp.zeros((1, DH), F32)
        for i, (tails, states, _) in enumerate(earlier):
            weight = jnp.where(valids[i], jnp.exp(logs[i] - best), 0.0)
            memory = memory + jnp.where(valids[i], weight * states[h].astype(F32), 0.0)
            normer = normer + jnp.where(valids[i], weight * tails[h, 0:1, :], 0.0)
        peak, denom = locals_of[h]
        carried = jnp.where(doc_col == first_doc, columns[:, h : h + 1] + best[:, 0:1], NEG)
        merged = jnp.maximum(peak, carried)
        own = jnp.exp(peak - merged)
        other = jnp.exp(carried - merged) * (DH**-0.5)
        query = q_ref[:, mine]
        high, low = halves(memory)
        reached = jnp.dot(query, high, preferred_element_type=F32) + jnp.dot(
            query, low, preferred_element_type=F32
        )
        numer = own * numer_ref[h] + other * reached
        denom = own * denom + other * jnp.sum(
            query.astype(F32) * normer, axis=1, keepdims=True
        )
        cell = numer / jnp.maximum(jnp.abs(denom), 1.0)
        square_sum = square_sum + cell * cell
        gated = jax.nn.sigmoid(og_ref[:, mine].astype(F32))
        y_all[tp, :, mine] = (gated * cell * cell_gain_ref[:, mine].astype(F32)).astype(BF16)
        for k in range(1, 3):
            mix_copy(k, h).start()
    squares_out[...] = to_rows(jnp.sum(square_sum, axis=1, keepdims=True))

    def square_copy(k):
        return remote(
            squares_out,
            squares_in.at[k - 1],
            squares_send.at[k - 1],
            squares_recv.at[k - 1],
            (sp, tp_at(k)),
        )

    for k in range(1, m):
        square_copy(k).start()
    here = cols_of(tp)
    attn = jnp.dot(y_all[tp], wout_ref[:, here], preferred_element_type=F32)
    pump(PUMPS[0])

    @pl.when(inner)
    def _():
        for j in (2, 3):
            z_copy(0, j, 1).start()

    for h in range(heads):
        mix_arrival(2, h).wait_recv()
        mix_forward(h).start()
    pump(PUMPS[1])
    for k in (1, 2, 3):
        w_arrival(k).wait_recv()
        if k != 2:
            for h in range(heads):
                mix_arrival(k, h).wait_recv()
        attn = attn + jnp.dot(
            y_all[tp_at(k)], wcols[tp_at(k)], preferred_element_type=F32
        )
    squares = squares_out[...]
    for k in range(1, m):
        square_copy(k).wait_recv()
        squares = squares + squares_in[k - 1]
    inverse = lax.rsqrt(to_columns(squares)[:, 0:1] / (heads * DH * m) + EPS)
    first = (resid_ref[...].astype(F32) + attn * inverse).astype(BF16)
    first_ref[...] = first
    first = first.astype(F32)

    def plane(bit):
        return p + bit * (1 - 2 * p)

    def rows_of(bit):
        return pl.ds(pl.multiple_of(plane(bit) * rows, rows), rows)

    normed[rows_of(0), here] = (first * mixer_gain_ref[...].astype(F32)).astype(BF16)

    def group_at(bits):
        return (sp + (bits // 4) * (partner - sp), tp_at(bits % 4))

    def normed_block(bits):
        return normed.at[rows_of(bits // 4), cols_of(tp_at(bits % 4))]

    def normed_copy(source, flip):
        block = normed_block(source)
        rel = source + flip - 1
        return remote(block, block, normed_send.at[rel], normed_recv.at[rel], group_at(flip))

    def normed_arrival(rel):
        block = normed_block(rel)
        return remote(
            block, block, normed_send.at[rel - 1], normed_recv.at[rel - 1], group_at(rel % 2 or rel)
        )

    routes = ((0, 2), (0, 4), (0, 1), (2, 1), (4, 2), (4, 1), (6, 1))
    sums_out[0] = to_rows(jnp.sum(first * first, axis=1, keepdims=True))

    def sums_copy(k):
        return remote(
            sums_out.at[k // 4],
            sums_in.at[k - 1],
            sums_send.at[k - 1],
            sums_recv.at[k - 1],
            group_at(k),
        )

    for k in range(1, m):
        sums_copy(k).start()
    for route in routes[:3]:
        normed_copy(*route).start()
    total = sums_out[0]
    for k in range(1, m):
        sums_copy(k).wait_recv()
        total = total + sums_in[k - 1]
    sums_out[1] = total
    sums_copy(4).start()

    @pl.when(jnp.logical_not(inner))
    def _():
        z_copy(0, 2, 1).start()

    y_copy(1, 0, 0).start()
    pump(PUMPS[2])
    y_copy(1, 0, 1).start()
    normed_arrival(2).wait_recv()
    normed_copy(2, 1).start()
    normed_arrival(4).wait_recv()
    normed_copy(4, 2).start()
    normed_copy(4, 1).start()
    normed_arrival(1).wait_recv()
    normed_arrival(3).wait_recv()
    pump(ups - 1)

    @pl.when(inner)
    def _():
        for j in (2, 3):
            z_copy(1, j, 0).start()

    pump(ups)

    z_copy(1, 1, 0).start()

    @pl.when(jnp.logical_not(inner))
    def _():
        z_copy(1, 2, 0).start()

    z_copy(1, 1, 1).start()

    @pl.when(jnp.logical_not(inner))
    def _():
        z_copy(1, 2, 1).start()

    for i in range(n // 2):
        for piece in range(CHUNKS):
            y_arrival(0, i, piece).wait_recv()

    tile = min(own_width, 256)

    def up_half(bit, line_sums):
        scale = lax.rsqrt(to_columns(line_sums)[:, 0:1] / (width * m) + EPS)

        def up_tile(t, carry):
            cols = pl.ds(pl.multiple_of(t * tile, tile), tile)
            raw = jnp.dot(normed[rows_of(bit), :], up_all[:, cols], preferred_element_type=F32)
            hidden = jnp.maximum(raw * scale, 0.0)
            squared[rows_of(bit), cols] = (hidden * hidden).astype(BF16)
            return carry

        lax.fori_loop(0, own_width // tile, up_tile, 0)

    up_half(0, total)
    pump(ups + 1)

    @pl.when(inner)
    def _():
        for j in (2, 3):
            z_copy(1, j, 1).start()

    normed_arrival(6).wait_recv()
    normed_copy(6, 1).start()
    normed_arrival(5).wait_recv()
    normed_arrival(7).wait_recv()
    sums_copy(4).wait_recv()
    up_half(1, sums_in[3])
    pump(ups + PUMPS[3])

    pairs = [(0, piece) for piece in range(CHUNKS)] + list(order)
    units = [(j, side, piece) for j, piece in pairs for side in range(2)]

    def place(i):
        j, side, piece = units[i]
        owner = z_at(j)
        return owner, owner // 2, y + side * (1 - 2 * y), piece

    def sib_copy(i):
        _, far_x, half, piece = place(i)
        return remote(
            parts.at[i],
            sib_in.at[far_x, half, piece],
            sib_send.at[far_x, half, piece],
            sib_recv.at[far_x, half, piece],
            (sp, tp_at(1)),
        )

    def x_copy(i):
        _, far_x, half, piece = place(i)
        return remote(
            comb.at[far_x, half, piece],
            x_in.at[half, piece],
            x_send.at[half, piece],
            x_recv.at[half, piece],
            (sp, tp_at(2)),
        )

    def last_copy(i):
        _, far_x, half, piece = place(i)
        return remote(
            last_out.at[half, piece],
            last_in.at[half, piece],
            last_send.at[half, piece],
            last_recv.at[half, piece],
            (partner, tp),
        )

    def down_unit(i):
        owner, _, half, piece = place(i)
        block = 2 * owner + half
        for bit in range(2):
            there = slice(bit * rows, (bit + 1) * rows)
            parts[i, there, :] = jnp.dot(
                squared[there, :], down_all[block, piece], preferred_element_type=F32
            ).astype(BF16)

        @pl.when(owner % 2 != c)
        def _():
            sib_copy(i).start()

    def combine(i):
        owner, far_x, half, piece = place(i)

        @pl.when(owner % 2 == c)
        def _():
            sib_copy(i).wait_recv()
            comb[far_x, half, piece] = (
                parts[i].astype(F32) + sib_in[far_x, half, piece].astype(F32)
            ).astype(BF16)

            @pl.when(far_x != x)
            def _():
                x_copy(i).start()

    def settle(i):
        owner, far_x, half, piece = place(i)

        @pl.when(owner == tp)
        def _():
            x_copy(i).wait_recv()
            last_out[half, piece] = (
                comb[far_x, half, piece, rows_of(1), :].astype(F32)
                + x_in[half, piece, rows_of(1), :].astype(F32)
            ).astype(BF16)
            last_copy(i).start()

    for i, (j, side, piece) in enumerate(units):
        if side == 0:
            pump(min(len(events), ups + max(0, i // 2 + 1 - CHUNKS + LEAD)))
        else:
            y_arrival(1, j, piece).wait_recv()
        down_unit(i)
        if i > 0:
            combine(i - 1)
        if i >= SETTLE:
            settle(i - SETTLE)
    combine(len(units) - 1)
    for i in range(len(units) - SETTLE, len(units)):
        settle(i)

    for half in range(2):
        for piece in range(CHUNKS):
            start = half * depth + piece * down_piece
            cols = slice(start, start + down_piece)
            total = first_ref[:, cols].astype(F32)
            total = total + comb[x, half, piece, rows_of(0), :].astype(F32)
            total = total + x_in[half, piece, rows_of(0), :].astype(F32)
            there = last_in.at[half, piece]
            remote(
                there, there, last_send.at[half, piece], last_recv.at[half, piece], (partner, tp)
            ).wait_recv()
            total = total + last_in[half, piece].astype(F32)
            out_ref[:, cols] = total.astype(BF16)

    for k in range(1, m):
        w_copy(k).wait_send()
        square_copy(k).wait_send()
        for h in range(heads):
            (mix_copy(k, h) if k < 3 else mix_forward(h)).wait_send()
    for k in range(1, m + 1):
        sums_copy(k).wait_send()
    for route in routes:
        normed_copy(*route).wait_send()
    for stream in range(2):
        for piece in range(CHUNKS):
            for j in range(1, 3):
                z_copy(stream, j, piece).wait_send()

            @pl.when(inner)
            def _():
                z_copy(stream, 3, piece).wait_send()
                z_forward(stream, piece).wait_send()

            for i in range(n // 2):
                y_copy(stream, i, piece).wait_send()
    for copy in near_copies():
        copy.wait_send()
    for k in range(1, back + 1):

        @pl.when(z + k < lines)
        def _():
            for copy in state_copies(k):
                copy.wait_send()

    for i in range(len(units)):
        owner = place(i)[0]

        @pl.when(owner % 2 != c)
        def _():
            sib_copy(i).wait_send()

        @pl.when(owner % 2 == c)
        def _():

            @pl.when(place(i)[1] != x)
            def _():
                x_copy(i).wait_send()

        @pl.when(owner == tp)
        def _():
            last_copy(i).wait_send()


PUMPS = (1, 2, 4, 2, 3)
LEAD = 1
SETTLE = 8


def fused(
    n,
    m,
    queries,
    keys,
    values,
    output_gate_logits,
    input_gate_log,
    forget_gate_logits,
    extra_decay_log,
    document,
    residual,
    cell_norm_gain,
    output_weight,
    mixer_norm_gain,
    up_weight,
    down_weight,
):
    rows, heads = queries.shape[0], queries.shape[1] // DH
    depth, hidden_width = up_weight.shape
    width = residual.shape[1]
    own_width = hidden_width // 2
    lines = n // 2
    back = min(lines - 1, ((MOST - 2) // rows + 2) // 2)
    dma = pltpu.SemaphoreType.DMA
    return pl.pallas_call(
        functools.partial(layer_kernel, n, m, back),
        out_shape=jax.ShapeDtypeStruct((rows, width), BF16),
        in_specs=[pl.BlockSpec(memory_space=pltpu.VMEM)] * 14,
        out_specs=pl.BlockSpec(memory_space=pltpu.VMEM),
        scratch_shapes=[
            pltpu.VMEM((n * depth, own_width), BF16),
            pltpu.VMEM((n, CHUNKS, own_width, depth // CHUNKS), BF16),
            pltpu.VMEM((m, heads * DH, width), BF16),
            pltpu.VMEM((heads, DH, DH), BF16),
            pltpu.VMEM((heads, DH, DH), BF16),
            pltpu.VMEM((heads, DH, DH), BF16),
            pltpu.VMEM((back, heads, DH, DH), BF16),
            pltpu.VMEM((heads, 8, DH), F32),
            pltpu.VMEM((heads, 8, DH), F32),
            pltpu.VMEM((heads, 8, DH), F32),
            pltpu.VMEM((back, heads, 8, DH), F32),
            pltpu.VMEM((heads, rows, DH), F32),
            pltpu.VMEM((m, rows, heads * DH), BF16),
            pltpu.VMEM((8, rows), F32),
            pltpu.VMEM((m - 1, 8, rows), F32),
            pltpu.VMEM((rows, width), BF16),
            pltpu.VMEM((2 * rows, m * width), BF16),
            pltpu.VMEM((2, 8, rows), F32),
            pltpu.VMEM((m, 8, rows), F32),
            pltpu.VMEM((2 * rows, own_width), BF16),
            pltpu.VMEM((n * CHUNKS, 2 * rows, depth // CHUNKS), BF16),
            pltpu.VMEM((2, 2, CHUNKS, 2 * rows, depth // CHUNKS), BF16),
            pltpu.VMEM((2, 2, CHUNKS, 2 * rows, depth // CHUNKS), BF16),
            pltpu.VMEM((2, CHUNKS, 2 * rows, depth // CHUNKS), BF16),
            pltpu.VMEM((2, CHUNKS, rows, depth // CHUNKS), BF16),
            pltpu.VMEM((2, CHUNKS, rows, depth // CHUNKS), BF16),
            dma((m - 1,)),
            dma((m - 1,)),
            dma((2, lines - 1, CHUNKS)),
            dma((2, lines - 1, CHUNKS)),
            dma((2, CHUNKS)),
            dma((2, lines, CHUNKS)),
            dma((2, lines, CHUNKS)),
            dma((2,)),
            dma((2,)),
            dma((back, 2)),
            dma((back, 2)),
            dma((m - 1, heads)),
            dma((m - 1, heads)),
            dma((m - 1,)),
            dma((m - 1,)),
            dma((2 * m - 1,)),
            dma((2 * m - 1,)),
            dma((m,)),
            dma((m,)),
            dma((2, 2, CHUNKS)),
            dma((2, 2, CHUNKS)),
            dma((2, CHUNKS)),
            dma((2, CHUNKS)),
            dma((2, CHUNKS)),
            dma((2, CHUNKS)),
        ],
        compiler_params=pltpu.CompilerParams(
            collective_id=0, has_side_effects=True, vmem_limit_bytes=60 * 1024 * 1024
        ),
        name="layer",
    )(
        queries,
        keys,
        values,
        output_gate_logits,
        forget_gate_logits.T,
        extra_decay_log.T,
        input_gate_log.T,
        document[None, :],
        residual,
        cell_norm_gain[None, :],
        mixer_norm_gain[None, :],
        output_weight,
        up_weight,
        down_weight,
    )


def either(n, m, *args):
    depth, hidden_width = args[12].shape
    heads = args[0].shape[1] // DH
    fits = n == 8 and m == 4 and depth % 128 == 0 and hidden_width % 512 == 0
    fits = fits and 3 * heads <= 8 and args[8].shape[1] == 2 * depth
    fits = fits and args[0].shape[0] % 256 == 0
    if fits:
        return fused(n, m, *args)
    return local(*args)


def solution(mesh):
    in_specs = (
        P("sp", "tp"),
        P("sp", "tp"),
        P("sp", "tp"),
        P("sp", "tp"),
        P("sp", "tp"),
        P("sp", "tp"),
        P("sp", "tp"),
        P("sp"),
        P("sp", "tp"),
        P("tp"),
        P("tp", None),
        P("tp"),
        P("sp", "tp"),
        P("tp", "sp"),
    )
    out_specs = P("sp", "tp")
    body = functools.partial(either, mesh.shape["sp"], mesh.shape["tp"])
    return jax.shard_map(body, mesh=mesh, in_specs=in_specs, out_specs=out_specs, check_vma=False)
```

```python
import functools

import jax
import jax.numpy as jnp
from jax import lax
from jax.experimental import pallas as pl
from jax.experimental.pallas import tpu as pltpu
from jax.sharding import PartitionSpec as P

DH = 128
BLOCK = 128
MOST = 2048


NEG = -1e30
EPS = 1e-06
HIGH = lax.Precision.HIGHEST


def carried_in(value, axis, join, neutral):
    count, mine = (lax.axis_size(axis), lax.axis_index(axis))
    pieces = jax.tree.map(lambda part: lax.all_gather(part, axis), value)
    subtotal = jax.tree.map(
        lambda part, zero: jnp.full_like(part, 0) + jnp.asarray(zero, part.dtype), value, neutral
    )

    def step(position, subtotal):
        longer = join(subtotal, jax.tree.map(lambda part: part[position], pieces))
        return jax.tree.map(lambda new, old: jnp.where(position < mine, new, old), longer, subtotal)

    return lax.fori_loop(0, count - 1, step, subtotal)


def block_terms(carry, inputs):
    memory, normer, stabil, last_doc = carry
    q_blk, k_blk, v_blk, gate_in, gate_log, doc_blk = inputs
    length = doc_blk.shape[0]
    causal = jnp.arange(length)[:, None] >= jnp.arange(length)[None, :]
    cumulative = jnp.cumsum(gate_log, axis=-1)
    same_doc = (doc_blk[:, None] == doc_blk[None, :]) & causal
    pair_log = cumulative[:, :, None] - cumulative[:, None, :] + gate_in[:, None, :]
    pair_log = jnp.where(same_doc[None], pair_log, NEG)
    live_rows = doc_blk == last_doc
    carried_log = jnp.where(live_rows[None, :], cumulative + stabil[:, None], NEG)
    peak_log = jnp.maximum(carried_log, jnp.max(pair_log, axis=-1))
    weights = jnp.exp(pair_log - peak_log[:, :, None])
    carried = jnp.exp(carried_log - peak_log)
    scores = jnp.einsum("htd,hsd->hts", q_blk, k_blk, precision=HIGH) * weights
    numerator = carried[:, :, None] * jnp.einsum("htd,hde->hte", q_blk, memory, precision=HIGH)
    numerator = numerator + jnp.einsum("hts,hse->hte", scores, v_blk, precision=HIGH)
    denominator = carried * jnp.einsum("htd,hd->ht", q_blk, normer, precision=HIGH) + jnp.sum(
        scores, axis=-1
    )
    end_doc = doc_blk[-1]
    end_cum = cumulative[:, -1]
    keep_log = jnp.where(
        (doc_blk == end_doc)[None, :], end_cum[:, None] - cumulative + gate_in, NEG
    )
    old_log = jnp.where(last_doc == end_doc, end_cum + stabil, NEG)
    new_stab = jnp.maximum(old_log, jnp.max(keep_log, axis=-1))
    scaled = jnp.exp(keep_log - new_stab[:, None])
    decayed = jnp.exp(old_log - new_stab)
    memory = decayed[:, None, None] * memory + jnp.einsum(
        "hs,hsd,hse->hde", scaled, k_blk, v_blk, precision=HIGH
    )
    normer = decayed[:, None] * normer + jnp.einsum("hs,hsd->hd", scaled, k_blk, precision=HIGH)
    return ((memory, normer, new_stab, end_doc), (numerator, denominator, peak_log, cumulative))


def split_heads(source, blocks):
    return source.astype(jnp.float32).reshape(blocks, BLOCK, -1, DH).transpose(0, 2, 1, 3)


def split_gates(source, blocks):
    return source.reshape(blocks, BLOCK, -1).transpose(0, 2, 1)


def within_block_pass(
    queries, keys, values, input_gate_log, forget_gate_logits, extra_decay_log, document
):
    blocks = queries.shape[0] // BLOCK
    head_count = queries.shape[1] // DH
    query_heads = split_heads(queries, blocks) * DH ** (-0.5)
    forget_log_values = jax.nn.log_sigmoid(forget_gate_logits) + extra_decay_log
    inputs = (
        query_heads,
        split_heads(keys, blocks),
        split_heads(values, blocks),
        split_gates(input_gate_log, blocks),
        split_gates(forget_log_values, blocks),
        document.reshape(blocks, BLOCK),
    )
    initial = (
        jnp.zeros((head_count, DH, DH), jnp.float32),
        jnp.zeros((head_count, DH), jnp.float32),
        jnp.full((head_count,), NEG, jnp.float32),
        jnp.array(-1, jnp.int32),
    )
    final_state, output_rows = lax.scan(block_terms, initial, inputs)
    return (query_heads, final_state, output_rows)


def head_mix(cell_out, output_gate_logits, cell_norm_gain):
    row_count = output_gate_logits.shape[0]
    head_count = cell_out.shape[1]
    hidden = cell_out.transpose(0, 2, 1, 3).reshape(row_count, head_count * DH)
    squares = lax.psum(jnp.sum(hidden * hidden, axis=1), "tp")
    inverse = lax.rsqrt(squares / (head_count * DH * lax.axis_size("tp")) + EPS)
    gated = jax.nn.sigmoid(output_gate_logits.astype(jnp.float32))
    gains = cell_norm_gain.astype(jnp.float32)
    return (gated * hidden * inverse[:, None] * gains[None, :]).astype(jnp.bfloat16)


def join_states(earlier, later):
    mem_a, norm_a, stab_a, log_a, first_a, last_a = earlier
    mem_b, norm_b, stab_b, log_b, first_b, last_b = later
    joined = last_a == last_b
    stab_ab = jnp.where(joined, jnp.maximum(log_b + stab_a, stab_b), stab_b)
    weight_a = jnp.where(joined, jnp.exp(log_b + stab_a - stab_ab), 0.0)
    weight_b = jnp.exp(stab_b - stab_ab)
    memory = weight_a[:, None, None] * mem_a + weight_b[:, None, None] * mem_b
    normer = weight_a[:, None] * norm_a + weight_b[:, None] * norm_b
    blank_b = last_b < 0
    memory = jnp.where(blank_b, mem_a, memory)
    normer = jnp.where(blank_b, norm_a, normer)
    stabil = jnp.where(blank_b, stab_a, stab_ab)
    first_doc = jnp.where(first_a < 0, first_b, first_a)
    last_doc = jnp.where(blank_b, last_a, last_b)
    return (memory, normer, stabil, log_a + log_b, first_doc, last_doc)


def local(
    queries,
    keys,
    values,
    output_gate_logits,
    input_gate_log,
    forget_gate_logits,
    extra_decay_log,
    document,
    residual,
    cell_norm_gain,
    output_weight,
    mixer_norm_gain,
    up_weight,
    down_weight,
):
    query_heads, final_state, output_rows = within_block_pass(
        queries, keys, values, input_gate_log, forget_gate_logits, extra_decay_log, document
    )
    numerator, denominator, peak_log, cumulative = output_rows
    memory, normer, stabil, last_doc = final_state
    step_logs = cumulative[:, :, -1]
    offsets = jnp.cumsum(step_logs, axis=0) - step_logs
    through = cumulative + offsets[:, :, None]
    summary = (memory, normer, stabil, jnp.sum(step_logs, axis=0), document[0], last_doc)
    identity = (
        jnp.zeros_like(memory),
        jnp.zeros_like(normer),
        jnp.full_like(stabil, NEG),
        jnp.zeros_like(stabil),
        jnp.array(-1, jnp.int32),
        jnp.array(-1, jnp.int32),
    )
    prefix = carried_in(summary, "sp", join_states, identity)
    doc_blocks = document.reshape(-1, BLOCK)
    carried_log = jnp.where(
        (doc_blocks == prefix[5])[:, None, :], through + prefix[2][None, :, None], NEG
    )
    merged_peak = jnp.maximum(peak_log, carried_log)
    own_weight = jnp.exp(peak_log - merged_peak)
    far_weight = jnp.exp(carried_log - merged_peak)
    numerator = own_weight[..., None] * numerator + far_weight[..., None] * jnp.einsum(
        "nhtd,hde->nhte", query_heads, prefix[0], precision=HIGH
    )
    denominator = own_weight * denominator + far_weight * jnp.einsum(
        "nhtd,hd->nht", query_heads, prefix[1], precision=HIGH
    )
    cell_out = numerator / jnp.maximum(jnp.abs(denominator), 1.0)[..., None]
    mixed = head_mix(cell_out, output_gate_logits, cell_norm_gain)
    head_terms = jnp.dot(mixed, output_weight, preferred_element_type=jnp.float32)
    width = residual.shape[1]
    model_width = width * lax.axis_size("tp")
    own_sum = lax.psum_scatter(
        head_terms.astype(jnp.bfloat16), "tp", scatter_dimension=1, tiled=True
    ).astype(jnp.float32)
    first_sum = (residual.astype(jnp.float32) + own_sum).astype(jnp.bfloat16)
    first_wide = lax.optimization_barrier(first_sum).astype(jnp.float32)
    squares = lax.psum(jnp.sum(first_wide * first_wide, axis=1), "tp")
    inverse = lax.rsqrt(squares / model_width + EPS)
    normed_own = (first_wide * inverse[:, None] * mixer_norm_gain.astype(jnp.float32)).astype(
        jnp.bfloat16
    )
    normed_full = lax.all_gather(normed_own, "tp", axis=1, tiled=True)
    hidden = jnp.dot(
        normed_full,
        lax.all_gather(up_weight, "sp", axis=0, tiled=True),
        preferred_element_type=jnp.float32,
    )
    squared = jnp.square(jax.nn.relu(hidden)).astype(jnp.bfloat16)
    channel = jnp.dot(
        squared,
        lax.all_gather(down_weight, "sp", axis=1, tiled=True),
        preferred_element_type=jnp.float32,
    )
    own_channel = lax.psum_scatter(
        channel.astype(jnp.bfloat16), "tp", scatter_dimension=1, tiled=True
    ).astype(jnp.float32)
    return (lax.optimization_barrier(first_sum).astype(jnp.float32) + own_channel).astype(
        jnp.bfloat16
    )


MESH = pl.DeviceIdType.MESH
F32 = jnp.float32
BF16 = jnp.bfloat16
CHUNKS = 2
SUBS = 2


def to_columns(rows):
    pad = jnp.zeros((128 - rows.shape[0], rows.shape[1]), F32)
    return jnp.transpose(jnp.concatenate([rows, pad], axis=0))


def to_rows(column):
    return jnp.transpose(jnp.broadcast_to(column, (column.shape[0], 128)))[0:8, :]


def halves(wide):
    high = wide.astype(BF16)
    return high, (wide - high.astype(F32)).astype(BF16)


def two_pass(wide, narrow):
    high, low = halves(wide)
    return jnp.dot(high, narrow, preferred_element_type=F32) + jnp.dot(
        low, narrow, preferred_element_type=F32
    )


def layer_kernel(
    n,
    m,
    back,
    q_ref,
    k_ref,
    v_ref,
    og_ref,
    forget_ref,
    extra_ref,
    input_ref,
    doc_ref,
    resid_ref,
    cell_gain_ref,
    mixer_gain_ref,
    wout_ref,
    up_ref,
    down_ref,
    out_ref,
    up_all,
    down_all,
    wcols,
    state_out,
    near_state,
    pair_state,
    state_in,
    tail_out,
    near_tail,
    pair_tail,
    tail_in,
    numer_ref,
    y_all,
    squares_out,
    squares_in,
    first_ref,
    normed,
    sums_out,
    sums_in,
    squared,
    parts,
    sib_in,
    comb,
    x_in,
    last_out,
    last_in,
    diag_in,
    w_send,
    w_recv,
    z_send,
    z_recv,
    relay_send,
    y_send,
    y_recv,
    near_send,
    near_recv,
    state_send,
    state_recv,
    mix_send,
    mix_recv,
    squares_send,
    squares_recv,
    normed_send,
    normed_recv,
    sums_send,
    sums_recv,
    sib_send,
    sib_recv,
    x_send,
    x_recv,
    diag_recv,
    last_send,
    last_recv,
):
    sp, tp = lax.axis_index("sp"), lax.axis_index("tp")
    rows, heads = q_ref.shape[0], q_ref.shape[1] // DH
    depth, hidden_width = up_ref.shape
    own_width = hidden_width // 2
    width = resid_ref.shape[1]
    up_piece, down_piece = depth // (CHUNKS * SUBS), depth // CHUNKS
    deep_piece = own_width // SUBS
    z, y, lines = sp // 2, sp % 2, n // 2
    p, x, c = z % 2, tp // 2, tp % 2

    def z_at(j):
        return (z, z + 1 - 2 * p, z + 2 - 4 * (z // 2), n // 2 - 1 - z)[j]

    def tp_at(bits):
        far_c = c + (bits % 2) * (1 - 2 * c)
        far_x = x + ((bits // 2) % 2) * (1 - 2 * x)
        return 2 * far_x + far_c

    partner = 2 * z_at(1) + y
    beside = 2 * z + 1 - y

    barrier = pltpu.get_barrier_semaphore()
    for k in range(1, n):
        pl.semaphore_signal(barrier, device_id=((sp + k) % n, tp), device_id_type=MESH)
    for k in range(1, m):
        pl.semaphore_signal(barrier, device_id=(sp, (tp + k) % m), device_id_type=MESH)
    pl.semaphore_signal(barrier, device_id=(partner, tp_at(2)), device_id_type=MESH)
    pl.semaphore_wait(barrier, n + m - 1)

    def remote(src, dst, send_sem, recv_sem, device):
        return pltpu.make_async_remote_copy(
            src_ref=src,
            dst_ref=dst,
            send_sem=send_sem,
            recv_sem=recv_sem,
            device_id=device,
            device_id_type=MESH,
        )

    def cols_of(owner):
        return pl.ds(pl.multiple_of(owner * width, width), width)

    def w_copy(k):
        return remote(
            wout_ref.at[:, cols_of(tp_at(k))],
            wcols.at[tp],
            w_send.at[k - 1],
            w_recv.at[k - 1],
            (sp, tp_at(k)),
        )

    def w_arrival(k):
        there = wcols.at[tp_at(k)]
        return remote(there, there, w_send.at[k - 1], w_recv.at[k - 1], (sp, tp_at(k)))

    def slot(stream, block, piece):
        if stream == 0:
            start = pl.multiple_of(block * depth + piece * up_piece, up_piece)
            return up_all.at[pl.ds(start, up_piece), :]
        deep = pl.ds(piece % SUBS * deep_piece, deep_piece)
        return down_all.at[block, piece // SUBS, deep]

    def own_piece(stream, half, piece):
        if stream == 0:
            lanes = pl.ds(pl.multiple_of(half * own_width, own_width), own_width)
            return up_ref.at[pl.ds(piece * up_piece, up_piece), lanes]
        start = pl.multiple_of(half * own_width + piece % SUBS * deep_piece, deep_piece)
        cols = pl.ds(piece // SUBS * down_piece, down_piece)
        return down_ref.at[pl.ds(start, deep_piece), cols]

    def z_copy(stream, j, piece):
        return remote(
            own_piece(stream, z_at(j) % 2, piece),
            slot(stream, sp, piece),
            z_send.at[stream, j - 1, piece],
            z_recv.at[stream, j - 1, piece],
            (2 * z_at(j) + y, tp),
        )

    inner = p + z // 2 == 1

    def z_forward(stream, piece):
        there = slot(stream, 2 * z_at(1) + y, piece)
        return remote(
            there,
            there,
            relay_send.at[stream, piece],
            z_recv.at[stream, 2, piece],
            (2 * z_at(2) + y, tp),
        )

    def z_arrival(stream, j, piece):
        there = slot(stream, 2 * z_at(j) + y, piece)
        return remote(
            there,
            there,
            z_send.at[stream, j - 1, piece],
            z_recv.at[stream, j - 1, piece],
            (2 * z_at(j) + y, tp),
        )

    def y_copy(stream, i, piece):
        there = slot(stream, 2 * z_at(i) + y, piece)
        return remote(
            own_piece(stream, p, piece) if i == 0 else there,
            there,
            y_send.at[stream, i, piece],
            y_recv.at[stream, i, piece],
            (beside, tp),
        )

    def y_arrival(stream, i, piece):
        there = slot(stream, 2 * z_at(i) + 1 - y, piece)
        return remote(
            there,
            there,
            y_send.at[stream, i, piece],
            y_recv.at[stream, i, piece],
            (beside, tp),
        )

    order = ((1, 0), (1, 1), (2, 0), (3, 0), (2, 1), (3, 1))
    down_order = ((1, 0), (2, 0), (3, 0), (1, 1), (2, 1), (3, 1))
    events = [
        (stream, j, SUBS * piece + i)
        for stream in range(2)
        for j, piece in (order, down_order)[stream]
        for i in range(SUBS)
    ]

    def z_start(stream, j, piece):
        for i in range(SUBS):
            z_copy(stream, j, SUBS * piece + i).start()

    def y_start(stream, piece):
        for i in range(SUBS):
            y_copy(stream, 0, SUBS * piece + i).start()

    done = [0]

    def pump(until):
        while done[0] < min(SUBS * until, len(events)):
            event = done[0]
            stream, j, piece = events[event]
            done[0] += 1
            z_arrival(stream, j, piece).wait_recv()
            y_copy(stream, j, piece).start()
            if j == 1:

                @pl.when(inner)
                def _():
                    z_forward(stream, piece).start()

    ups = len(order)

    for k in range(1, m):
        w_copy(k).start()

    document = doc_ref[...].astype(F32)
    across = lax.broadcasted_iota(jnp.int32, (rows, rows), 1)
    along = lax.broadcasted_iota(jnp.int32, (rows, rows), 0)
    upper = (along <= across).astype(BF16)
    forget = jax.nn.log_sigmoid(forget_ref[...]) + extra_ref[...]
    high = forget.astype(BF16).astype(F32)
    middle = (forget - high).astype(BF16).astype(F32)
    low = forget - high - middle
    slab = lax.broadcasted_iota(jnp.int32, (8, rows), 0)
    split = jnp.zeros((8, rows), F32)
    for h in range(heads):
        for i, part in enumerate((high, middle, low)):
            split = jnp.where(slab == heads * i + h, part[h : h + 1, :], split)
    summed = jnp.dot(split.astype(BF16), upper, preferred_element_type=F32)
    last_doc = document[:, rows - 1 : rows]
    sums, entry, totals, stabs, scaled = [], [], [], [], []
    for h in range(heads):
        line_sum = summed[h : h + 1, :]
        for i in range(1, 3):
            line_sum = line_sum + summed[heads * i + h : heads * i + h + 1, :]
        sums.append(line_sum)
        entry.append(input_ref[h : h + 1, :] - line_sum)
        total = line_sum[:, rows - 1 : rows]
        keep = jnp.where(document == last_doc, total + entry[h], NEG)
        stab = jnp.max(keep, axis=1, keepdims=True)
        totals.append(total)
        stabs.append(stab)
        scaled.append(jnp.exp(keep - stab))
    packed = jnp.broadcast_to(document, (8, rows))
    for h in range(heads):
        packed = jnp.where(slab == h, sums[h], packed)
        packed = jnp.where(slab == heads + h, scaled[h], packed)
    columns = to_columns(packed)
    doc_col = columns[:, 2 * heads : 2 * heads + 1]
    line = lax.broadcasted_iota(jnp.int32, (8, DH), 0)
    for h in range(heads):
        mine = slice(h * DH, (h + 1) * DH)
        weighted = k_ref[:, mine].astype(F32) * columns[:, heads + h : heads + h + 1]
        state_out[h] = lax.dot_general(
            weighted.astype(BF16),
            v_ref[:, mine],
            (((0,), (0,)), ((), ())),
            preferred_element_type=F32,
        ).astype(BF16)
        tail = jnp.broadcast_to(jnp.sum(weighted, axis=0, keepdims=True), (8, DH))
        tail = jnp.where(line == 1, stabs[h], tail)
        tail = jnp.where(line == 2, totals[h], tail)
        tail = jnp.where(line == 3, last_doc, tail)
        tail_out[h] = tail

    def pair_of(refs, send_sem, recv_sem, device):
        return [
            remote(src, dst, send_sem.at[i], recv_sem.at[i], device)
            for i, (src, dst) in enumerate(refs)
        ]

    def near_copies():
        refs = ((tail_out, near_tail), (state_out, near_state))
        return pair_of(refs, near_send, near_recv, (beside, tp))

    def state_copies(k):
        refs = ((pair_tail, tail_in.at[k - 1]), (pair_state, state_in.at[k - 1]))
        return pair_of(
            refs, state_send.at[k - 1], state_recv.at[k - 1], (2 * ((z + k) % lines) + y, tp)
        )

    for copy in near_copies():
        copy.start()
    z_start(0, 1, 0)

    @pl.when(inner)
    def _():
        z_start(0, 3, 0)

    for piece in range(CHUNKS):
        y_start(0, piece)

    for k in range(1, back + 1):

        @pl.when(z < k)
        def _():
            tail_in[k - 1] = jnp.zeros((heads, 8, DH), F32)
            state_in[k - 1] = jnp.zeros((heads, DH, DH), BF16)

    half_lanes = pl.ds(pl.multiple_of(p * own_width, own_width), own_width)
    up_all[pl.ds(pl.multiple_of(sp * depth, depth), depth), :] = up_ref[:, half_lanes]
    for piece in range(CHUNKS):
        cols = slice(piece * down_piece, (piece + 1) * down_piece)
        down_all[sp, piece] = down_ref[half_lanes, cols]

    @pl.when(x == z // 2)
    def _():
        diag_in[...] = jnp.zeros(diag_in.shape, BF16)

    step = min(rows, 256)
    locals_of = []
    for h in range(heads):
        mine = slice(h * DH, (h + 1) * DH)
        peaks, denoms = [], []
        for start in range(0, rows, step):
            stop = start + step
            here = slice(start, stop)
            scores = lax.dot_general(
                q_ref[here, mine],
                k_ref[0:stop, mine],
                (((1,), (1,)), ((), ())),
                preferred_element_type=F32,
            ) * (DH**-0.5)
            pair = columns[here, h : h + 1] + entry[h][:, 0:stop]
            seen = (doc_col[here] == document[:, 0:stop]) & (
                along[here, 0:stop] >= across[here, 0:stop]
            )
            pair = jnp.where(seen, pair, NEG)
            peak = jnp.max(pair, axis=1, keepdims=True)
            scores = scores * jnp.exp(pair - peak)
            numer_ref[h, here, :] = two_pass(scores, v_ref[0:stop, mine])
            peaks.append(peak)
            denoms.append(jnp.sum(scores, axis=1, keepdims=True))
        locals_of.append((jnp.concatenate(peaks, axis=0), jnp.concatenate(denoms, axis=0)))

    for copy in near_copies():
        copy.wait_recv()
    for h in range(heads):
        own_tail, far_tail = tail_out[h], near_tail[h]
        old_tail = jnp.where(y == 0, own_tail, far_tail)
        new_tail = jnp.where(y == 0, far_tail, own_tail)
        own_state, far_state = state_out[h].astype(F32), near_state[h].astype(F32)
        old_state = jnp.where(y == 0, own_state, far_state)
        new_state = jnp.where(y == 0, far_state, own_state)
        joined = old_tail[3:4, :] == new_tail[3:4, :]
        old_log = jnp.where(joined, old_tail[1:2, :] + new_tail[2:3, :], NEG)
        stab = jnp.maximum(old_log, new_tail[1:2, :])
        old_weight = jnp.where(joined, jnp.exp(old_log - stab), 0.0)
        new_weight = jnp.exp(new_tail[1:2, :] - stab)
        pair_state[h] = (
            jnp.where(joined, old_weight * old_state, 0.0) + new_weight * new_state
        ).astype(BF16)
        tail = jnp.where(joined, old_weight * old_tail, 0.0) + new_weight * new_tail
        tail = jnp.where(line == 1, stab, tail)
        tail = jnp.where(line == 2, old_tail + new_tail, tail)
        pair_tail[h] = jnp.where(line == 3, new_tail, tail)

    for k in range(1, back + 1):

        @pl.when(z + k < lines)
        def _():
            for copy in state_copies(k):
                copy.start()

    z_start(0, 1, 1)
    z_start(0, 2, 0)
    for k in range(1, back + 1):

        @pl.when(z >= k)
        def _():
            for copy in state_copies(k):
                copy.wait_recv()

    def mix_copy(k, h):
        here = y_all.at[tp, :, pl.ds(h * DH, DH)]
        return remote(
            here, here, mix_send.at[k - 1, h], mix_recv.at[k - 1, h], (sp, tp_at(k))
        )

    def mix_forward(h):
        there = y_all.at[tp_at(2), :, pl.ds(h * DH, DH)]
        return remote(there, there, mix_send.at[2, h], mix_recv.at[2, h], (sp, tp_at(1)))

    def mix_arrival(k, h):
        there = y_all.at[tp_at(k), :, pl.ds(h * DH, DH)]
        return remote(
            there, there, mix_send.at[k - 1, h], mix_recv.at[k - 1, h], (sp, tp_at(k))
        )

    first_doc = document[:, 0:1]
    square_sum = jnp.zeros((rows, DH), F32)
    for h in range(heads):
        mine = slice(h * DH, (h + 1) * DH)
        earlier = [(near_tail, near_state, y == 1)]
        earlier += [(tail_in.at[k], state_in.at[k], z > k) for k in range(back)]
        between = jnp.zeros((1, DH), F32)
        logs, valids = [], []
        best = jnp.full((1, DH), NEG, F32)
        for tails, _, exists in earlier:
            tail = tails[h]
            valid = (tail[3:4, :] == first_doc) & jnp.broadcast_to(exists, (1, DH))
            log = jnp.where(valid, between + tail[1:2, :], NEG)
            between = between + jnp.where(exists, tail[2:3, :], 0.0)
            best = jnp.maximum(best, log)
            logs.append(log)
            valids.append(valid)
        memory = jnp.zeros((DH, DH), F32)
        normer = jnp.zeros((1, DH), F32)
        for i, (tails, states, _) in enumerate(earlier):
            weight = jnp.where(valids[i], jnp.exp(logs[i] - best), 0.0)
            memory = memory + jnp.where(valids[i], weight * states[h].astype(F32), 0.0)
            normer = normer + jnp.where(valids[i], weight * tails[h, 0:1, :], 0.0)
        peak, denom = locals_of[h]
        carried = jnp.where(doc_col == first_doc, columns[:, h : h + 1] + best[:, 0:1], NEG)
        merged = jnp.maximum(peak, carried)
        own = jnp.exp(peak - merged)
        other = jnp.exp(carried - merged) * (DH**-0.5)
        query = q_ref[:, mine]
        high, low = halves(memory)
        reached = jnp.dot(query, high, preferred_element_type=F32) + jnp.dot(
            query, low, preferred_element_type=F32
        )
        numer = own * numer_ref[h] + other * reached
        denom = own * denom + other * jnp.sum(
            query.astype(F32) * normer, axis=1, keepdims=True
        )
        cell = numer / jnp.maximum(jnp.abs(denom), 1.0)
        square_sum = square_sum + cell * cell
        gated = jax.nn.sigmoid(og_ref[:, mine].astype(F32))
        y_all[tp, :, mine] = (gated * cell * cell_gain_ref[mine].astype(F32)[None, :]).astype(BF16)
        for k in range(1, 3):
            mix_copy(k, h).start()
    squares_out[...] = to_rows(jnp.sum(square_sum, axis=1, keepdims=True))

    def square_copy(k):
        return remote(
            squares_out,
            squares_in.at[k - 1],
            squares_send.at[k - 1],
            squares_recv.at[k - 1],
            (sp, tp_at(k)),
        )

    for k in range(1, m):
        square_copy(k).start()
    here = cols_of(tp)
    attn = jnp.dot(y_all[tp], wout_ref[:, here], preferred_element_type=F32)
    pump(PUMPS[0])

    @pl.when(inner)
    def _():
        for j in (2, 3):
            z_start(0, j, 1)

    for h in range(heads):
        mix_arrival(2, h).wait_recv()
        mix_forward(h).start()
    pump(PUMPS[1])
    for k in (1, 2, 3):
        w_arrival(k).wait_recv()
        if k != 2:
            for h in range(heads):
                mix_arrival(k, h).wait_recv()
        attn = attn + jnp.dot(
            y_all[tp_at(k)], wcols[tp_at(k)], preferred_element_type=F32
        )
    squares = squares_out[...]
    for k in range(1, m):
        square_copy(k).wait_recv()
        squares = squares + squares_in[k - 1]
    inverse = lax.rsqrt(to_columns(squares)[:, 0:1] / (heads * DH * m) + EPS)
    first = (resid_ref[...].astype(F32) + attn * inverse).astype(BF16)
    first_ref[...] = first
    first = first.astype(F32)

    def plane(bit):
        return p + bit * (1 - 2 * p)

    def rows_of(bit):
        return pl.ds(pl.multiple_of(plane(bit) * rows, rows), rows)

    normed[rows_of(0), here] = (first * mixer_gain_ref[...].astype(F32)[None, :]).astype(BF16)

    def group_at(bits):
        return (sp + (bits // 4) * (partner - sp), tp_at(bits % 4))

    def normed_block(bits):
        return normed.at[rows_of(bits // 4), cols_of(tp_at(bits % 4))]

    def normed_copy(source, flip):
        block = normed_block(source)
        rel = source + flip - 1
        return remote(block, block, normed_send.at[rel], normed_recv.at[rel], group_at(flip))

    def normed_arrival(rel):
        block = normed_block(rel)
        return remote(
            block, block, normed_send.at[rel - 1], normed_recv.at[rel - 1], group_at(rel % 2 or rel)
        )

    routes = ((0, 2), (0, 4), (0, 1), (2, 1), (4, 2), (4, 1), (6, 1))
    sums_out[0] = to_rows(jnp.sum(first * first, axis=1, keepdims=True))

    def sums_copy(k):
        return remote(
            sums_out.at[k // 4],
            sums_in.at[k - 1],
            sums_send.at[k - 1],
            sums_recv.at[k - 1],
            group_at(k),
        )

    for k in range(1, m):
        sums_copy(k).start()
    for route in routes[:3]:
        normed_copy(*route).start()
    total = sums_out[0]
    for k in range(1, m):
        sums_copy(k).wait_recv()
        total = total + sums_in[k - 1]
    sums_out[1] = total
    sums_copy(4).start()

    @pl.when(jnp.logical_not(inner))
    def _():
        z_start(0, 2, 1)

    y_start(1, 0)
    pump(PUMPS[2])
    normed_arrival(2).wait_recv()
    normed_copy(2, 1).start()
    normed_arrival(4).wait_recv()
    normed_copy(4, 2).start()
    normed_copy(4, 1).start()
    normed_arrival(1).wait_recv()
    normed_arrival(3).wait_recv()
    pump(ups - 1)

    @pl.when(inner)
    def _():
        for j in (2, 3):
            z_start(1, j, 0)

    pump(ups)

    z_start(1, 1, 0)

    @pl.when(jnp.logical_not(inner))
    def _():
        z_start(1, 2, 0)

    y_start(1, 1)
    for i in range(n // 2):
        for piece in range(CHUNKS * SUBS):
            y_arrival(0, i, piece).wait_recv()

    tile = min(own_width, 256)

    def up_half(bit, line_sums):
        scale = lax.rsqrt(to_columns(line_sums)[:, 0:1] / (width * m) + EPS)

        def up_tile(t, carry):
            cols = pl.ds(pl.multiple_of(t * tile, tile), tile)
            raw = jnp.dot(normed[rows_of(bit), :], up_all[:, cols], preferred_element_type=F32)
            hidden = jnp.maximum(raw * scale, 0.0)
            squared[rows_of(bit), cols] = (hidden * hidden).astype(BF16)
            return carry

        lax.fori_loop(0, own_width // tile, up_tile, 0)

    up_half(0, total)
    pump(ups + 1)


    normed_arrival(6).wait_recv()
    normed_copy(6, 1).start()
    normed_arrival(5).wait_recv()
    normed_arrival(7).wait_recv()
    sums_copy(4).wait_recv()
    up_half(1, sums_in[3])
    for j in (1, 2):
        z_start(1, j, 1)

    @pl.when(inner)
    def _():
        z_start(1, 3, 1)


    pairs = [(0, piece) for piece in range(CHUNKS)] + list(down_order)
    units = [(j, side, piece) for j, piece in pairs for side in range(2)]

    def place(i):
        j, side, piece = units[i]
        owner = z_at(j)
        return owner, owner // 2, y + side * (1 - 2 * y), piece

    def sib_copy(i, bit):
        _, far_x, half, piece = place(i)
        here = pl.ds(bit * rows if isinstance(bit, int) else pl.multiple_of(bit * rows, rows), rows)
        return remote(
            parts.at[i, here],
            sib_in.at[far_x, half, piece, here],
            sib_send.at[far_x, half, piece, bit],
            sib_recv.at[far_x, half, piece, bit],
            (sp, tp_at(1)),
        )

    def x_copy(i, cross):
        _, far_x, half, piece = place(i)
        late = cross == 1 and units[i][0] > 1
        return remote(
            comb.at[far_x, half, piece, rows_of(cross)],
            diag_in.at[half, piece] if late else x_in.at[half, piece, rows_of(cross)],
            x_send.at[half, piece, cross],
            diag_recv.at[half, piece] if late else x_recv.at[half, piece, cross],
            (partner if late else sp, tp_at(2)),
        )

    def last_copy(i):
        _, far_x, half, piece = place(i)
        late = units[i][0] > 1
        return remote(
            comb.at[far_x, half, piece, rows_of(1)] if late else last_out.at[half, piece],
            last_in.at[half, piece],
            last_send.at[half, piece],
            last_recv.at[half, piece],
            (partner, tp),
        )

    def down_units(*which):
        deep = [down_all[2 * place(i)[0] + place(i)[2], place(i)[3]] for i in which]
        deep = jnp.concatenate(deep, axis=1)
        for bit in range(2):
            here = slice(bit * rows, (bit + 1) * rows)
            wide = jnp.dot(squared[here, :], deep, preferred_element_type=F32).astype(BF16)
            for k, i in enumerate(which):
                parts[i, here, :] = wide[:, k * down_piece : (k + 1) * down_piece]
        for i in which:

            @pl.when(place(i)[0] % 2 != c)
            def _():
                for bit in range(2):
                    sib_copy(i, bit).start()

    def combine(i):
        owner, far_x, half, piece = place(i)

        @pl.when(owner % 2 == c)
        def _():
            for cross in (1, 0):
                here = rows_of(cross)
                sib_copy(i, plane(cross)).wait_recv()
                comb[far_x, half, piece, here, :] = (
                    parts[i, here, :].astype(F32)
                    + sib_in[far_x, half, piece, here, :].astype(F32)
                ).astype(BF16)

                @pl.when(far_x != x)
                def _():
                    x_copy(i, cross).start()

                if cross == 1 and units[i][0] > 1:

                    @pl.when(far_x == x)
                    def _():
                        last_copy(i).start()

    def settle(i):
        owner, far_x, half, piece = place(i)

        @pl.when(owner == tp)
        def _():
            x_copy(i, 1).wait_recv()
            last_out[half, piece] = (
                comb[far_x, half, piece, rows_of(1), :].astype(F32)
                + x_in[half, piece, rows_of(1), :].astype(F32)
            ).astype(BF16)
            last_copy(i).start()

    early = [i for i, unit in enumerate(units) if unit[0] < 2]
    settling = {len(pairs) - 4 + i // 2: early[i : i + 2] for i in range(0, len(early), 2)}
    waiting = []
    for k, (j, piece) in enumerate(pairs):
        pump(ups + max(0, k + 1 - CHUNKS + LEAD))
        ready = (2 * k, 2 * k + 1)
        if k >= SINGLES:
            down_units(ready[0])
            combine(ready[0])
        for i in range(SUBS):
            y_arrival(1, j, SUBS * piece + i).wait_recv()
        down_units(*ready[1 if k >= SINGLES else 0 :])
        for i in waiting:
            combine(i)
        waiting = list(ready) if k < 2 else []
        if k >= 2:
            for i in ready[1 if k >= SINGLES else 0 :]:
                combine(i)
        for i in settling.get(k, ()):
            settle(i)
    for i in waiting:
        combine(i)

    for half in range(2):
        for piece in range(CHUNKS):
            start = half * depth + piece * down_piece
            cols = slice(start, start + down_piece)
            total = first_ref[:, cols].astype(F32)
            total = total + comb[x, half, piece, rows_of(0), :].astype(F32)

            def landed(ref, send_sem, recv_sem):
                remote(ref, ref, send_sem, recv_sem, (partner, tp)).wait_recv()
                return ref[...].astype(F32)

            total = total + landed(
                x_in.at[half, piece, rows_of(0)],
                x_send.at[half, piece, 0],
                x_recv.at[half, piece, 0],
            )
            total = total + landed(
                last_in.at[half, piece], last_send.at[half, piece], last_recv.at[half, piece]
            )

            @pl.when(x != z // 2)
            def _():
                landed(
                    diag_in.at[half, piece], x_send.at[half, piece, 0], diag_recv.at[half, piece]
                )

            total = total + diag_in[half, piece].astype(F32)
            out_ref[:, cols] = total.astype(BF16)

    for k in range(1, m):
        w_copy(k).wait_send()
        square_copy(k).wait_send()
        for h in range(heads):
            (mix_copy(k, h) if k < 3 else mix_forward(h)).wait_send()
    for k in range(1, m + 1):
        sums_copy(k).wait_send()
    for route in routes:
        normed_copy(*route).wait_send()
    for stream in range(2):
        for piece in range(CHUNKS * SUBS):
            for j in range(1, 3):
                z_copy(stream, j, piece).wait_send()

            @pl.when(inner)
            def _():
                z_copy(stream, 3, piece).wait_send()
                z_forward(stream, piece).wait_send()

            for i in range(n // 2):
                y_copy(stream, i, piece).wait_send()
    for copy in near_copies():
        copy.wait_send()
    for k in range(1, back + 1):

        @pl.when(z + k < lines)
        def _():
            for copy in state_copies(k):
                copy.wait_send()

    for i in range(len(units)):
        owner = place(i)[0]

        @pl.when(owner % 2 != c)
        def _():
            for bit in range(2):
                sib_copy(i, bit).wait_send()

        @pl.when((owner % 2 == c) & (place(i)[1] != x))
        def _():
            for cross in range(2):
                x_copy(i, cross).wait_send()

        @pl.when(owner == tp)
        def _():
            last_copy(i).wait_send()


PUMPS = (1, 2, 4, 2, 3)
LEAD = 1
SINGLES = 3


def fused(
    n,
    m,
    queries,
    keys,
    values,
    output_gate_logits,
    input_gate_log,
    forget_gate_logits,
    extra_decay_log,
    document,
    residual,
    cell_norm_gain,
    output_weight,
    mixer_norm_gain,
    up_weight,
    down_weight,
):
    rows, heads = queries.shape[0], queries.shape[1] // DH
    depth, hidden_width = up_weight.shape
    width = residual.shape[1]
    own_width = hidden_width // 2
    lines = n // 2
    back = min(lines - 1, ((MOST - 2) // rows + 2) // 2)
    dma = pltpu.SemaphoreType.DMA
    return pl.pallas_call(
        functools.partial(layer_kernel, n, m, back),
        out_shape=jax.ShapeDtypeStruct((rows, width), BF16),
        in_specs=[pl.BlockSpec(memory_space=pltpu.VMEM)] * 14,
        out_specs=pl.BlockSpec(memory_space=pltpu.VMEM),
        scratch_shapes=[
            pltpu.VMEM((n * depth, own_width), BF16),
            pltpu.VMEM((n, CHUNKS, own_width, depth // CHUNKS), BF16),
            pltpu.VMEM((m, heads * DH, width), BF16),
            pltpu.VMEM((heads, DH, DH), BF16),
            pltpu.VMEM((heads, DH, DH), BF16),
            pltpu.VMEM((heads, DH, DH), BF16),
            pltpu.VMEM((back, heads, DH, DH), BF16),
            pltpu.VMEM((heads, 8, DH), F32),
            pltpu.VMEM((heads, 8, DH), F32),
            pltpu.VMEM((heads, 8, DH), F32),
            pltpu.VMEM((back, heads, 8, DH), F32),
            pltpu.VMEM((heads, rows, DH), F32),
            pltpu.VMEM((m, rows, heads * DH), BF16),
            pltpu.VMEM((8, rows), F32),
            pltpu.VMEM((m - 1, 8, rows), F32),
            pltpu.VMEM((rows, width), BF16),
            pltpu.VMEM((2 * rows, m * width), BF16),
            pltpu.VMEM((2, 8, rows), F32),
            pltpu.VMEM((m, 8, rows), F32),
            pltpu.VMEM((2 * rows, own_width), BF16),
            pltpu.VMEM((n * CHUNKS, 2 * rows, depth // CHUNKS), BF16),
            pltpu.VMEM((2, 2, CHUNKS, 2 * rows, depth // CHUNKS), BF16),
            pltpu.VMEM((2, 2, CHUNKS, 2 * rows, depth // CHUNKS), BF16),
            pltpu.VMEM((2, CHUNKS, 2 * rows, depth // CHUNKS), BF16),
            pltpu.VMEM((2, CHUNKS, rows, depth // CHUNKS), BF16),
            pltpu.VMEM((2, CHUNKS, rows, depth // CHUNKS), BF16),
            pltpu.VMEM((2, CHUNKS, rows, depth // CHUNKS), BF16),
            dma((m - 1,)),
            dma((m - 1,)),
            dma((2, lines - 1, CHUNKS * SUBS)),
            dma((2, lines - 1, CHUNKS * SUBS)),
            dma((2, CHUNKS * SUBS)),
            dma((2, lines, CHUNKS * SUBS)),
            dma((2, lines, CHUNKS * SUBS)),
            dma((2,)),
            dma((2,)),
            dma((back, 2)),
            dma((back, 2)),
            dma((m - 1, heads)),
            dma((m - 1, heads)),
            dma((m - 1,)),
            dma((m - 1,)),
            dma((2 * m - 1,)),
            dma((2 * m - 1,)),
            dma((m,)),
            dma((m,)),
            dma((2, 2, CHUNKS, 2)),
            dma((2, 2, CHUNKS, 2)),
            dma((2, CHUNKS, 2)),
            dma((2, CHUNKS, 2)),
            dma((2, CHUNKS)),
            dma((2, CHUNKS)),
            dma((2, CHUNKS)),
        ],
        compiler_params=pltpu.CompilerParams(
            collective_id=0, has_side_effects=True, vmem_limit_bytes=60 * 1024 * 1024
        ),
        name="layer",
    )(
        queries,
        keys,
        values,
        output_gate_logits,
        forget_gate_logits.T,
        extra_decay_log.T,
        input_gate_log.T,
        document[None, :],
        residual,
        cell_norm_gain,
        mixer_norm_gain,
        output_weight,
        up_weight,
        down_weight,
    )


def either(n, m, *args):
    depth, hidden_width = args[12].shape
    heads = args[0].shape[1] // DH
    fits = n == 8 and m == 4 and depth % 128 == 0 and hidden_width % 512 == 0
    fits = fits and 3 * heads <= 8 and args[8].shape[1] == 2 * depth
    fits = fits and args[0].shape[0] % 256 == 0
    if fits:
        return fused(n, m, *args)
    return local(*args)


def solution(mesh):
    in_specs = (
        P("sp", "tp"),
        P("sp", "tp"),
        P("sp", "tp"),
        P("sp", "tp"),
        P("sp", "tp"),
        P("sp", "tp"),
        P("sp", "tp"),
        P("sp"),
        P("sp", "tp"),
        P("tp"),
        P("tp", None),
        P("tp"),
        P("sp", "tp"),
        P("tp", "sp"),
    )
    out_specs = P("sp", "tp")
    body = functools.partial(either, mesh.shape["sp"], mesh.shape["tp"])
    return jax.shard_map(body, mesh=mesh, in_specs=in_specs, out_specs=out_specs, check_vma=False)
```

```python
import functools

import jax
import jax.numpy as jnp
from jax import lax
from jax.experimental import pallas as pl
from jax.experimental.pallas import tpu as pltpu
from jax.sharding import PartitionSpec as P

DH = 128
BLOCK = 128
MOST = 2048


NEG = -1e30
EPS = 1e-06
HIGH = lax.Precision.HIGHEST


def carried_in(value, axis, join, neutral):
    count, mine = (lax.axis_size(axis), lax.axis_index(axis))
    pieces = jax.tree.map(lambda part: lax.all_gather(part, axis), value)
    subtotal = jax.tree.map(
        lambda part, zero: jnp.full_like(part, 0) + jnp.asarray(zero, part.dtype), value, neutral
    )

    def step(position, subtotal):
        longer = join(subtotal, jax.tree.map(lambda part: part[position], pieces))
        return jax.tree.map(lambda new, old: jnp.where(position < mine, new, old), longer, subtotal)

    return lax.fori_loop(0, count - 1, step, subtotal)


def block_terms(carry, inputs):
    memory, normer, stabil, last_doc = carry
    q_blk, k_blk, v_blk, gate_in, gate_log, doc_blk = inputs
    length = doc_blk.shape[0]
    causal = jnp.arange(length)[:, None] >= jnp.arange(length)[None, :]
    cumulative = jnp.cumsum(gate_log, axis=-1)
    same_doc = (doc_blk[:, None] == doc_blk[None, :]) & causal
    pair_log = cumulative[:, :, None] - cumulative[:, None, :] + gate_in[:, None, :]
    pair_log = jnp.where(same_doc[None], pair_log, NEG)
    live_rows = doc_blk == last_doc
    carried_log = jnp.where(live_rows[None, :], cumulative + stabil[:, None], NEG)
    peak_log = jnp.maximum(carried_log, jnp.max(pair_log, axis=-1))
    weights = jnp.exp(pair_log - peak_log[:, :, None])
    carried = jnp.exp(carried_log - peak_log)
    scores = jnp.einsum("htd,hsd->hts", q_blk, k_blk, precision=HIGH) * weights
    numerator = carried[:, :, None] * jnp.einsum("htd,hde->hte", q_blk, memory, precision=HIGH)
    numerator = numerator + jnp.einsum("hts,hse->hte", scores, v_blk, precision=HIGH)
    denominator = carried * jnp.einsum("htd,hd->ht", q_blk, normer, precision=HIGH) + jnp.sum(
        scores, axis=-1
    )
    end_doc = doc_blk[-1]
    end_cum = cumulative[:, -1]
    keep_log = jnp.where(
        (doc_blk == end_doc)[None, :], end_cum[:, None] - cumulative + gate_in, NEG
    )
    old_log = jnp.where(last_doc == end_doc, end_cum + stabil, NEG)
    new_stab = jnp.maximum(old_log, jnp.max(keep_log, axis=-1))
    scaled = jnp.exp(keep_log - new_stab[:, None])
    decayed = jnp.exp(old_log - new_stab)
    memory = decayed[:, None, None] * memory + jnp.einsum(
        "hs,hsd,hse->hde", scaled, k_blk, v_blk, precision=HIGH
    )
    normer = decayed[:, None] * normer + jnp.einsum("hs,hsd->hd", scaled, k_blk, precision=HIGH)
    return ((memory, normer, new_stab, end_doc), (numerator, denominator, peak_log, cumulative))


def split_heads(source, blocks):
    return source.astype(jnp.float32).reshape(blocks, BLOCK, -1, DH).transpose(0, 2, 1, 3)


def split_gates(source, blocks):
    return source.reshape(blocks, BLOCK, -1).transpose(0, 2, 1)


def within_block_pass(
    queries, keys, values, input_gate_log, forget_gate_logits, extra_decay_log, document
):
    blocks = queries.shape[0] // BLOCK
    head_count = queries.shape[1] // DH
    query_heads = split_heads(queries, blocks) * DH ** (-0.5)
    forget_log_values = jax.nn.log_sigmoid(forget_gate_logits) + extra_decay_log
    inputs = (
        query_heads,
        split_heads(keys, blocks),
        split_heads(values, blocks),
        split_gates(input_gate_log, blocks),
        split_gates(forget_log_values, blocks),
        document.reshape(blocks, BLOCK),
    )
    initial = (
        jnp.zeros((head_count, DH, DH), jnp.float32),
        jnp.zeros((head_count, DH), jnp.float32),
        jnp.full((head_count,), NEG, jnp.float32),
        jnp.array(-1, jnp.int32),
    )
    final_state, output_rows = lax.scan(block_terms, initial, inputs)
    return (query_heads, final_state, output_rows)


def head_mix(cell_out, output_gate_logits, cell_norm_gain):
    row_count = output_gate_logits.shape[0]
    head_count = cell_out.shape[1]
    hidden = cell_out.transpose(0, 2, 1, 3).reshape(row_count, head_count * DH)
    squares = lax.psum(jnp.sum(hidden * hidden, axis=1), "tp")
    inverse = lax.rsqrt(squares / (head_count * DH * lax.axis_size("tp")) + EPS)
    gated = jax.nn.sigmoid(output_gate_logits.astype(jnp.float32))
    gains = cell_norm_gain.astype(jnp.float32)
    return (gated * hidden * inverse[:, None] * gains[None, :]).astype(jnp.bfloat16)


def join_states(earlier, later):
    mem_a, norm_a, stab_a, log_a, first_a, last_a = earlier
    mem_b, norm_b, stab_b, log_b, first_b, last_b = later
    joined = last_a == last_b
    stab_ab = jnp.where(joined, jnp.maximum(log_b + stab_a, stab_b), stab_b)
    weight_a = jnp.where(joined, jnp.exp(log_b + stab_a - stab_ab), 0.0)
    weight_b = jnp.exp(stab_b - stab_ab)
    memory = weight_a[:, None, None] * mem_a + weight_b[:, None, None] * mem_b
    normer = weight_a[:, None] * norm_a + weight_b[:, None] * norm_b
    blank_b = last_b < 0
    memory = jnp.where(blank_b, mem_a, memory)
    normer = jnp.where(blank_b, norm_a, normer)
    stabil = jnp.where(blank_b, stab_a, stab_ab)
    first_doc = jnp.where(first_a < 0, first_b, first_a)
    last_doc = jnp.where(blank_b, last_a, last_b)
    return (memory, normer, stabil, log_a + log_b, first_doc, last_doc)


def local(
    queries,
    keys,
    values,
    output_gate_logits,
    input_gate_log,
    forget_gate_logits,
    extra_decay_log,
    document,
    residual,
    cell_norm_gain,
    output_weight,
    mixer_norm_gain,
    up_weight,
    down_weight,
):
    query_heads, final_state, output_rows = within_block_pass(
        queries, keys, values, input_gate_log, forget_gate_logits, extra_decay_log, document
    )
    numerator, denominator, peak_log, cumulative = output_rows
    memory, normer, stabil, last_doc = final_state
    step_logs = cumulative[:, :, -1]
    offsets = jnp.cumsum(step_logs, axis=0) - step_logs
    through = cumulative + offsets[:, :, None]
    summary = (memory, normer, stabil, jnp.sum(step_logs, axis=0), document[0], last_doc)
    identity = (
        jnp.zeros_like(memory),
        jnp.zeros_like(normer),
        jnp.full_like(stabil, NEG),
        jnp.zeros_like(stabil),
        jnp.array(-1, jnp.int32),
        jnp.array(-1, jnp.int32),
    )
    prefix = carried_in(summary, "sp", join_states, identity)
    doc_blocks = document.reshape(-1, BLOCK)
    carried_log = jnp.where(
        (doc_blocks == prefix[5])[:, None, :], through + prefix[2][None, :, None], NEG
    )
    merged_peak = jnp.maximum(peak_log, carried_log)
    own_weight = jnp.exp(peak_log - merged_peak)
    far_weight = jnp.exp(carried_log - merged_peak)
    numerator = own_weight[..., None] * numerator + far_weight[..., None] * jnp.einsum(
        "nhtd,hde->nhte", query_heads, prefix[0], precision=HIGH
    )
    denominator = own_weight * denominator + far_weight * jnp.einsum(
        "nhtd,hd->nht", query_heads, prefix[1], precision=HIGH
    )
    cell_out = numerator / jnp.maximum(jnp.abs(denominator), 1.0)[..., None]
    mixed = head_mix(cell_out, output_gate_logits, cell_norm_gain)
    head_terms = jnp.dot(mixed, output_weight, preferred_element_type=jnp.float32)
    width = residual.shape[1]
    model_width = width * lax.axis_size("tp")
    own_sum = lax.psum_scatter(
        head_terms.astype(jnp.bfloat16), "tp", scatter_dimension=1, tiled=True
    ).astype(jnp.float32)
    first_sum = (residual.astype(jnp.float32) + own_sum).astype(jnp.bfloat16)
    first_wide = lax.optimization_barrier(first_sum).astype(jnp.float32)
    squares = lax.psum(jnp.sum(first_wide * first_wide, axis=1), "tp")
    inverse = lax.rsqrt(squares / model_width + EPS)
    normed_own = (first_wide * inverse[:, None] * mixer_norm_gain.astype(jnp.float32)).astype(
        jnp.bfloat16
    )
    normed_full = lax.all_gather(normed_own, "tp", axis=1, tiled=True)
    hidden = jnp.dot(
        normed_full,
        lax.all_gather(up_weight, "sp", axis=0, tiled=True),
        preferred_element_type=jnp.float32,
    )
    squared = jnp.square(jax.nn.relu(hidden)).astype(jnp.bfloat16)
    channel = jnp.dot(
        squared,
        lax.all_gather(down_weight, "sp", axis=1, tiled=True),
        preferred_element_type=jnp.float32,
    )
    own_channel = lax.psum_scatter(
        channel.astype(jnp.bfloat16), "tp", scatter_dimension=1, tiled=True
    ).astype(jnp.float32)
    return (lax.optimization_barrier(first_sum).astype(jnp.float32) + own_channel).astype(
        jnp.bfloat16
    )


MESH = pl.DeviceIdType.MESH
F32 = jnp.float32
BF16 = jnp.bfloat16
CHUNKS = 2
SUBS = 2


def to_columns(rows):
    pad = jnp.zeros((128 - rows.shape[0], rows.shape[1]), F32)
    return jnp.transpose(jnp.concatenate([rows, pad], axis=0))


def to_rows(column):
    return jnp.transpose(jnp.broadcast_to(column, (column.shape[0], 128)))[0:8, :]


def halves(wide):
    high = wide.astype(BF16)
    return high, (wide - high.astype(F32)).astype(BF16)


def two_pass(wide, narrow):
    high, low = halves(wide)
    return jnp.dot(high, narrow, preferred_element_type=F32) + jnp.dot(
        low, narrow, preferred_element_type=F32
    )


def layer_kernel(
    n,
    m,
    back,
    q_hbm,
    k_hbm,
    v_hbm,
    og_hbm,
    forget_ref,
    extra_ref,
    input_ref,
    doc_ref,
    resid_hbm,
    cell_gain_ref,
    mixer_gain_ref,
    wout_hbm,
    up_hbm,
    down_hbm,
    out_hbm,
    k_ref,
    v_ref,
    up_ref,
    q_ref,
    wout_ref,
    down_ref,
    og_ref,
    resid_ref,
    out_ref,
    up_all,
    down_all,
    wcols,
    state_out,
    near_state,
    pair_state,
    state_in,
    tail_out,
    near_tail,
    pair_tail,
    tail_in,
    numer_ref,
    y_all,
    squares_out,
    squares_in,
    first_ref,
    normed,
    sums_out,
    sums_in,
    squared,
    parts,
    sib_in,
    comb,
    x_in,
    last_out,
    last_in,
    diag_in,
    w_send,
    w_recv,
    z_send,
    z_recv,
    relay_send,
    y_send,
    y_recv,
    near_send,
    near_recv,
    state_send,
    state_recv,
    mix_send,
    mix_recv,
    squares_send,
    squares_recv,
    normed_send,
    normed_recv,
    sums_send,
    sums_recv,
    sib_send,
    sib_recv,
    x_send,
    x_recv,
    diag_recv,
    last_send,
    last_recv,
    load_sem,
    store_sem,
):
    loads = (
        (up_hbm, up_ref),
        (k_hbm, k_ref),
        (v_hbm, v_ref),
        (wout_hbm, wout_ref),
        (q_hbm, q_ref),
        (down_hbm, down_ref),
        (og_hbm, og_ref),
        (resid_hbm, resid_ref),
    )

    def fetch(ref):
        at = [dst is ref for _, dst in loads].index(True)
        return pltpu.make_async_copy(*loads[at], load_sem.at[at])

    for _, ref in loads:
        fetch(ref).start()
    sp, tp = lax.axis_index("sp"), lax.axis_index("tp")
    rows, heads = q_ref.shape[0], q_ref.shape[1] // DH
    depth, hidden_width = up_ref.shape
    own_width = hidden_width // 2
    width = resid_ref.shape[1]
    up_piece, down_piece = depth // (CHUNKS * SUBS), depth // CHUNKS
    deep_piece = own_width // SUBS
    z, y, lines = sp // 2, sp % 2, n // 2
    p, x, c = z % 2, tp // 2, tp % 2

    def z_at(j):
        return (z, z + 1 - 2 * p, z + 2 - 4 * (z // 2), n // 2 - 1 - z)[j]

    def tp_at(bits):
        far_c = c + (bits % 2) * (1 - 2 * c)
        far_x = x + ((bits // 2) % 2) * (1 - 2 * x)
        return 2 * far_x + far_c

    partner = 2 * z_at(1) + y
    beside = 2 * z + 1 - y

    barrier = pltpu.get_barrier_semaphore()
    for k in range(1, n):
        pl.semaphore_signal(barrier, device_id=((sp + k) % n, tp), device_id_type=MESH)
    for k in range(1, m):
        pl.semaphore_signal(barrier, device_id=(sp, (tp + k) % m), device_id_type=MESH)
    pl.semaphore_signal(barrier, device_id=(partner, tp_at(2)), device_id_type=MESH)
    pl.semaphore_wait(barrier, n + m - 1)

    def remote(src, dst, send_sem, recv_sem, device):
        return pltpu.make_async_remote_copy(
            src_ref=src,
            dst_ref=dst,
            send_sem=send_sem,
            recv_sem=recv_sem,
            device_id=device,
            device_id_type=MESH,
        )

    def cols_of(owner):
        return pl.ds(pl.multiple_of(owner * width, width), width)

    def w_copy(k):
        return remote(
            wout_ref.at[:, cols_of(tp_at(k))],
            wcols.at[tp],
            w_send.at[k - 1],
            w_recv.at[k - 1],
            (sp, tp_at(k)),
        )

    def w_arrival(k):
        there = wcols.at[tp_at(k)]
        return remote(there, there, w_send.at[k - 1], w_recv.at[k - 1], (sp, tp_at(k)))

    def slot(stream, block, piece):
        if stream == 0:
            start = pl.multiple_of(block * depth + piece * up_piece, up_piece)
            return up_all.at[pl.ds(start, up_piece), :]
        deep = pl.ds(piece % SUBS * deep_piece, deep_piece)
        return down_all.at[block, piece // SUBS, deep]

    def own_piece(stream, half, piece):
        if stream == 0:
            lanes = pl.ds(pl.multiple_of(half * own_width, own_width), own_width)
            return up_ref.at[pl.ds(piece * up_piece, up_piece), lanes]
        start = pl.multiple_of(half * own_width + piece % SUBS * deep_piece, deep_piece)
        cols = pl.ds(piece // SUBS * down_piece, down_piece)
        return down_ref.at[pl.ds(start, deep_piece), cols]

    def z_copy(stream, j, piece):
        return remote(
            own_piece(stream, z_at(j) % 2, piece),
            slot(stream, sp, piece),
            z_send.at[stream, j - 1, piece],
            z_recv.at[stream, j - 1, piece],
            (2 * z_at(j) + y, tp),
        )

    inner = p + z // 2 == 1

    def z_forward(stream, piece):
        there = slot(stream, 2 * z_at(1) + y, piece)
        return remote(
            there,
            there,
            relay_send.at[stream, piece],
            z_recv.at[stream, 2, piece],
            (2 * z_at(2) + y, tp),
        )

    def z_arrival(stream, j, piece):
        there = slot(stream, 2 * z_at(j) + y, piece)
        return remote(
            there,
            there,
            z_send.at[stream, j - 1, piece],
            z_recv.at[stream, j - 1, piece],
            (2 * z_at(j) + y, tp),
        )

    def y_copy(stream, i, piece):
        there = slot(stream, 2 * z_at(i) + y, piece)
        return remote(
            own_piece(stream, p, piece) if i == 0 else there,
            there,
            y_send.at[stream, i, piece],
            y_recv.at[stream, i, piece],
            (beside, tp),
        )

    def y_arrival(stream, i, piece):
        there = slot(stream, 2 * z_at(i) + 1 - y, piece)
        return remote(
            there,
            there,
            y_send.at[stream, i, piece],
            y_recv.at[stream, i, piece],
            (beside, tp),
        )

    order = ((1, 0), (1, 1), (2, 0), (3, 0), (2, 1), (3, 1))
    down_order = ((1, 0), (2, 0), (3, 0), (1, 1), (2, 1), (3, 1))
    events = [
        (stream, j, SUBS * piece + i)
        for stream in range(2)
        for j, piece in (order, down_order)[stream]
        for i in range(SUBS)
    ]

    def z_start(stream, j, piece):
        for i in range(SUBS):
            z_copy(stream, j, SUBS * piece + i).start()

    def y_start(stream, piece):
        for i in range(SUBS):
            y_copy(stream, 0, SUBS * piece + i).start()

    done = [0]

    def relay(event):
        stream, j, piece = events[event]
        z_arrival(stream, j, piece).wait_recv()
        y_copy(stream, j, piece).start()
        if j == 1:

            @pl.when(inner)
            def _():
                z_forward(stream, piece).start()

    def pump(until):
        while done[0] < min(SUBS * until, len(events)):
            event = done[0]
            relay(event)
            done[0] += 1

    def relay_when(condition, down_events):
        if down_events:

            @pl.when(condition)
            def _():
                for event in down_events:
                    relay(SUBS * ups + event)

    ups = len(order)

    fetch(up_ref).wait()
    z_start(0, 1, 0)

    @pl.when(inner)
    def _():
        z_start(0, 3, 0)

    fetch(wout_ref).wait()
    for k in range(1, m):
        w_copy(k).start()

    document = doc_ref[...].astype(F32)
    across = lax.broadcasted_iota(jnp.int32, (rows, rows), 1)
    along = lax.broadcasted_iota(jnp.int32, (rows, rows), 0)
    upper = (along <= across).astype(BF16)
    forget = jax.nn.log_sigmoid(forget_ref[...]) + extra_ref[...]
    high = forget.astype(BF16).astype(F32)
    middle = (forget - high).astype(BF16).astype(F32)
    low = forget - high - middle
    slab = lax.broadcasted_iota(jnp.int32, (8, rows), 0)
    split = jnp.zeros((8, rows), F32)
    for h in range(heads):
        for i, part in enumerate((high, middle, low)):
            split = jnp.where(slab == heads * i + h, part[h : h + 1, :], split)
    summed = jnp.dot(split.astype(BF16), upper, preferred_element_type=F32)
    last_doc = document[:, rows - 1 : rows]
    sums, entry, totals, stabs, scaled = [], [], [], [], []
    for h in range(heads):
        line_sum = summed[h : h + 1, :]
        for i in range(1, 3):
            line_sum = line_sum + summed[heads * i + h : heads * i + h + 1, :]
        sums.append(line_sum)
        entry.append(input_ref[h : h + 1, :] - line_sum)
        total = line_sum[:, rows - 1 : rows]
        keep = jnp.where(document == last_doc, total + entry[h], NEG)
        stab = jnp.max(keep, axis=1, keepdims=True)
        totals.append(total)
        stabs.append(stab)
        scaled.append(jnp.exp(keep - stab))
    packed = jnp.broadcast_to(document, (8, rows))
    for h in range(heads):
        packed = jnp.where(slab == h, sums[h], packed)
        packed = jnp.where(slab == heads + h, scaled[h], packed)
    columns = to_columns(packed)
    doc_col = columns[:, 2 * heads : 2 * heads + 1]
    line = lax.broadcasted_iota(jnp.int32, (8, DH), 0)
    fetch(k_ref).wait()
    fetch(v_ref).wait()
    for h in range(heads):
        mine = slice(h * DH, (h + 1) * DH)
        weighted = k_ref[:, mine].astype(F32) * columns[:, heads + h : heads + h + 1]
        state_out[h] = lax.dot_general(
            weighted.astype(BF16),
            v_ref[:, mine],
            (((0,), (0,)), ((), ())),
            preferred_element_type=F32,
        ).astype(BF16)
        tail = jnp.broadcast_to(jnp.sum(weighted, axis=0, keepdims=True), (8, DH))
        tail = jnp.where(line == 1, stabs[h], tail)
        tail = jnp.where(line == 2, totals[h], tail)
        tail = jnp.where(line == 3, last_doc, tail)
        tail_out[h] = tail

    def pair_of(refs, send_sem, recv_sem, device):
        return [
            remote(src, dst, send_sem.at[i], recv_sem.at[i], device)
            for i, (src, dst) in enumerate(refs)
        ]

    def near_copies():
        refs = ((tail_out, near_tail), (state_out, near_state))
        return pair_of(refs, near_send, near_recv, (beside, tp))

    def state_copies(k):
        refs = ((pair_tail, tail_in.at[k - 1]), (pair_state, state_in.at[k - 1]))
        return pair_of(
            refs, state_send.at[k - 1], state_recv.at[k - 1], (2 * ((z + k) % lines) + y, tp)
        )

    for copy in near_copies():
        copy.start()
    for piece in range(CHUNKS):
        y_start(0, piece)

    for k in range(1, back + 1):

        @pl.when(z < k)
        def _():
            tail_in[k - 1] = jnp.zeros((heads, 8, DH), F32)
            state_in[k - 1] = jnp.zeros((heads, DH, DH), BF16)

    fetch(down_ref).wait()
    half_lanes = pl.ds(pl.multiple_of(p * own_width, own_width), own_width)
    up_all[pl.ds(pl.multiple_of(sp * depth, depth), depth), :] = up_ref[:, half_lanes]
    for piece in range(CHUNKS):
        cols = slice(piece * down_piece, (piece + 1) * down_piece)
        down_all[sp, piece] = down_ref[half_lanes, cols]

    @pl.when(x == z // 2)
    def _():
        diag_in[...] = jnp.zeros(diag_in.shape, BF16)

    fetch(q_ref).wait()
    step = min(rows, 256)
    locals_of = []
    for h in range(heads):
        mine = slice(h * DH, (h + 1) * DH)
        peaks, denoms = [], []
        for start in range(0, rows, step):
            stop = start + step
            here = slice(start, stop)
            scores = lax.dot_general(
                q_ref[here, mine],
                k_ref[0:stop, mine],
                (((1,), (1,)), ((), ())),
                preferred_element_type=F32,
            ) * (DH**-0.5)
            pair = columns[here, h : h + 1] + entry[h][:, 0:stop]
            seen = (doc_col[here] == document[:, 0:stop]) & (
                along[here, 0:stop] >= across[here, 0:stop]
            )
            pair = jnp.where(seen, pair, NEG)
            peak = jnp.max(pair, axis=1, keepdims=True)
            scores = scores * jnp.exp(pair - peak)
            numer_ref[h, here, :] = two_pass(scores, v_ref[0:stop, mine])
            peaks.append(peak)
            denoms.append(jnp.sum(scores, axis=1, keepdims=True))
        locals_of.append((jnp.concatenate(peaks, axis=0), jnp.concatenate(denoms, axis=0)))

    for copy in near_copies():
        copy.wait_recv()
    for h in range(heads):
        own_tail, far_tail = tail_out[h], near_tail[h]
        old_tail = jnp.where(y == 0, own_tail, far_tail)
        new_tail = jnp.where(y == 0, far_tail, own_tail)
        own_state, far_state = state_out[h].astype(F32), near_state[h].astype(F32)
        old_state = jnp.where(y == 0, own_state, far_state)
        new_state = jnp.where(y == 0, far_state, own_state)
        joined = old_tail[3:4, :] == new_tail[3:4, :]
        old_log = jnp.where(joined, old_tail[1:2, :] + new_tail[2:3, :], NEG)
        stab = jnp.maximum(old_log, new_tail[1:2, :])
        old_weight = jnp.where(joined, jnp.exp(old_log - stab), 0.0)
        new_weight = jnp.exp(new_tail[1:2, :] - stab)
        pair_state[h] = (
            jnp.where(joined, old_weight * old_state, 0.0) + new_weight * new_state
        ).astype(BF16)
        tail = jnp.where(joined, old_weight * old_tail, 0.0) + new_weight * new_tail
        tail = jnp.where(line == 1, stab, tail)
        tail = jnp.where(line == 2, old_tail + new_tail, tail)
        pair_tail[h] = jnp.where(line == 3, new_tail, tail)

    for k in range(1, back + 1):

        @pl.when(z + k < lines)
        def _():
            for copy in state_copies(k):
                copy.start()

    z_start(0, 1, 1)
    z_start(0, 2, 0)
    for k in range(1, back + 1):

        @pl.when(z >= k)
        def _():
            for copy in state_copies(k):
                copy.wait_recv()

    def mix_copy(k, h):
        here = y_all.at[tp, :, pl.ds(h * DH, DH)]
        return remote(
            here, here, mix_send.at[k - 1, h], mix_recv.at[k - 1, h], (sp, tp_at(k))
        )

    def mix_forward(h):
        there = y_all.at[tp_at(2), :, pl.ds(h * DH, DH)]
        return remote(there, there, mix_send.at[2, h], mix_recv.at[2, h], (sp, tp_at(1)))

    def mix_arrival(k, h):
        there = y_all.at[tp_at(k), :, pl.ds(h * DH, DH)]
        return remote(
            there, there, mix_send.at[k - 1, h], mix_recv.at[k - 1, h], (sp, tp_at(k))
        )

    fetch(og_ref).wait()
    first_doc = document[:, 0:1]
    square_sum = jnp.zeros((rows, DH), F32)
    for h in range(heads):
        mine = slice(h * DH, (h + 1) * DH)
        earlier = [(near_tail, near_state, y == 1)]
        earlier += [(tail_in.at[k], state_in.at[k], z > k) for k in range(back)]
        between = jnp.zeros((1, DH), F32)
        logs, valids = [], []
        best = jnp.full((1, DH), NEG, F32)
        for tails, _, exists in earlier:
            tail = tails[h]
            valid = (tail[3:4, :] == first_doc) & jnp.broadcast_to(exists, (1, DH))
            log = jnp.where(valid, between + tail[1:2, :], NEG)
            between = between + jnp.where(exists, tail[2:3, :], 0.0)
            best = jnp.maximum(best, log)
            logs.append(log)
            valids.append(valid)
        memory = jnp.zeros((DH, DH), F32)
        normer = jnp.zeros((1, DH), F32)
        for i, (tails, states, _) in enumerate(earlier):
            weight = jnp.where(valids[i], jnp.exp(logs[i] - best), 0.0)
            memory = memory + jnp.where(valids[i], weight * states[h].astype(F32), 0.0)
            normer = normer + jnp.where(valids[i], weight * tails[h, 0:1, :], 0.0)
        peak, denom = locals_of[h]
        carried = jnp.where(doc_col == first_doc, columns[:, h : h + 1] + best[:, 0:1], NEG)
        merged = jnp.maximum(peak, carried)
        own = jnp.exp(peak - merged)
        other = jnp.exp(carried - merged) * (DH**-0.5)
        query = q_ref[:, mine]
        high, low = halves(memory)
        reached = jnp.dot(query, high, preferred_element_type=F32) + jnp.dot(
            query, low, preferred_element_type=F32
        )
        numer = own * numer_ref[h] + other * reached
        denom = own * denom + other * jnp.sum(
            query.astype(F32) * normer, axis=1, keepdims=True
        )
        cell = numer / jnp.maximum(jnp.abs(denom), 1.0)
        square_sum = square_sum + cell * cell
        gated = jax.nn.sigmoid(og_ref[:, mine].astype(F32))
        y_all[tp, :, mine] = (gated * cell * cell_gain_ref[mine].astype(F32)[None, :]).astype(BF16)
        for k in range(1, 3):
            mix_copy(k, h).start()
    squares_out[...] = to_rows(jnp.sum(square_sum, axis=1, keepdims=True))

    def square_copy(k):
        return remote(
            squares_out,
            squares_in.at[k - 1],
            squares_send.at[k - 1],
            squares_recv.at[k - 1],
            (sp, tp_at(k)),
        )

    for k in range(1, m):
        square_copy(k).start()
    here = cols_of(tp)
    attn = jnp.dot(y_all[tp], wout_ref[:, here], preferred_element_type=F32)
    pump(PUMPS[0])

    @pl.when(inner)
    def _():
        for j in (2, 3):
            z_start(0, j, 1)

    for h in range(heads):
        mix_arrival(2, h).wait_recv()
        mix_forward(h).start()
    pump(PUMPS[1])
    for k in (1, 2, 3):
        w_arrival(k).wait_recv()
        if k != 2:
            for h in range(heads):
                mix_arrival(k, h).wait_recv()
        attn = attn + jnp.dot(
            y_all[tp_at(k)], wcols[tp_at(k)], preferred_element_type=F32
        )
    squares = squares_out[...]
    for k in range(1, m):
        square_copy(k).wait_recv()
        squares = squares + squares_in[k - 1]
    fetch(resid_ref).wait()
    inverse = lax.rsqrt(to_columns(squares)[:, 0:1] / (heads * DH * m) + EPS)
    first = (resid_ref[...].astype(F32) + attn * inverse).astype(BF16)
    first_ref[...] = first
    first = first.astype(F32)

    def plane(bit):
        return p + bit * (1 - 2 * p)

    def rows_of(bit):
        return pl.ds(pl.multiple_of(plane(bit) * rows, rows), rows)

    normed[rows_of(0), here] = (first * mixer_gain_ref[...].astype(F32)[None, :]).astype(BF16)

    def group_at(bits):
        return (sp + (bits // 4) * (partner - sp), tp_at(bits % 4))

    def normed_block(bits):
        return normed.at[rows_of(bits // 4), cols_of(tp_at(bits % 4))]

    def normed_copy(source, flip):
        block = normed_block(source)
        rel = source + flip - 1
        return remote(block, block, normed_send.at[rel], normed_recv.at[rel], group_at(flip))

    def normed_arrival(rel):
        block = normed_block(rel)
        return remote(
            block, block, normed_send.at[rel - 1], normed_recv.at[rel - 1], group_at(rel % 2 or rel)
        )

    routes = ((0, 2), (0, 4), (0, 1), (2, 1), (4, 2), (4, 1), (6, 1))
    sums_out[0] = to_rows(jnp.sum(first * first, axis=1, keepdims=True))

    def sums_copy(k):
        return remote(
            sums_out.at[k // 4],
            sums_in.at[k - 1],
            sums_send.at[k - 1],
            sums_recv.at[k - 1],
            group_at(k),
        )

    for k in range(1, m):
        sums_copy(k).start()
    for route in routes[:3]:
        normed_copy(*route).start()
    total = sums_out[0]
    for k in range(1, m):
        sums_copy(k).wait_recv()
        total = total + sums_in[k - 1]
    sums_out[1] = total
    sums_copy(4).start()

    @pl.when(jnp.logical_not(inner))
    def _():
        z_start(0, 2, 1)

    y_start(1, 0)
    pump(PUMPS[2])
    normed_arrival(2).wait_recv()
    normed_copy(2, 1).start()
    normed_arrival(4).wait_recv()
    normed_copy(4, 2).start()
    normed_copy(4, 1).start()
    normed_arrival(1).wait_recv()
    normed_arrival(3).wait_recv()
    pump(ups - 1)

    @pl.when(inner)
    def _():
        for j in (2, 3):
            z_start(1, j, 0)

    pump(ups)

    z_start(1, 1, 0)

    @pl.when(jnp.logical_not(inner))
    def _():
        z_start(1, 2, 0)

    y_start(1, 1)
    for i in range(n // 2):
        for piece in range(CHUNKS * SUBS):
            y_arrival(0, i, piece).wait_recv()

    tile = min(own_width, 256)

    def up_half(bit, line_sums):
        scale = lax.rsqrt(to_columns(line_sums)[:, 0:1] / (width * m) + EPS)

        def up_tile(t, carry):
            cols = pl.ds(pl.multiple_of(t * tile, tile), tile)
            raw = jnp.dot(normed[rows_of(bit), :], up_all[:, cols], preferred_element_type=F32)
            hidden = jnp.maximum(raw * scale, 0.0)
            squared[rows_of(bit), cols] = (hidden * hidden).astype(BF16)
            return carry

        lax.fori_loop(0, own_width // tile, up_tile, 0)

    up_half(0, total)
    pump(ups + 1)


    normed_arrival(6).wait_recv()
    normed_copy(6, 1).start()
    normed_arrival(5).wait_recv()
    normed_arrival(7).wait_recv()
    sums_copy(4).wait_recv()
    up_half(1, sums_in[3])
    for j in (1, 2):
        z_start(1, j, 1)

    @pl.when(inner)
    def _():
        z_start(1, 3, 1)


    pairs = [(0, piece) for piece in range(CHUNKS)] + list(down_order)
    units = [(j, side, piece) for j, piece in pairs for side in range(2)]

    def place(i):
        j, side, piece = units[i]
        owner = z_at(j)
        return owner, owner // 2, y + side * (1 - 2 * y), piece

    def sib_copy(i, bit):
        _, far_x, half, piece = place(i)
        here = pl.ds(bit * rows if isinstance(bit, int) else pl.multiple_of(bit * rows, rows), rows)
        return remote(
            parts.at[i, here],
            sib_in.at[far_x, half, piece, here],
            sib_send.at[far_x, half, piece, bit],
            sib_recv.at[far_x, half, piece, bit],
            (sp, tp_at(1)),
        )

    def x_copy(i, cross):
        _, far_x, half, piece = place(i)
        late = cross == 1 and units[i][0] > 1
        return remote(
            comb.at[far_x, half, piece, rows_of(cross)],
            diag_in.at[half, piece] if late else x_in.at[half, piece, rows_of(cross)],
            x_send.at[half, piece, cross],
            diag_recv.at[half, piece] if late else x_recv.at[half, piece, cross],
            (partner if late else sp, tp_at(2)),
        )

    def last_copy(i):
        _, far_x, half, piece = place(i)
        late = units[i][0] > 1
        return remote(
            comb.at[far_x, half, piece, rows_of(1)] if late else last_out.at[half, piece],
            last_in.at[half, piece],
            last_send.at[half, piece],
            last_recv.at[half, piece],
            (partner, tp),
        )

    def down_units(*which):
        deep = [down_all[2 * place(i)[0] + place(i)[2], place(i)[3]] for i in which]
        deep = jnp.concatenate(deep, axis=1)
        for bit in range(2):
            here = slice(bit * rows, (bit + 1) * rows)
            wide = jnp.dot(squared[here, :], deep, preferred_element_type=F32).astype(BF16)
            for k, i in enumerate(which):
                parts[i, here, :] = wide[:, k * down_piece : (k + 1) * down_piece]
        for i in which:

            @pl.when(place(i)[0] % 2 != c)
            def _():
                for bit in range(2):
                    sib_copy(i, bit).start()

    def combine(i):
        owner, far_x, half, piece = place(i)

        @pl.when(owner % 2 == c)
        def _():
            for cross in (1, 0):
                here = rows_of(cross)
                sib_copy(i, plane(cross)).wait_recv()
                comb[far_x, half, piece, here, :] = (
                    parts[i, here, :].astype(F32)
                    + sib_in[far_x, half, piece, here, :].astype(F32)
                ).astype(BF16)

                @pl.when(far_x != x)
                def _():
                    x_copy(i, cross).start()

                if cross == 1 and units[i][0] > 1:

                    @pl.when(far_x == x)
                    def _():
                        last_copy(i).start()

    def settle(i):
        owner, far_x, half, piece = place(i)

        @pl.when(owner == tp)
        def _():
            x_copy(i, 1).wait_recv()
            last_out[half, piece] = (
                comb[far_x, half, piece, rows_of(1), :].astype(F32)
                + x_in[half, piece, rows_of(1), :].astype(F32)
            ).astype(BF16)
            last_copy(i).start()

    waiting = []
    for k, (j, piece) in enumerate(pairs):
        relay_when(z + 1 < lines, LEADS.get(k))
        relay_when(z + 1 == lines, FAR_LEADS.get(k))
        ready = (2 * k, 2 * k + 1)
        if k >= SINGLES:
            down_units(ready[0])
            combine(ready[0])
        relay_when(z + 1 == lines, FAR_MIDS.get(k))
        if k in SETTLES:
            settle(2 * SETTLES[k])
            settle(2 * SETTLES[k] + 1)
        for i in range(SUBS):
            y_arrival(1, j, SUBS * piece + i).wait_recv()
        down_units(*ready[1 if k >= SINGLES else 0 :])
        for i in waiting:
            combine(i)
        waiting = list(ready) if k < 2 else []
        if k >= 2:
            for i in ready[1 if k >= SINGLES else 0 :]:
                combine(i)
        relay_when(z + 1 == lines, FAR_TRAILS.get(k))
    for i in waiting:
        combine(i)

    def store(half, piece):
        start = half * depth + piece * down_piece
        cols = pl.ds(start, down_piece)
        return pltpu.make_async_copy(
            out_ref.at[:, cols], out_hbm.at[:, cols], store_sem.at[half, piece]
        )

    for half in range(2):
        for piece in range(CHUNKS):
            start = half * depth + piece * down_piece
            cols = slice(start, start + down_piece)
            total = first_ref[:, cols].astype(F32)
            total = total + comb[x, half, piece, rows_of(0), :].astype(F32)

            def landed(ref, send_sem, recv_sem):
                remote(ref, ref, send_sem, recv_sem, (partner, tp)).wait_recv()
                return ref[...].astype(F32)

            total = total + landed(
                x_in.at[half, piece, rows_of(0)],
                x_send.at[half, piece, 0],
                x_recv.at[half, piece, 0],
            )
            total = total + landed(
                last_in.at[half, piece], last_send.at[half, piece], last_recv.at[half, piece]
            )

            @pl.when(x != z // 2)
            def _():
                landed(
                    diag_in.at[half, piece], x_send.at[half, piece, 0], diag_recv.at[half, piece]
                )

            total = total + diag_in[half, piece].astype(F32)
            out_ref[:, cols] = total.astype(BF16)
            store(half, piece).start()

    for k in range(1, m):
        w_copy(k).wait_send()
        square_copy(k).wait_send()
        for h in range(heads):
            (mix_copy(k, h) if k < 3 else mix_forward(h)).wait_send()
    for k in range(1, m + 1):
        sums_copy(k).wait_send()
    for route in routes:
        normed_copy(*route).wait_send()
    for stream in range(2):
        for piece in range(CHUNKS * SUBS):
            for j in range(1, 3):
                z_copy(stream, j, piece).wait_send()

            @pl.when(inner)
            def _():
                z_copy(stream, 3, piece).wait_send()
                z_forward(stream, piece).wait_send()

            for i in range(n // 2):
                y_copy(stream, i, piece).wait_send()
    for copy in near_copies():
        copy.wait_send()
    for k in range(1, back + 1):

        @pl.when(z + k < lines)
        def _():
            for copy in state_copies(k):
                copy.wait_send()

    for i in range(len(units)):
        owner = place(i)[0]

        @pl.when(owner % 2 != c)
        def _():
            for bit in range(2):
                sib_copy(i, bit).wait_send()

        @pl.when((owner % 2 == c) & (place(i)[1] != x))
        def _():
            for cross in range(2):
                x_copy(i, cross).wait_send()

        @pl.when(owner == tp)
        def _():
            last_copy(i).wait_send()

    for half in range(2):
        for piece in range(CHUNKS):
            store(half, piece).wait()


PUMPS = (1, 2, 4, 2, 3)
LEADS = {2: (2, 3), 3: (4, 5), 4: (6, 7), 5: (8, 9), 6: (10, 11)}
FAR_LEADS = {2: (2, 3)}
SETTLES = {3: 0, 4: 1, 5: 2, 7: 5}
FAR_MIDS = {3: (6, 7), 4: (8, 9), 6: (10,)}
FAR_TRAILS = {3: (4, 5), 6: (11,)}
SINGLES = 3


def fused(
    n,
    m,
    queries,
    keys,
    values,
    output_gate_logits,
    input_gate_log,
    forget_gate_logits,
    extra_decay_log,
    document,
    residual,
    cell_norm_gain,
    output_weight,
    mixer_norm_gain,
    up_weight,
    down_weight,
):
    rows, heads = queries.shape[0], queries.shape[1] // DH
    depth, hidden_width = up_weight.shape
    width = residual.shape[1]
    own_width = hidden_width // 2
    lines = n // 2
    back = min(lines - 1, ((MOST - 2) // rows + 2) // 2)
    dma = pltpu.SemaphoreType.DMA
    near, far = pltpu.VMEM, pl.ANY
    spaces = [far] * 4 + [near] * 4 + [far, near, near, far, far, far]
    return pl.pallas_call(
        functools.partial(layer_kernel, n, m, back),
        out_shape=jax.ShapeDtypeStruct((rows, width), BF16),
        in_specs=[pl.BlockSpec(memory_space=space) for space in spaces],
        out_specs=pl.BlockSpec(memory_space=pl.ANY),
        scratch_shapes=[
            pltpu.VMEM(keys.shape, BF16),
            pltpu.VMEM(values.shape, BF16),
            pltpu.VMEM(up_weight.shape, BF16),
            pltpu.VMEM(queries.shape, BF16),
            pltpu.VMEM(output_weight.shape, BF16),
            pltpu.VMEM(down_weight.shape, BF16),
            pltpu.VMEM(output_gate_logits.shape, BF16),
            pltpu.VMEM(residual.shape, BF16),
            pltpu.VMEM((rows, width), BF16),
            pltpu.VMEM((n * depth, own_width), BF16),
            pltpu.VMEM((n, CHUNKS, own_width, depth // CHUNKS), BF16),
            pltpu.VMEM((m, heads * DH, width), BF16),
            pltpu.VMEM((heads, DH, DH), BF16),
            pltpu.VMEM((heads, DH, DH), BF16),
            pltpu.VMEM((heads, DH, DH), BF16),
            pltpu.VMEM((back, heads, DH, DH), BF16),
            pltpu.VMEM((heads, 8, DH), F32),
            pltpu.VMEM((heads, 8, DH), F32),
            pltpu.VMEM((heads, 8, DH), F32),
            pltpu.VMEM((back, heads, 8, DH), F32),
            pltpu.VMEM((heads, rows, DH), F32),
            pltpu.VMEM((m, rows, heads * DH), BF16),
            pltpu.VMEM((8, rows), F32),
            pltpu.VMEM((m - 1, 8, rows), F32),
            pltpu.VMEM((rows, width), BF16),
            pltpu.VMEM((2 * rows, m * width), BF16),
            pltpu.VMEM((2, 8, rows), F32),
            pltpu.VMEM((m, 8, rows), F32),
            pltpu.VMEM((2 * rows, own_width), BF16),
            pltpu.VMEM((n * CHUNKS, 2 * rows, depth // CHUNKS), BF16),
            pltpu.VMEM((2, 2, CHUNKS, 2 * rows, depth // CHUNKS), BF16),
            pltpu.VMEM((2, 2, CHUNKS, 2 * rows, depth // CHUNKS), BF16),
            pltpu.VMEM((2, CHUNKS, 2 * rows, depth // CHUNKS), BF16),
            pltpu.VMEM((2, CHUNKS, rows, depth // CHUNKS), BF16),
            pltpu.VMEM((2, CHUNKS, rows, depth // CHUNKS), BF16),
            pltpu.VMEM((2, CHUNKS, rows, depth // CHUNKS), BF16),
            dma((m - 1,)),
            dma((m - 1,)),
            dma((2, lines - 1, CHUNKS * SUBS)),
            dma((2, lines - 1, CHUNKS * SUBS)),
            dma((2, CHUNKS * SUBS)),
            dma((2, lines, CHUNKS * SUBS)),
            dma((2, lines, CHUNKS * SUBS)),
            dma((2,)),
            dma((2,)),
            dma((back, 2)),
            dma((back, 2)),
            dma((m - 1, heads)),
            dma((m - 1, heads)),
            dma((m - 1,)),
            dma((m - 1,)),
            dma((2 * m - 1,)),
            dma((2 * m - 1,)),
            dma((m,)),
            dma((m,)),
            dma((2, 2, CHUNKS, 2)),
            dma((2, 2, CHUNKS, 2)),
            dma((2, CHUNKS, 2)),
            dma((2, CHUNKS, 2)),
            dma((2, CHUNKS)),
            dma((2, CHUNKS)),
            dma((2, CHUNKS)),
            dma((8,)),
            dma((2, CHUNKS)),
        ],
        compiler_params=pltpu.CompilerParams(
            collective_id=0, has_side_effects=True, vmem_limit_bytes=60 * 1024 * 1024
        ),
        name="layer",
    )(
        queries,
        keys,
        values,
        output_gate_logits,
        forget_gate_logits.T,
        extra_decay_log.T,
        input_gate_log.T,
        document[None, :],
        residual,
        cell_norm_gain,
        mixer_norm_gain,
        output_weight,
        up_weight,
        down_weight,
    )


def either(n, m, *args):
    depth, hidden_width = args[12].shape
    heads = args[0].shape[1] // DH
    fits = n == 8 and m == 4 and depth % 128 == 0 and hidden_width % 512 == 0
    fits = fits and 3 * heads <= 8 and args[8].shape[1] == 2 * depth
    fits = fits and args[0].shape[0] % 256 == 0
    if fits:
        return fused(n, m, *args)
    return local(*args)


def solution(mesh):
    in_specs = (
        P("sp", "tp"),
        P("sp", "tp"),
        P("sp", "tp"),
        P("sp", "tp"),
        P("sp", "tp"),
        P("sp", "tp"),
        P("sp", "tp"),
        P("sp"),
        P("sp", "tp"),
        P("tp"),
        P("tp", None),
        P("tp"),
        P("sp", "tp"),
        P("tp", "sp"),
    )
    out_specs = P("sp", "tp")
    body = functools.partial(either, mesh.shape["sp"], mesh.shape["tp"])
    return jax.shard_map(body, mesh=mesh, in_specs=in_specs, out_specs=out_specs, check_vma=False)
```

```python
import functools

import jax
import jax.numpy as jnp
from jax import lax
from jax.experimental import pallas as pl
from jax.experimental.pallas import tpu as pltpu
from jax.sharding import PartitionSpec as P

DH = 128
BLOCK = 128
MOST = 2048


NEG = -1e30
EPS = 1e-06
HIGH = lax.Precision.HIGHEST


def carried_in(value, axis, join, neutral):
    count, mine = (lax.axis_size(axis), lax.axis_index(axis))
    pieces = jax.tree.map(lambda part: lax.all_gather(part, axis), value)
    subtotal = jax.tree.map(
        lambda part, zero: jnp.full_like(part, 0) + jnp.asarray(zero, part.dtype), value, neutral
    )

    def step(position, subtotal):
        longer = join(subtotal, jax.tree.map(lambda part: part[position], pieces))
        return jax.tree.map(lambda new, old: jnp.where(position < mine, new, old), longer, subtotal)

    return lax.fori_loop(0, count - 1, step, subtotal)


def block_terms(carry, inputs):
    memory, normer, stabil, last_doc = carry
    q_blk, k_blk, v_blk, gate_in, gate_log, doc_blk = inputs
    length = doc_blk.shape[0]
    causal = jnp.arange(length)[:, None] >= jnp.arange(length)[None, :]
    cumulative = jnp.cumsum(gate_log, axis=-1)
    same_doc = (doc_blk[:, None] == doc_blk[None, :]) & causal
    pair_log = cumulative[:, :, None] - cumulative[:, None, :] + gate_in[:, None, :]
    pair_log = jnp.where(same_doc[None], pair_log, NEG)
    live_rows = doc_blk == last_doc
    carried_log = jnp.where(live_rows[None, :], cumulative + stabil[:, None], NEG)
    peak_log = jnp.maximum(carried_log, jnp.max(pair_log, axis=-1))
    weights = jnp.exp(pair_log - peak_log[:, :, None])
    carried = jnp.exp(carried_log - peak_log)
    scores = jnp.einsum("htd,hsd->hts", q_blk, k_blk, precision=HIGH) * weights
    numerator = carried[:, :, None] * jnp.einsum("htd,hde->hte", q_blk, memory, precision=HIGH)
    numerator = numerator + jnp.einsum("hts,hse->hte", scores, v_blk, precision=HIGH)
    denominator = carried * jnp.einsum("htd,hd->ht", q_blk, normer, precision=HIGH) + jnp.sum(
        scores, axis=-1
    )
    end_doc = doc_blk[-1]
    end_cum = cumulative[:, -1]
    keep_log = jnp.where(
        (doc_blk == end_doc)[None, :], end_cum[:, None] - cumulative + gate_in, NEG
    )
    old_log = jnp.where(last_doc == end_doc, end_cum + stabil, NEG)
    new_stab = jnp.maximum(old_log, jnp.max(keep_log, axis=-1))
    scaled = jnp.exp(keep_log - new_stab[:, None])
    decayed = jnp.exp(old_log - new_stab)
    memory = decayed[:, None, None] * memory + jnp.einsum(
        "hs,hsd,hse->hde", scaled, k_blk, v_blk, precision=HIGH
    )
    normer = decayed[:, None] * normer + jnp.einsum("hs,hsd->hd", scaled, k_blk, precision=HIGH)
    return ((memory, normer, new_stab, end_doc), (numerator, denominator, peak_log, cumulative))


def split_heads(source, blocks):
    return source.astype(jnp.float32).reshape(blocks, BLOCK, -1, DH).transpose(0, 2, 1, 3)


def split_gates(source, blocks):
    return source.reshape(blocks, BLOCK, -1).transpose(0, 2, 1)


def within_block_pass(
    queries, keys, values, input_gate_log, forget_gate_logits, extra_decay_log, document
):
    blocks = queries.shape[0] // BLOCK
    head_count = queries.shape[1] // DH
    query_heads = split_heads(queries, blocks) * DH ** (-0.5)
    forget_log_values = jax.nn.log_sigmoid(forget_gate_logits) + extra_decay_log
    inputs = (
        query_heads,
        split_heads(keys, blocks),
        split_heads(values, blocks),
        split_gates(input_gate_log, blocks),
        split_gates(forget_log_values, blocks),
        document.reshape(blocks, BLOCK),
    )
    initial = (
        jnp.zeros((head_count, DH, DH), jnp.float32),
        jnp.zeros((head_count, DH), jnp.float32),
        jnp.full((head_count,), NEG, jnp.float32),
        jnp.array(-1, jnp.int32),
    )
    final_state, output_rows = lax.scan(block_terms, initial, inputs)
    return (query_heads, final_state, output_rows)


def head_mix(cell_out, output_gate_logits, cell_norm_gain):
    row_count = output_gate_logits.shape[0]
    head_count = cell_out.shape[1]
    hidden = cell_out.transpose(0, 2, 1, 3).reshape(row_count, head_count * DH)
    squares = lax.psum(jnp.sum(hidden * hidden, axis=1), "tp")
    inverse = lax.rsqrt(squares / (head_count * DH * lax.axis_size("tp")) + EPS)
    gated = jax.nn.sigmoid(output_gate_logits.astype(jnp.float32))
    gains = cell_norm_gain.astype(jnp.float32)
    return (gated * hidden * inverse[:, None] * gains[None, :]).astype(jnp.bfloat16)


def join_states(earlier, later):
    mem_a, norm_a, stab_a, log_a, first_a, last_a = earlier
    mem_b, norm_b, stab_b, log_b, first_b, last_b = later
    joined = last_a == last_b
    stab_ab = jnp.where(joined, jnp.maximum(log_b + stab_a, stab_b), stab_b)
    weight_a = jnp.where(joined, jnp.exp(log_b + stab_a - stab_ab), 0.0)
    weight_b = jnp.exp(stab_b - stab_ab)
    memory = weight_a[:, None, None] * mem_a + weight_b[:, None, None] * mem_b
    normer = weight_a[:, None] * norm_a + weight_b[:, None] * norm_b
    blank_b = last_b < 0
    memory = jnp.where(blank_b, mem_a, memory)
    normer = jnp.where(blank_b, norm_a, normer)
    stabil = jnp.where(blank_b, stab_a, stab_ab)
    first_doc = jnp.where(first_a < 0, first_b, first_a)
    last_doc = jnp.where(blank_b, last_a, last_b)
    return (memory, normer, stabil, log_a + log_b, first_doc, last_doc)


def local(
    queries,
    keys,
    values,
    output_gate_logits,
    input_gate_log,
    forget_gate_logits,
    extra_decay_log,
    document,
    residual,
    cell_norm_gain,
    output_weight,
    mixer_norm_gain,
    up_weight,
    down_weight,
):
    query_heads, final_state, output_rows = within_block_pass(
        queries, keys, values, input_gate_log, forget_gate_logits, extra_decay_log, document
    )
    numerator, denominator, peak_log, cumulative = output_rows
    memory, normer, stabil, last_doc = final_state
    step_logs = cumulative[:, :, -1]
    offsets = jnp.cumsum(step_logs, axis=0) - step_logs
    through = cumulative + offsets[:, :, None]
    summary = (memory, normer, stabil, jnp.sum(step_logs, axis=0), document[0], last_doc)
    identity = (
        jnp.zeros_like(memory),
        jnp.zeros_like(normer),
        jnp.full_like(stabil, NEG),
        jnp.zeros_like(stabil),
        jnp.array(-1, jnp.int32),
        jnp.array(-1, jnp.int32),
    )
    prefix = carried_in(summary, "sp", join_states, identity)
    doc_blocks = document.reshape(-1, BLOCK)
    carried_log = jnp.where(
        (doc_blocks == prefix[5])[:, None, :], through + prefix[2][None, :, None], NEG
    )
    merged_peak = jnp.maximum(peak_log, carried_log)
    own_weight = jnp.exp(peak_log - merged_peak)
    far_weight = jnp.exp(carried_log - merged_peak)
    numerator = own_weight[..., None] * numerator + far_weight[..., None] * jnp.einsum(
        "nhtd,hde->nhte", query_heads, prefix[0], precision=HIGH
    )
    denominator = own_weight * denominator + far_weight * jnp.einsum(
        "nhtd,hd->nht", query_heads, prefix[1], precision=HIGH
    )
    cell_out = numerator / jnp.maximum(jnp.abs(denominator), 1.0)[..., None]
    mixed = head_mix(cell_out, output_gate_logits, cell_norm_gain)
    head_terms = jnp.dot(mixed, output_weight, preferred_element_type=jnp.float32)
    width = residual.shape[1]
    model_width = width * lax.axis_size("tp")
    own_sum = lax.psum_scatter(
        head_terms.astype(jnp.bfloat16), "tp", scatter_dimension=1, tiled=True
    ).astype(jnp.float32)
    first_sum = (residual.astype(jnp.float32) + own_sum).astype(jnp.bfloat16)
    first_wide = lax.optimization_barrier(first_sum).astype(jnp.float32)
    squares = lax.psum(jnp.sum(first_wide * first_wide, axis=1), "tp")
    inverse = lax.rsqrt(squares / model_width + EPS)
    normed_own = (first_wide * inverse[:, None] * mixer_norm_gain.astype(jnp.float32)).astype(
        jnp.bfloat16
    )
    normed_full = lax.all_gather(normed_own, "tp", axis=1, tiled=True)
    hidden = jnp.dot(
        normed_full,
        lax.all_gather(up_weight, "sp", axis=0, tiled=True),
        preferred_element_type=jnp.float32,
    )
    squared = jnp.square(jax.nn.relu(hidden)).astype(jnp.bfloat16)
    channel = jnp.dot(
        squared,
        lax.all_gather(down_weight, "sp", axis=1, tiled=True),
        preferred_element_type=jnp.float32,
    )
    own_channel = lax.psum_scatter(
        channel.astype(jnp.bfloat16), "tp", scatter_dimension=1, tiled=True
    ).astype(jnp.float32)
    return (lax.optimization_barrier(first_sum).astype(jnp.float32) + own_channel).astype(
        jnp.bfloat16
    )


MESH = pl.DeviceIdType.MESH
F32 = jnp.float32
BF16 = jnp.bfloat16
CHUNKS = 2
SUBS = 2


def to_columns(rows):
    pad = jnp.zeros((128 - rows.shape[0], rows.shape[1]), F32)
    return jnp.transpose(jnp.concatenate([rows, pad], axis=0))


def to_rows(column):
    return jnp.transpose(jnp.broadcast_to(column, (column.shape[0], 128)))[0:8, :]


def halves(wide):
    high = wide.astype(BF16)
    return high, (wide - high.astype(F32)).astype(BF16)


def two_pass(wide, narrow):
    high, low = halves(wide)
    return jnp.dot(high, narrow, preferred_element_type=F32) + jnp.dot(
        low, narrow, preferred_element_type=F32
    )


def layer_kernel(
    n,
    m,
    back,
    q_hbm,
    k_hbm,
    v_hbm,
    og_hbm,
    forget_ref,
    extra_ref,
    input_ref,
    doc_ref,
    resid_hbm,
    cell_gain_ref,
    mixer_gain_ref,
    wout_hbm,
    up_hbm,
    down_hbm,
    out_hbm,
    k_ref,
    v_ref,
    up_ref,
    q_ref,
    wout_ref,
    down_ref,
    og_ref,
    resid_ref,
    out_ref,
    up_all,
    down_all,
    wcols,
    state_out,
    near_state,
    pair_state,
    state_in,
    tail_out,
    near_tail,
    pair_tail,
    tail_in,
    numer_ref,
    y_all,
    squares_out,
    squares_in,
    first_ref,
    normed,
    sums_out,
    sums_in,
    squared,
    parts,
    sib_in,
    comb,
    x_in,
    last_out,
    last_in,
    diag_in,
    w_send,
    w_recv,
    z_send,
    z_recv,
    relay_send,
    y_send,
    y_recv,
    near_send,
    near_recv,
    state_send,
    state_recv,
    mix_send,
    mix_recv,
    squares_send,
    squares_recv,
    normed_send,
    normed_recv,
    sums_send,
    sums_recv,
    sib_send,
    sib_recv,
    x_send,
    x_recv,
    diag_recv,
    last_send,
    last_recv,
    load_sem,
    store_sem,
):
    loads = (
        (up_hbm, up_ref),
        (k_hbm, k_ref),
        (v_hbm, v_ref),
        (wout_hbm, wout_ref),
        (q_hbm, q_ref),
        (down_hbm, down_ref),
        (og_hbm, og_ref),
        (resid_hbm, resid_ref),
    )

    def fetch(ref):
        at = [dst is ref for _, dst in loads].index(True)
        return pltpu.make_async_copy(*loads[at], load_sem.at[at])

    for _, ref in loads:
        fetch(ref).start()
    sp, tp = lax.axis_index("sp"), lax.axis_index("tp")
    rows, heads = q_ref.shape[0], q_ref.shape[1] // DH
    depth, hidden_width = up_ref.shape
    own_width = hidden_width // 2
    width = resid_ref.shape[1]
    up_piece, down_piece = depth // (CHUNKS * SUBS), depth // CHUNKS
    deep_piece = own_width // SUBS
    z, y, lines = sp // 2, sp % 2, n // 2
    p, x, c = z % 2, tp // 2, tp % 2

    def z_at(j):
        return (z, z + 1 - 2 * p, z + 2 - 4 * (z // 2), n // 2 - 1 - z)[j]

    def tp_at(bits):
        far_c = c + (bits % 2) * (1 - 2 * c)
        far_x = x + ((bits // 2) % 2) * (1 - 2 * x)
        return 2 * far_x + far_c

    partner = 2 * z_at(1) + y
    beside = 2 * z + 1 - y

    barrier = pltpu.get_barrier_semaphore()
    for k in range(1, n):
        pl.semaphore_signal(barrier, device_id=((sp + k) % n, tp), device_id_type=MESH)
    for k in range(1, m):
        pl.semaphore_signal(barrier, device_id=(sp, (tp + k) % m), device_id_type=MESH)
    pl.semaphore_signal(barrier, device_id=(partner, tp_at(2)), device_id_type=MESH)
    pl.semaphore_wait(barrier, n + m - 1)

    def remote(src, dst, send_sem, recv_sem, device):
        return pltpu.make_async_remote_copy(
            src_ref=src,
            dst_ref=dst,
            send_sem=send_sem,
            recv_sem=recv_sem,
            device_id=device,
            device_id_type=MESH,
        )

    def cols_of(owner):
        return pl.ds(pl.multiple_of(owner * width, width), width)

    def w_copy(k):
        return remote(
            wout_ref.at[:, cols_of(tp_at(k))],
            wcols.at[tp],
            w_send.at[k - 1],
            w_recv.at[k - 1],
            (sp, tp_at(k)),
        )

    def w_arrival(k):
        there = wcols.at[tp_at(k)]
        return remote(there, there, w_send.at[k - 1], w_recv.at[k - 1], (sp, tp_at(k)))

    def slot(stream, block, piece):
        if stream == 0:
            start = pl.multiple_of(block * depth + piece * up_piece, up_piece)
            return up_all.at[pl.ds(start, up_piece), :]
        deep = pl.ds(piece % SUBS * deep_piece, deep_piece)
        return down_all.at[block, piece // SUBS, deep]

    def own_piece(stream, half, piece):
        if stream == 0:
            lanes = pl.ds(pl.multiple_of(half * own_width, own_width), own_width)
            return up_ref.at[pl.ds(piece * up_piece, up_piece), lanes]
        start = pl.multiple_of(half * own_width + piece % SUBS * deep_piece, deep_piece)
        cols = pl.ds(piece // SUBS * down_piece, down_piece)
        return down_ref.at[pl.ds(start, deep_piece), cols]

    def z_copy(stream, j, piece):
        return remote(
            own_piece(stream, z_at(j) % 2, piece),
            slot(stream, sp, piece),
            z_send.at[stream, j - 1, piece],
            z_recv.at[stream, j - 1, piece],
            (2 * z_at(j) + y, tp),
        )

    inner = p + z // 2 == 1

    def z_forward(stream, piece):
        there = slot(stream, 2 * z_at(1) + y, piece)
        return remote(
            there,
            there,
            relay_send.at[stream, piece],
            z_recv.at[stream, 2, piece],
            (2 * z_at(2) + y, tp),
        )

    def z_arrival(stream, j, piece):
        there = slot(stream, 2 * z_at(j) + y, piece)
        return remote(
            there,
            there,
            z_send.at[stream, j - 1, piece],
            z_recv.at[stream, j - 1, piece],
            (2 * z_at(j) + y, tp),
        )

    def y_copy(stream, i, piece):
        there = slot(stream, 2 * z_at(i) + y, piece)
        return remote(
            own_piece(stream, p, piece) if i == 0 else there,
            there,
            y_send.at[stream, i, piece],
            y_recv.at[stream, i, piece],
            (beside, tp),
        )

    def y_arrival(stream, i, piece):
        there = slot(stream, 2 * z_at(i) + 1 - y, piece)
        return remote(
            there,
            there,
            y_send.at[stream, i, piece],
            y_recv.at[stream, i, piece],
            (beside, tp),
        )

    order = ((1, 0), (1, 1), (2, 0), (3, 0), (2, 1), (3, 1))
    down_order = ((1, 0), (2, 0), (3, 0), (1, 1), (2, 1), (3, 1))
    events = [
        (stream, j, SUBS * piece + i)
        for stream in range(2)
        for j, piece in (order, down_order)[stream]
        for i in range(SUBS)
    ]

    def z_start(stream, j, piece):
        for i in range(SUBS):
            z_copy(stream, j, SUBS * piece + i).start()

    def y_start(stream, piece):
        for i in range(SUBS):
            y_copy(stream, 0, SUBS * piece + i).start()

    done = [0]

    def relay(event):
        stream, j, piece = events[event]
        z_arrival(stream, j, piece).wait_recv()
        y_copy(stream, j, piece).start()
        if j == 1:

            @pl.when(inner)
            def _():
                z_forward(stream, piece).start()

    def pump(until):
        while done[0] < min(SUBS * until, len(events)):
            event = done[0]
            relay(event)
            done[0] += 1

    def relay_when(condition, down_events):
        if down_events:

            @pl.when(condition)
            def _():
                for event in down_events:
                    relay(SUBS * ups + event)

    ups = len(order)

    fetch(up_ref).wait()
    z_start(0, 1, 0)

    @pl.when(inner)
    def _():
        z_start(0, 3, 0)

    fetch(wout_ref).wait()
    for k in range(1, m):
        w_copy(k).start()

    document = doc_ref[...].astype(F32)
    across = lax.broadcasted_iota(jnp.int32, (rows, rows), 1)
    along = lax.broadcasted_iota(jnp.int32, (rows, rows), 0)
    upper = (along <= across).astype(BF16)
    forget = jax.nn.log_sigmoid(forget_ref[...]) + extra_ref[...]
    high = forget.astype(BF16).astype(F32)
    middle = (forget - high).astype(BF16).astype(F32)
    low = forget - high - middle
    slab = lax.broadcasted_iota(jnp.int32, (8, rows), 0)
    split = jnp.zeros((8, rows), F32)
    for h in range(heads):
        for i, part in enumerate((high, middle, low)):
            split = jnp.where(slab == heads * i + h, part[h : h + 1, :], split)
    summed = jnp.dot(split.astype(BF16), upper, preferred_element_type=F32)
    last_doc = document[:, rows - 1 : rows]
    sums, entry, totals, stabs, scaled = [], [], [], [], []
    for h in range(heads):
        line_sum = summed[h : h + 1, :]
        for i in range(1, 3):
            line_sum = line_sum + summed[heads * i + h : heads * i + h + 1, :]
        sums.append(line_sum)
        entry.append(input_ref[h : h + 1, :] - line_sum)
        total = line_sum[:, rows - 1 : rows]
        keep = jnp.where(document == last_doc, total + entry[h], NEG)
        stab = jnp.max(keep, axis=1, keepdims=True)
        totals.append(total)
        stabs.append(stab)
        scaled.append(jnp.exp(keep - stab))
    packed = jnp.broadcast_to(document, (8, rows))
    for h in range(heads):
        packed = jnp.where(slab == h, sums[h], packed)
        packed = jnp.where(slab == heads + h, scaled[h], packed)
    columns = to_columns(packed)
    doc_col = columns[:, 2 * heads : 2 * heads + 1]
    line = lax.broadcasted_iota(jnp.int32, (8, DH), 0)
    fetch(k_ref).wait()
    fetch(v_ref).wait()
    for h in range(heads):
        mine = slice(h * DH, (h + 1) * DH)
        weighted = k_ref[:, mine].astype(F32) * columns[:, heads + h : heads + h + 1]
        state_out[h] = lax.dot_general(
            weighted.astype(BF16),
            v_ref[:, mine],
            (((0,), (0,)), ((), ())),
            preferred_element_type=F32,
        ).astype(BF16)
        tail = jnp.broadcast_to(jnp.sum(weighted, axis=0, keepdims=True), (8, DH))
        tail = jnp.where(line == 1, stabs[h], tail)
        tail = jnp.where(line == 2, totals[h], tail)
        tail = jnp.where(line == 3, last_doc, tail)
        tail_out[h] = tail

    def pair_of(refs, send_sem, recv_sem, device):
        return [
            remote(src, dst, send_sem.at[i], recv_sem.at[i], device)
            for i, (src, dst) in enumerate(refs)
        ]

    def near_copies():
        refs = ((tail_out, near_tail), (state_out, near_state))
        return pair_of(refs, near_send, near_recv, (beside, tp))

    def state_copies(k):
        refs = ((pair_tail, tail_in.at[k - 1]), (pair_state, state_in.at[k - 1]))
        return pair_of(
            refs, state_send.at[k - 1], state_recv.at[k - 1], (2 * ((z + k) % lines) + y, tp)
        )

    for copy in near_copies():
        copy.start()
    for piece in range(CHUNKS):
        y_start(0, piece)

    for k in range(1, back + 1):

        @pl.when(z < k)
        def _():
            tail_in[k - 1] = jnp.zeros((heads, 8, DH), F32)
            state_in[k - 1] = jnp.zeros((heads, DH, DH), BF16)

    fetch(down_ref).wait()
    half_lanes = pl.ds(pl.multiple_of(p * own_width, own_width), own_width)
    up_all[pl.ds(pl.multiple_of(sp * depth, depth), depth), :] = up_ref[:, half_lanes]
    for piece in range(CHUNKS):
        cols = slice(piece * down_piece, (piece + 1) * down_piece)
        down_all[sp, piece] = down_ref[half_lanes, cols]

    @pl.when(x == z // 2)
    def _():
        diag_in[...] = jnp.zeros(diag_in.shape, BF16)

    fetch(q_ref).wait()
    step = min(rows, 256)
    locals_of = []
    for h in range(heads):
        mine = slice(h * DH, (h + 1) * DH)
        peaks, denoms = [], []
        for start in range(0, rows, step):
            stop = start + step
            here = slice(start, stop)
            scores = lax.dot_general(
                q_ref[here, mine],
                k_ref[0:stop, mine],
                (((1,), (1,)), ((), ())),
                preferred_element_type=F32,
            ) * (DH**-0.5)
            pair = columns[here, h : h + 1] + entry[h][:, 0:stop]
            seen = (doc_col[here] == document[:, 0:stop]) & (
                along[here, 0:stop] >= across[here, 0:stop]
            )
            pair = jnp.where(seen, pair, NEG)
            peak = jnp.max(pair, axis=1, keepdims=True)
            scores = scores * jnp.exp(pair - peak)
            numer_ref[h, here, :] = two_pass(scores, v_ref[0:stop, mine])
            peaks.append(peak)
            denoms.append(jnp.sum(scores, axis=1, keepdims=True))
        locals_of.append((jnp.concatenate(peaks, axis=0), jnp.concatenate(denoms, axis=0)))

    for copy in near_copies():
        copy.wait_recv()
    for h in range(heads):
        own_tail, far_tail = tail_out[h], near_tail[h]
        old_tail = jnp.where(y == 0, own_tail, far_tail)
        new_tail = jnp.where(y == 0, far_tail, own_tail)
        own_state, far_state = state_out[h].astype(F32), near_state[h].astype(F32)
        old_state = jnp.where(y == 0, own_state, far_state)
        new_state = jnp.where(y == 0, far_state, own_state)
        joined = old_tail[3:4, :] == new_tail[3:4, :]
        old_log = jnp.where(joined, old_tail[1:2, :] + new_tail[2:3, :], NEG)
        stab = jnp.maximum(old_log, new_tail[1:2, :])
        old_weight = jnp.where(joined, jnp.exp(old_log - stab), 0.0)
        new_weight = jnp.exp(new_tail[1:2, :] - stab)
        pair_state[h] = (
            jnp.where(joined, old_weight * old_state, 0.0) + new_weight * new_state
        ).astype(BF16)
        tail = jnp.where(joined, old_weight * old_tail, 0.0) + new_weight * new_tail
        tail = jnp.where(line == 1, stab, tail)
        tail = jnp.where(line == 2, old_tail + new_tail, tail)
        pair_tail[h] = jnp.where(line == 3, new_tail, tail)

    for k in range(1, back + 1):

        @pl.when(z + back + 1 - k < lines)
        def _():
            for copy in state_copies(back + 1 - k):
                copy.start()

    z_start(0, 1, 1)
    z_start(0, 2, 0)
    for k in range(1, back + 1):

        @pl.when(z >= k)
        def _():
            for copy in state_copies(k):
                copy.wait_recv()

    def mix_copy(k, h):
        here = y_all.at[tp, :, pl.ds(h * DH, DH)]
        return remote(
            here, here, mix_send.at[k - 1, h], mix_recv.at[k - 1, h], (sp, tp_at(k))
        )

    def mix_forward(h):
        there = y_all.at[tp_at(2), :, pl.ds(h * DH, DH)]
        return remote(there, there, mix_send.at[2, h], mix_recv.at[2, h], (sp, tp_at(1)))

    def mix_arrival(k, h):
        there = y_all.at[tp_at(k), :, pl.ds(h * DH, DH)]
        return remote(
            there, there, mix_send.at[k - 1, h], mix_recv.at[k - 1, h], (sp, tp_at(k))
        )

    fetch(og_ref).wait()
    first_doc = document[:, 0:1]
    square_sum = jnp.zeros((rows, DH), F32)
    for h in range(heads):
        mine = slice(h * DH, (h + 1) * DH)
        earlier = [(near_tail, near_state, y == 1)]
        earlier += [(tail_in.at[k], state_in.at[k], z > k) for k in range(back)]
        between = jnp.zeros((1, DH), F32)
        logs, valids = [], []
        best = jnp.full((1, DH), NEG, F32)
        for tails, _, exists in earlier:
            tail = tails[h]
            valid = (tail[3:4, :] == first_doc) & jnp.broadcast_to(exists, (1, DH))
            log = jnp.where(valid, between + tail[1:2, :], NEG)
            between = between + jnp.where(exists, tail[2:3, :], 0.0)
            best = jnp.maximum(best, log)
            logs.append(log)
            valids.append(valid)
        memory = jnp.zeros((DH, DH), F32)
        normer = jnp.zeros((1, DH), F32)
        for i, (tails, states, _) in enumerate(earlier):
            weight = jnp.where(valids[i], jnp.exp(logs[i] - best), 0.0)
            memory = memory + jnp.where(valids[i], weight * states[h].astype(F32), 0.0)
            normer = normer + jnp.where(valids[i], weight * tails[h, 0:1, :], 0.0)
        peak, denom = locals_of[h]
        carried = jnp.where(doc_col == first_doc, columns[:, h : h + 1] + best[:, 0:1], NEG)
        merged = jnp.maximum(peak, carried)
        own = jnp.exp(peak - merged)
        other = jnp.exp(carried - merged) * (DH**-0.5)
        query = q_ref[:, mine]
        high, low = halves(memory)
        reached = jnp.dot(query, high, preferred_element_type=F32) + jnp.dot(
            query, low, preferred_element_type=F32
        )
        numer = own * numer_ref[h] + other * reached
        denom = own * denom + other * jnp.sum(
            query.astype(F32) * normer, axis=1, keepdims=True
        )
        cell = numer / jnp.maximum(jnp.abs(denom), 1.0)
        square_sum = square_sum + cell * cell
        gated = jax.nn.sigmoid(og_ref[:, mine].astype(F32))
        y_all[tp, :, mine] = (gated * cell * cell_gain_ref[mine].astype(F32)[None, :]).astype(BF16)
        for k in range(1, 3):
            mix_copy(k, h).start()
    squares_out[...] = to_rows(jnp.sum(square_sum, axis=1, keepdims=True))

    def square_copy(k):
        return remote(
            squares_out,
            squares_in.at[k - 1],
            squares_send.at[k - 1],
            squares_recv.at[k - 1],
            (sp, tp_at(k)),
        )

    for k in range(1, m):
        square_copy(k).start()
    here = cols_of(tp)
    attn = jnp.dot(y_all[tp], wout_ref[:, here], preferred_element_type=F32)
    pump(PUMPS[0])

    @pl.when(inner)
    def _():
        for j in (2, 3):
            z_start(0, j, 1)

    for h in range(heads):
        mix_arrival(2, h).wait_recv()
        mix_forward(h).start()
    pump(PUMPS[1])
    for k in (1, 2, 3):
        w_arrival(k).wait_recv()
        if k != 2:
            for h in range(heads):
                mix_arrival(k, h).wait_recv()
        attn = attn + jnp.dot(
            y_all[tp_at(k)], wcols[tp_at(k)], preferred_element_type=F32
        )
    squares = squares_out[...]
    for k in range(1, m):
        square_copy(k).wait_recv()
        squares = squares + squares_in[k - 1]
    fetch(resid_ref).wait()
    inverse = lax.rsqrt(to_columns(squares)[:, 0:1] / (heads * DH * m) + EPS)
    first = (resid_ref[...].astype(F32) + attn * inverse).astype(BF16)
    first_ref[...] = first
    first = first.astype(F32)

    def plane(bit):
        return p + bit * (1 - 2 * p)

    def rows_of(bit):
        return pl.ds(pl.multiple_of(plane(bit) * rows, rows), rows)

    normed[rows_of(0), here] = (first * mixer_gain_ref[...].astype(F32)[None, :]).astype(BF16)

    def group_at(bits):
        return (sp + (bits // 4) * (partner - sp), tp_at(bits % 4))

    def normed_block(bits):
        return normed.at[rows_of(bits // 4), cols_of(tp_at(bits % 4))]

    def normed_copy(source, flip):
        block = normed_block(source)
        rel = source + flip - 1
        return remote(block, block, normed_send.at[rel], normed_recv.at[rel], group_at(flip))

    def normed_arrival(rel):
        block = normed_block(rel)
        return remote(
            block, block, normed_send.at[rel - 1], normed_recv.at[rel - 1], group_at(rel % 2 or rel)
        )

    routes = ((0, 2), (0, 4), (0, 1), (2, 1), (4, 2), (4, 1), (6, 1))
    sums_out[0] = to_rows(jnp.sum(first * first, axis=1, keepdims=True))

    def sums_copy(k):
        return remote(
            sums_out.at[k // 4],
            sums_in.at[k - 1],
            sums_send.at[k - 1],
            sums_recv.at[k - 1],
            group_at(k),
        )

    for k in range(1, m):
        sums_copy(k).start()
    for route in routes[:3]:
        normed_copy(*route).start()
    total = sums_out[0]
    for k in range(1, m):
        sums_copy(k).wait_recv()
        total = total + sums_in[k - 1]
    sums_out[1] = total
    sums_copy(4).start()

    @pl.when(jnp.logical_not(inner))
    def _():
        z_start(0, 2, 1)

    y_start(1, 0)
    pump(PUMPS[2])
    normed_arrival(2).wait_recv()
    normed_copy(2, 1).start()
    normed_arrival(4).wait_recv()
    normed_copy(4, 2).start()
    normed_copy(4, 1).start()
    normed_arrival(1).wait_recv()
    normed_arrival(3).wait_recv()
    pump(ups - 1)

    @pl.when(inner)
    def _():
        for j in (2, 3):
            z_start(1, j, 0)

    pump(ups)

    z_start(1, 1, 0)

    @pl.when(jnp.logical_not(inner))
    def _():
        z_start(1, 2, 0)

    y_start(1, 1)
    for i in range(n // 2):
        for piece in range(CHUNKS * SUBS):
            y_arrival(0, i, piece).wait_recv()

    tile = min(own_width, 256)

    def up_half(bit, line_sums):
        scale = lax.rsqrt(to_columns(line_sums)[:, 0:1] / (width * m) + EPS)

        def up_tile(t, carry):
            cols = pl.ds(pl.multiple_of(t * tile, tile), tile)
            raw = jnp.dot(normed[rows_of(bit), :], up_all[:, cols], preferred_element_type=F32)
            hidden = jnp.maximum(raw * scale, 0.0)
            squared[rows_of(bit), cols] = (hidden * hidden).astype(BF16)
            return carry

        lax.fori_loop(0, own_width // tile, up_tile, 0)

    up_half(0, total)
    pump(ups + 1)


    normed_arrival(6).wait_recv()
    normed_copy(6, 1).start()
    normed_arrival(5).wait_recv()
    normed_arrival(7).wait_recv()
    sums_copy(4).wait_recv()
    up_half(1, sums_in[3])
    for j in (1, 2):
        z_start(1, j, 1)

    @pl.when(inner)
    def _():
        z_start(1, 3, 1)


    pairs = [(0, piece) for piece in range(CHUNKS)] + list(down_order)
    units = [(j, side, piece) for j, piece in pairs for side in range(2)]

    def place(i):
        j, side, piece = units[i]
        owner = z_at(j)
        return owner, owner // 2, y + side * (1 - 2 * y), piece

    def sib_copy(i, bit):
        _, far_x, half, piece = place(i)
        here = pl.ds(bit * rows if isinstance(bit, int) else pl.multiple_of(bit * rows, rows), rows)
        return remote(
            parts.at[i, here],
            sib_in.at[far_x, half, piece, here],
            sib_send.at[far_x, half, piece, bit],
            sib_recv.at[far_x, half, piece, bit],
            (sp, tp_at(1)),
        )

    def x_copy(i, cross):
        _, far_x, half, piece = place(i)
        late = cross == 1 and units[i][0] > 1
        return remote(
            comb.at[far_x, half, piece, rows_of(cross)],
            diag_in.at[half, piece] if late else x_in.at[half, piece, rows_of(cross)],
            x_send.at[half, piece, cross],
            diag_recv.at[half, piece] if late else x_recv.at[half, piece, cross],
            (partner if late else sp, tp_at(2)),
        )

    def last_copy(i):
        _, far_x, half, piece = place(i)
        late = units[i][0] > 1
        return remote(
            comb.at[far_x, half, piece, rows_of(1)] if late else last_out.at[half, piece],
            last_in.at[half, piece],
            last_send.at[half, piece],
            last_recv.at[half, piece],
            (partner, tp),
        )

    def down_units(*which):
        deep = [down_all[2 * place(i)[0] + place(i)[2], place(i)[3]] for i in which]
        deep = jnp.concatenate(deep, axis=1)
        for bit in range(2):
            here = slice(bit * rows, (bit + 1) * rows)
            wide = jnp.dot(squared[here, :], deep, preferred_element_type=F32).astype(BF16)
            for k, i in enumerate(which):
                parts[i, here, :] = wide[:, k * down_piece : (k + 1) * down_piece]
        for i in which:

            @pl.when(place(i)[0] % 2 != c)
            def _():
                for bit in range(2):
                    sib_copy(i, bit).start()

    def combine(i):
        owner, far_x, half, piece = place(i)

        @pl.when(owner % 2 == c)
        def _():
            for cross in (1, 0):
                here = rows_of(cross)
                sib_copy(i, plane(cross)).wait_recv()
                comb[far_x, half, piece, here, :] = (
                    parts[i, here, :].astype(F32)
                    + sib_in[far_x, half, piece, here, :].astype(F32)
                ).astype(BF16)

                @pl.when(far_x != x)
                def _():
                    x_copy(i, cross).start()

                if cross == 1 and units[i][0] > 1:

                    @pl.when(far_x == x)
                    def _():
                        last_copy(i).start()

    def settle(i):
        owner, far_x, half, piece = place(i)

        @pl.when(owner == tp)
        def _():
            x_copy(i, 1).wait_recv()
            last_out[half, piece] = (
                comb[far_x, half, piece, rows_of(1), :].astype(F32)
                + x_in[half, piece, rows_of(1), :].astype(F32)
            ).astype(BF16)
            last_copy(i).start()

    waiting = []
    for k, (j, piece) in enumerate(pairs):
        relay_when(z + 1 < lines, LEADS.get(k))
        relay_when(z + 1 == lines, FAR_LEADS.get(k))
        ready = (2 * k, 2 * k + 1)
        if k >= SINGLES:
            down_units(ready[0])
            combine(ready[0])
        relay_when(z + 1 == lines, FAR_MIDS.get(k))
        if k in SETTLES:
            settle(2 * SETTLES[k])
            settle(2 * SETTLES[k] + 1)
        for i in range(SUBS):
            y_arrival(1, j, SUBS * piece + i).wait_recv()
        down_units(*ready[1 if k >= SINGLES else 0 :])
        for i in waiting:
            combine(i)
        waiting = list(ready) if k < 2 else []
        if k >= 2:
            for i in ready[1 if k >= SINGLES else 0 :]:
                combine(i)
        relay_when(z + 1 == lines, FAR_TRAILS.get(k))
    for i in waiting:
        combine(i)

    for k in range(1, m):
        w_copy(k).wait_send()
        square_copy(k).wait_send()
        for h in range(heads):
            (mix_copy(k, h) if k < 3 else mix_forward(h)).wait_send()
    for k in range(1, m + 1):
        sums_copy(k).wait_send()
    for route in routes:
        normed_copy(*route).wait_send()
    for stream in range(2):
        for piece in range(CHUNKS * SUBS):
            for j in range(1, 3):
                z_copy(stream, j, piece).wait_send()

            @pl.when(inner)
            def _():
                z_copy(stream, 3, piece).wait_send()
                z_forward(stream, piece).wait_send()

            for i in range(n // 2):
                y_copy(stream, i, piece).wait_send()
    for copy in near_copies():
        copy.wait_send()
    for k in range(1, back + 1):

        @pl.when(z + k < lines)
        def _():
            for copy in state_copies(k):
                copy.wait_send()

    def store(half, piece):
        start = half * depth + piece * down_piece
        cols = pl.ds(start, down_piece)
        return pltpu.make_async_copy(
            out_ref.at[:, cols], out_hbm.at[:, cols], store_sem.at[half, piece]
        )

    for half in range(2):
        for piece in range(CHUNKS):
            start = half * depth + piece * down_piece
            cols = slice(start, start + down_piece)
            total = first_ref[:, cols].astype(F32)
            total = total + comb[x, half, piece, rows_of(0), :].astype(F32)

            def landed(ref, send_sem, recv_sem):
                remote(ref, ref, send_sem, recv_sem, (partner, tp)).wait_recv()
                return ref[...].astype(F32)

            total = total + landed(
                x_in.at[half, piece, rows_of(0)],
                x_send.at[half, piece, 0],
                x_recv.at[half, piece, 0],
            )
            total = total + landed(
                last_in.at[half, piece], last_send.at[half, piece], last_recv.at[half, piece]
            )

            @pl.when(x != z // 2)
            def _():
                landed(
                    diag_in.at[half, piece], x_send.at[half, piece, 0], diag_recv.at[half, piece]
                )

            total = total + diag_in[half, piece].astype(F32)
            out_ref[:, cols] = total.astype(BF16)
            store(half, piece).start()

    for i in range(len(units)):
        owner = place(i)[0]

        @pl.when(owner % 2 != c)
        def _():
            for bit in range(2):
                sib_copy(i, bit).wait_send()

        @pl.when((owner % 2 == c) & (place(i)[1] != x))
        def _():
            for cross in range(2):
                x_copy(i, cross).wait_send()

        @pl.when(owner == tp)
        def _():
            last_copy(i).wait_send()

    for half in range(2):
        for piece in range(CHUNKS):
            store(half, piece).wait()


PUMPS = (1, 2, 4, 2, 3)
LEADS = {2: (2, 3), 3: (4, 5), 4: (6, 7), 5: (8, 9), 6: (10, 11)}
FAR_LEADS = {2: (2, 3)}
SETTLES = {3: 0, 4: 1, 5: 2, 7: 5}
FAR_MIDS = {3: (6, 7), 4: (8, 9), 6: (10,)}
FAR_TRAILS = {3: (4, 5), 6: (11,)}
SINGLES = 3


def fused(
    n,
    m,
    queries,
    keys,
    values,
    output_gate_logits,
    input_gate_log,
    forget_gate_logits,
    extra_decay_log,
    document,
    residual,
    cell_norm_gain,
    output_weight,
    mixer_norm_gain,
    up_weight,
    down_weight,
):
    rows, heads = queries.shape[0], queries.shape[1] // DH
    depth, hidden_width = up_weight.shape
    width = residual.shape[1]
    own_width = hidden_width // 2
    lines = n // 2
    back = min(lines - 1, ((MOST - 2) // rows + 2) // 2)
    dma = pltpu.SemaphoreType.DMA
    near, far = pltpu.VMEM, pl.ANY
    spaces = [far] * 4 + [near] * 4 + [far, near, near, far, far, far]
    return pl.pallas_call(
        functools.partial(layer_kernel, n, m, back),
        out_shape=jax.ShapeDtypeStruct((rows, width), BF16),
        in_specs=[pl.BlockSpec(memory_space=space) for space in spaces],
        out_specs=pl.BlockSpec(memory_space=pl.ANY),
        scratch_shapes=[
            pltpu.VMEM(keys.shape, BF16),
            pltpu.VMEM(values.shape, BF16),
            pltpu.VMEM(up_weight.shape, BF16),
            pltpu.VMEM(queries.shape, BF16),
            pltpu.VMEM(output_weight.shape, BF16),
            pltpu.VMEM(down_weight.shape, BF16),
            pltpu.VMEM(output_gate_logits.shape, BF16),
            pltpu.VMEM(residual.shape, BF16),
            pltpu.VMEM((rows, width), BF16),
            pltpu.VMEM((n * depth, own_width), BF16),
            pltpu.VMEM((n, CHUNKS, own_width, depth // CHUNKS), BF16),
            pltpu.VMEM((m, heads * DH, width), BF16),
            pltpu.VMEM((heads, DH, DH), BF16),
            pltpu.VMEM((heads, DH, DH), BF16),
            pltpu.VMEM((heads, DH, DH), BF16),
            pltpu.VMEM((back, heads, DH, DH), BF16),
            pltpu.VMEM((heads, 8, DH), F32),
            pltpu.VMEM((heads, 8, DH), F32),
            pltpu.VMEM((heads, 8, DH), F32),
            pltpu.VMEM((back, heads, 8, DH), F32),
            pltpu.VMEM((heads, rows, DH), F32),
            pltpu.VMEM((m, rows, heads * DH), BF16),
            pltpu.VMEM((8, rows), F32),
            pltpu.VMEM((m - 1, 8, rows), F32),
            pltpu.VMEM((rows, width), BF16),
            pltpu.VMEM((2 * rows, m * width), BF16),
            pltpu.VMEM((2, 8, rows), F32),
            pltpu.VMEM((m, 8, rows), F32),
            pltpu.VMEM((2 * rows, own_width), BF16),
            pltpu.VMEM((n * CHUNKS, 2 * rows, depth // CHUNKS), BF16),
            pltpu.VMEM((2, 2, CHUNKS, 2 * rows, depth // CHUNKS), BF16),
            pltpu.VMEM((2, 2, CHUNKS, 2 * rows, depth // CHUNKS), BF16),
            pltpu.VMEM((2, CHUNKS, 2 * rows, depth // CHUNKS), BF16),
            pltpu.VMEM((2, CHUNKS, rows, depth // CHUNKS), BF16),
            pltpu.VMEM((2, CHUNKS, rows, depth // CHUNKS), BF16),
            pltpu.VMEM((2, CHUNKS, rows, depth // CHUNKS), BF16),
            dma((m - 1,)),
            dma((m - 1,)),
            dma((2, lines - 1, CHUNKS * SUBS)),
            dma((2, lines - 1, CHUNKS * SUBS)),
            dma((2, CHUNKS * SUBS)),
            dma((2, lines, CHUNKS * SUBS)),
            dma((2, lines, CHUNKS * SUBS)),
            dma((2,)),
            dma((2,)),
            dma((back, 2)),
            dma((back, 2)),
            dma((m - 1, heads)),
            dma((m - 1, heads)),
            dma((m - 1,)),
            dma((m - 1,)),
            dma((2 * m - 1,)),
            dma((2 * m - 1,)),
            dma((m,)),
            dma((m,)),
            dma((2, 2, CHUNKS, 2)),
            dma((2, 2, CHUNKS, 2)),
            dma((2, CHUNKS, 2)),
            dma((2, CHUNKS, 2)),
            dma((2, CHUNKS)),
            dma((2, CHUNKS)),
            dma((2, CHUNKS)),
            dma((8,)),
            dma((2, CHUNKS)),
        ],
        compiler_params=pltpu.CompilerParams(
            collective_id=0, has_side_effects=True, vmem_limit_bytes=60 * 1024 * 1024
        ),
        name="layer",
    )(
        queries,
        keys,
        values,
        output_gate_logits,
        forget_gate_logits.T,
        extra_decay_log.T,
        input_gate_log.T,
        document[None, :],
        residual,
        cell_norm_gain,
        mixer_norm_gain,
        output_weight,
        up_weight,
        down_weight,
    )


def either(n, m, *args):
    depth, hidden_width = args[12].shape
    heads = args[0].shape[1] // DH
    fits = n == 8 and m == 4 and depth % 128 == 0 and hidden_width % 512 == 0
    fits = fits and 3 * heads <= 8 and args[8].shape[1] == 2 * depth
    fits = fits and args[0].shape[0] % 256 == 0
    if fits:
        return fused(n, m, *args)
    return local(*args)


def solution(mesh):
    in_specs = (
        P("sp", "tp"),
        P("sp", "tp"),
        P("sp", "tp"),
        P("sp", "tp"),
        P("sp", "tp"),
        P("sp", "tp"),
        P("sp", "tp"),
        P("sp"),
        P("sp", "tp"),
        P("tp"),
        P("tp", None),
        P("tp"),
        P("sp", "tp"),
        P("tp", "sp"),
    )
    out_specs = P("sp", "tp")
    body = functools.partial(either, mesh.shape["sp"], mesh.shape["tp"])
    return jax.shard_map(body, mesh=mesh, in_specs=in_specs, out_specs=out_specs, check_vma=False)
```
